32 devices in a mesh: sp: 8 (over z, x), tp: 4 (over y, core).
Axes of the slice: x: 2, y: 2, z: 4, core: 2. Of those that a mesh axis runs over, the one named last changes fastest.
Arguments:
- inputs: bfloat16 [5120, 2048], P('sp', 'tp'), may hold values from -6 to 6
- norm_gain: bfloat16 [2048], P('tp'), may hold values from 0.099609375 to 1.8984375
- query_weight: bfloat16 [2048, 2048], P('sp', 'tp'), may hold values from -0.125 to 0.125
- key_weight: bfloat16 [2048, 2048], P('sp', 'tp'), may hold values from -0.125 to 0.125
- value_weight: bfloat16 [2048, 2048], P('sp', 'tp'), may hold values from -0.125 to 0.125
- outgate_weight: bfloat16 [2048, 2048], P('sp', 'tp'), may hold values from -0.125 to 0.125
- inputgate_weight: bfloat16 [2048, 8], replicated, may hold values from -1 to 1
- forget_weight: bfloat16 [2048, 8], replicated, may hold values from -0.125 to 0.125
- forget_bias: float32 [8], P('tp'), may hold values from -1.1 to 2.25
- conv_query: float32 [4, 2048], P(None, 'tp'), may hold values from -3 to 3
- conv_key: float32 [4, 2048], P(None, 'tp'), may hold values from -3 to 3
- cell_gain: float32 [2048], P('tp'), may hold values from 0.1 to 1.9
- pool_weight: bfloat16 [2048, 1024], P('sp', 'tp'), may hold values from -0.125 to 0.125
- group_weight: bfloat16 [8, 128, 128], P('tp'), may hold values from -0.5 to 0.5
- pool_gain: float32 [1024], P('tp'), may hold values from 0.1 to 1.9
- cell_out_weight: bfloat16 [2048, 2048], P('tp', 'sp'), may hold values from -0.109375 to 0.109375
- pool_out_weight: bfloat16 [1024, 2048], P('tp', 'sp'), may hold values from -0.109375 to 0.109375
Outputs:
- mixed: bfloat16 [5120, 2048], P(('sp', 'tp'))
The draws below stay inside these ranges and needn't reach their ends.
All inputs are finite; a program needn't handle non-finite values.
Results may differ from the reference program's by a relative error of at most 0.013.
The reference program's roundings to bfloat16 on the way (of `normed`, `cell_mix`, `pooled` and `pool_mix`) count: a program that leaves them out, or rounds other values in their place, can miss the bound.
Values may be sent and summed in bfloat16 or wider, within the bound.
A program may use at most 128 MiB of HBM per device.

```python
import math
import jax
import jax.numpy as jnp
from jax import lax

D = 2048
HM = 8
DH = 256
PG = 8
CG = 128
LEVELS = 4
CONV = 4
TOK_DEV = 640
TOKENS = 5120
N_SP = 8


def draw_inputs(key, part):
    jitter = jax.random.normal(jax.random.fold_in(key, 12), (TOKENS, D), jnp.float32)
    values = jnp.clip(jitter, -6.0, 6.0)
    return values.astype(jnp.bfloat16)


def draw_inputgate_weight(key, part):
    spread = D ** (-0.5)
    jitter = jnp.clip(jax.random.normal(jax.random.fold_in(key, 13), (D, HM), jnp.float32), -6.0, 6.0) * spread
    values = jitter
    return values.astype(jnp.bfloat16)


def block_scale(own_key, shape, cuts, smallest, top_value):
    def one(dim, blocks):
        draws = jax.random.uniform(jax.random.fold_in(jax.random.fold_in(own_key, 6), dim), (blocks,), jnp.float32, smallest / len(cuts), top_value / len(cuts))
        return jnp.repeat(jnp.exp(draws), shape[dim] // blocks).reshape((-1,) + (1,) * (len(shape) - dim - 1))

    gain = one(*cuts[0])
    for cut in cuts[1:]:
        gain = gain * one(*cut)
    return gain


def normal_values(key, extent, width, most, split=(), kind=jnp.bfloat16):
    values = jax.random.normal(key, extent, jnp.float32) * width
    if len(split) > 0:
        values = block_scale(key, extent, split, -0.22, 0.18) * values
    return jnp.clip(values, min=-most, max=most).astype(kind)


def setup_inputs(seed: int = 0) -> dict:
    key_of = jax.random.split(jax.random.key(seed), 18)
    return {
        "inputs": draw_inputs(jax.random.fold_in(key_of[17], 71), 0),
        "norm_gain": jnp.clip(1.0 + 0.18 * jax.random.normal(key_of[1], (D,), jnp.float32), 0.099609375, 1.8984375).astype(jnp.bfloat16),
        "query_weight": normal_values(key_of[2], (D, HM * DH), D ** -0.5, 0.125, ((0, 8), (1, 4))),
        "key_weight": normal_values(key_of[3], (D, HM * DH), D ** -0.5, 0.125, ((0, 8), (1, 4))),
        "value_weight": normal_values(key_of[4], (D, HM * DH), D ** -0.5, 0.125, ((0, 8), (1, 4))),
        "outgate_weight": normal_values(key_of[5], (D, HM * DH), D ** -0.5, 0.125, ((0, 8), (1, 4))),
        "inputgate_weight": draw_inputgate_weight(jax.random.fold_in(key_of[17], 71), 0),
        "forget_weight": normal_values(key_of[7], (D, HM), D ** -0.5, 0.125),
        "forget_bias": jnp.clip(-1.1 + 3.35 * jax.random.uniform(key_of[8], (HM,), jnp.float32) ** block_scale(key_of[8], (HM,), ((0, 4),), -0.2, 0.2), -1.1, 2.25),
        "conv_query": normal_values(key_of[9], (CONV, HM * DH), CONV ** -0.5, 3.0, ((1, 4),), jnp.float32),
        "conv_key": normal_values(key_of[10], (CONV, HM * DH), CONV ** -0.5, 3.0, ((1, 4),), jnp.float32),
        "cell_gain": jnp.clip(1.0 + 0.18 * jax.random.normal(key_of[11], (HM * DH,), jnp.float32), 0.1, 1.9),
        "pool_weight": normal_values(key_of[12], (D, PG * CG), D ** -0.5, 0.125, ((0, 8), (1, 4))),
        "group_weight": normal_values(key_of[13], (PG, CG, CG), CG ** -0.5, 0.5, ((0, 4),)),
        "pool_gain": jnp.clip(1.0 + 0.18 * jax.random.normal(key_of[14], (PG * CG,), jnp.float32), 0.1, 1.9),
        "cell_out_weight": normal_values(key_of[15], (HM * DH, D), (HM * DH + PG * CG) ** -0.5, 0.109375, ((0, 4), (1, 8))),
        "pool_out_weight": normal_values(key_of[16], (PG * CG, D), (HM * DH + PG * CG) ** -0.5, 0.109375, ((0, 4), (1, 8))),
    }


epsilon = 1e-06
big_negative = -1e+30
highest = lax.Precision.HIGHEST

def causal_taps(padded, taps):
    span_rows = padded.shape[0] - taps.shape[0] + 1
    running = jnp.zeros((span_rows, padded.shape[1]), jnp.float32)
    for lag_index in range(taps.shape[0]):
        running = running + taps[lag_index] * padded[lag_index:lag_index + span_rows].astype(jnp.float32)
    return running

def cell_block(carry, block_inputs):
    memory, normalizer, stabilizer = carry
    queries, key_rows, value_rows, log_in, log_keep = block_inputs
    query_wide = queries.astype(jnp.float32)
    key_wide = key_rows.astype(jnp.float32)
    value_wide = value_rows.astype(jnp.float32)
    length = queries.shape[0]
    cumulative = jnp.cumsum(log_keep, axis=0)
    cum_heads = cumulative.T
    in_heads = log_in.T
    causal = jnp.arange(length)[:, None] >= jnp.arange(length)[None, :]
    decay_log = cum_heads[:, :, None] - cum_heads[:, None, :] + in_heads[:, None, :]
    decay_log = jnp.where(causal[None, :, :], decay_log, -jnp.inf)
    carried_log = cum_heads + stabilizer[:, None]
    ceiling = jnp.maximum(carried_log, lax.optimization_barrier(jnp.max(decay_log, axis=2)))
    within = jnp.exp(decay_log - ceiling[:, :, None])
    carried = jnp.exp(carried_log - ceiling)
    raw_scores = jnp.einsum('thd,shd->hts', query_wide, key_wide, precision=highest)
    scores = (raw_scores * within).astype(jnp.bfloat16).astype(jnp.float32)
    numerator = carried.T[:, :, None] * jnp.einsum('hvk,thk->thv', memory, query_wide, precision=highest)
    numerator = numerator + jnp.einsum('hts,shv->thv', scores, value_wide, precision=highest)
    denominator = carried.T * jnp.einsum('hk,thk->th', normalizer, query_wide, precision=highest) + lax.optimization_barrier(jnp.sum(scores, axis=2)).T
    hidden = numerator / jnp.maximum(jnp.abs(denominator), jnp.exp(-ceiling.T))[:, :, None]
    final_log = cumulative[-1]
    lead_log = final_log[None, :] - cumulative + log_in
    new_stab = jnp.maximum(final_log + stabilizer, lax.optimization_barrier(jnp.max(lead_log, axis=0)))
    share_weight = jnp.exp(lead_log - new_stab[None, :])
    fade_factor = jnp.exp(final_log + stabilizer - new_stab)
    weighted = (value_wide * share_weight[:, :, None]).astype(jnp.bfloat16).astype(jnp.float32)
    memory = fade_factor[:, None, None] * memory + jnp.einsum('shv,shk->hvk', weighted, key_wide, precision=highest)
    normalizer = fade_factor[:, None] * normalizer + jnp.einsum('sh,shk->hk', share_weight, key_wide, precision=highest)
    return ((memory, normalizer, new_stab), hidden)

def reference(inputs, norm_gain, query_weight, key_weight, value_weight, outgate_weight, inputgate_weight, forget_weight, forget_bias, conv_query, conv_key, cell_gain, pool_weight, group_weight, pool_gain, cell_out_weight, pool_out_weight):
    wide_in = inputs.astype(jnp.float32)
    inverse_rms = lax.rsqrt(lax.optimization_barrier(jnp.mean(wide_in * wide_in, axis=1, keepdims=True)) + epsilon)
    normed = (wide_in * norm_gain.astype(jnp.float32)).astype(jnp.bfloat16)

    def project(weight):
        return jnp.dot(normed, weight, preferred_element_type=jnp.float32) * inverse_rms
    query_pre = project(query_weight).astype(jnp.bfloat16)
    key_pre = project(key_weight).astype(jnp.bfloat16)
    value_rows = project(value_weight).astype(jnp.bfloat16)
    outgate_pre = project(outgate_weight).astype(jnp.bfloat16)
    pool_pre = project(pool_weight).astype(jnp.bfloat16)
    log_in = project(inputgate_weight)
    log_keep = jax.nn.log_sigmoid(project(forget_weight) + forget_bias + math.log(TOKENS))
    margin = conv_query.shape[0] - 1
    query_taps = causal_taps(jnp.pad(query_pre, ((margin, 0), (0, 0))), conv_query)
    key_taps = causal_taps(jnp.pad(key_pre, ((margin, 0), (0, 0))), conv_key)
    queries = (jax.nn.silu(query_taps) * DH ** (-0.5)).astype(jnp.bfloat16)
    key_rows = jax.nn.silu(key_taps).astype(jnp.bfloat16)

    def to_blocks(array):
        return array.reshape((N_SP, TOK_DEV) + array.shape[1:])

    def split_heads(array):
        return array.reshape(TOKENS, HM, DH)
    start_carry = (jnp.zeros((HM, DH, DH), jnp.float32), jnp.zeros((HM, DH), jnp.float32), jnp.full((HM,), big_negative, jnp.float32))
    block_inputs = (to_blocks(split_heads(queries)), to_blocks(split_heads(key_rows)), to_blocks(split_heads(value_rows)), to_blocks(log_in), to_blocks(log_keep))
    ignored, hidden = lax.scan(cell_block, start_carry, block_inputs)
    hidden = hidden.reshape(TOKENS, HM, DH)
    normalized = hidden * lax.rsqrt(lax.optimization_barrier(jnp.mean(hidden * hidden, axis=2, keepdims=True)) + epsilon)
    cell_mix = (normalized.reshape(TOKENS, HM * DH) * cell_gain * jax.nn.sigmoid(outgate_pre.astype(jnp.float32))).astype(jnp.bfloat16)
    widest = 2 ** LEVELS - 1
    padded_pool = jnp.pad(pool_pre, ((widest, 0), (0, 0))).astype(jnp.float32)
    position = jnp.arange(TOKENS)
    pieces = []
    for group_index in range(PG):
        reach_rows = 2 ** (1 + group_index % LEVELS)
        columns = padded_pool[:, group_index * CG:(group_index + 1) * CG]
        window_sum = jnp.zeros((TOKENS, CG), jnp.float32)
        for lag_index in range(reach_rows):
            window_sum = window_sum + columns[widest - lag_index:widest - lag_index + TOKENS]
        counted = jnp.minimum(position + 1, reach_rows).astype(jnp.float32)[:, None]
        pieces.append(window_sum / counted - columns[widest:])
    pooled = jnp.stack(pieces, axis=1).astype(jnp.bfloat16)
    grouped_out = jnp.einsum('sgc,gcd->sgd', pooled.astype(jnp.float32), group_weight.astype(jnp.float32), precision=highest)
    pool_mix = (grouped_out.reshape(TOKENS, PG * CG) * pool_gain).astype(jnp.bfloat16)
    mixed = jnp.dot(cell_mix, cell_out_weight, preferred_element_type=jnp.float32)
    mixed = mixed + jnp.dot(pool_mix, pool_out_weight, preferred_element_type=jnp.float32)
    return mixed.astype(jnp.bfloat16)
```

```python
import functools
import math

import jax
import jax.numpy as jnp
from jax import lax
from jax.experimental import pallas as pl
from jax.experimental.pallas import tpu as pltpu
from jax.sharding import PartitionSpec as P

LEVELS = 4

epsilon = 1e-06
big_negative = -1e30
highest = lax.Precision.HIGHEST
MESH = pl.DeviceIdType.MESH


def remote(src, dst, send, recv, device):
    return pltpu.make_async_remote_copy(
        src_ref=src, dst_ref=dst, send_sem=send, recv_sem=recv,
        device_id=device, device_id_type=MESH,
    )


def columns_of(rows):
    filled = jnp.concatenate(
        rows + [jnp.zeros((128 - len(rows), rows[0].shape[1]), jnp.float32)], axis=0
    )
    return filled.T


def scanned(row, combine, fill):
    length = row.shape[1]
    lane = lax.broadcasted_iota(jnp.int32, (8, length), 1)
    value = jnp.broadcast_to(row, (8, length))
    step = 1
    while step < length:
        moved = pltpu.roll(value, step, 1)
        value = combine(value, jnp.where(lane >= step, moved, fill))
        step *= 2
    return value[:1]


def mixer_kernel(
    pairs, tall, tokens, head, group,
    x_ref, wp_ref, wo_ref, gatew_ref, bias_ref, taps_ref, gain_ref, group_ref, pool_gain_ref,
    out_ref,
    x_out, wp_out, wo_out, normed, inv_s, raw_gate, acc, pre_ref, w_ref,
    edge_q, edge_p, ext, ext_p, q_s, k_s, num_s, small_s, mix_s, st, st_low, st_in, low_in,
    give, got, total,
    local_sem, x_send, x_recv, s_send, s_recv, h_send, h_recv, r_send, r_recv,
    edge_sem, state_send, state_recv, send, recv, d_send, d_recv,
):
    f32, bf16 = jnp.float32, jnp.bfloat16
    height = out_ref.shape[0]
    span = 2 * tokens
    length = tokens
    features = x_out.shape[2]
    sp, tp = lax.axis_index("sp"), lax.axis_index("tp")
    pair, half = sp // 2, sp % 2
    row, side = tp // 2, tp % 2
    width = x_ref.shape[1]
    other = 2 * pair + 1 - half
    sibling = (sp, 2 * row + 1 - side)
    right = (2 * lax.rem(pair + 1, pairs) + half, tp)
    left = (2 * lax.rem(pair + pairs - 1, pairs) + half, tp)
    offsets = [(a, b) for a in range(2) for b in range(tall) if (a, b) != (0, 0)]
    peers = [
        (2 * pair + lax.rem(half + a, 2), 2 * lax.rem(row + b, tall) + side) for a, b in offsets
    ]

    places = [(a, b) for a in range(2) for b in range(tall)][::-1]
    count = len(places)

    def target(a, b):
        return (lax.rem(half + a, 2), lax.rem(row + b, tall))

    barrier = pltpu.get_barrier_semaphore()
    greeted = [sibling]
    for a, b in places[:-1]:
        h, r = target(a, b)
        greeted.append((2 * pair + h, 2 * r + side))
    for d in range(1, pairs):
        greeted.append((2 * lax.rem(pair + d, pairs) + half, tp))
    for device in greeted:
        pl.semaphore_signal(barrier, inc=1, device_id=device, device_id_type=MESH)
    pl.semaphore_wait(barrier, len(greeted))

    def x_block(h, r, s):
        column = pl.multiple_of((2 * r + s) * width, width)
        return x_out.at[h, :, pl.ds(column, width)]

    def ring_copies(k, direction, item):
        if direction == 0:
            source = lax.rem(pair - k + 1 + pairs, pairs)
        else:
            source = lax.rem(pair + k - 1, pairs)
        place = 2 * source + (half if item == 0 else 1 - half)
        target = right if direction == 0 else left
        own = k == 1 and item == 0
        index = ((k - 1) * 2 + direction) * 2 + item
        out = []
        for j, (whole, mine) in enumerate(((wp_out, wp_ref), (wo_out, wo_ref))):
            src = mine.at[half] if own else whole.at[place]
            out.append(
                remote(src, whole.at[place], r_send.at[index, j], r_recv.at[index, j], target)
            )
        return out

    steps = pairs // 2

    def has(k, direction, item):
        return k < steps or (k == steps and direction == item)

    swap = [
        remote(wp_ref.at[1 - half], wp_out.at[sp], h_send.at[0], h_recv.at[0], (other, tp)),
        remote(wo_ref.at[1 - half], wo_out.at[sp], h_send.at[1], h_recv.at[1], (other, tp)),
    ]
    for copy in swap:
        copy.start()
    rings = {}
    for direction in range(2):
        if has(1, direction, 0):
            rings[1, direction, 0] = ring_copies(1, direction, 0)
            for copy in rings[1, direction, 0]:
                copy.start()
    spread = []
    for i, device in enumerate(peers):
        copy = remote(x_ref, x_block(half, row, side), x_send.at[i], x_recv.at[i], device)
        copy.start()
        spread.append(copy)
    locals_ = [
        pltpu.make_async_copy(x_ref, x_block(half, row, side), local_sem.at[0]),
        pltpu.make_async_copy(wp_ref.at[half], wp_out.at[sp], local_sem.at[1]),
        pltpu.make_async_copy(wo_ref.at[half], wo_out.at[sp], local_sem.at[2]),
    ]
    for copy in locals_:
        copy.start()
    passed = [remote(x_ref, x_block(half, row, side), s_send.at[0], s_recv.at[0], sibling)]
    passed[0].start()

    acc[...] = jnp.zeros_like(acc)
    for copy in swap:
        copy.wait_recv()
    for direction in range(2):
        if has(1, direction, 1):
            rings[1, direction, 1] = ring_copies(1, direction, 1)
            for copy in rings[1, direction, 1]:
                copy.start()

    def advance(k):
        for item in range(2):
            for direction in range(2):
                if has(k, direction, item):
                    for copy in rings[k - 1, direction, item]:
                        copy.wait_recv()
                    rings[k, direction, item] = ring_copies(k, direction, item)
                    for copy in rings[k, direction, item]:
                        copy.start()
                elif has(k - 1, direction, item):
                    for copy in rings[k - 1, direction, item]:
                        copy.wait_recv()
            if k == 2 and item == 0:
                pass_on()

    def pass_on():
        for i, (a, b) in enumerate(offsets):
            spread[i].wait_recv()
            block = x_block(lax.rem(half + 2 - a, 2), lax.rem(row + tall - b, tall), side)
            copy = remote(block, block, s_send.at[i + 1], s_recv.at[i + 1], sibling)
            copy.start()
            passed.append(copy)

    for k in range(2, steps + 1):
        advance(k)
    if steps < 2:
        pass_on()
    for copy in passed:
        copy.wait_recv()
    for copy in locals_:
        copy.wait()

    whole_gain = x_out[0, tokens : tokens + 1, :].astype(f32)
    small_rows = 128 if tokens % 128 == 0 else tokens
    for h in range(2):
        @pl.loop(0, tokens // small_rows)
        def _(i):
            start = pl.multiple_of(i * small_rows, small_rows)
            wide = x_out[h, pl.ds(start, small_rows), :].astype(f32)
            squares = jnp.sum(wide * wide, axis=1, keepdims=True)
            there = pl.ds(h * tokens + start, small_rows)
            normed[there, :] = (wide * whole_gain).astype(bf16)
            inverse = lax.rsqrt(squares / features + epsilon)
            inv_s[there, :] = jnp.broadcast_to(inverse, (small_rows, 128))

    big_rows = 256 if span % 256 == 0 else span
    depth = wp_ref.shape[1]
    by_item = depth % 128 == 0

    def add_product(place):
        if by_item:
            @pl.loop(0, span // big_rows)
            def _(i):
                there = pl.ds(pl.multiple_of(i * big_rows, big_rows), big_rows)
                across = pl.ds(pl.multiple_of(place * depth, depth), depth)
                acc[there, :] += jnp.dot(
                    normed[there, across], wp_out[place], preferred_element_type=f32
                )

    @pl.loop(0, span // big_rows)
    def _(i):
        there = pl.ds(pl.multiple_of(i * big_rows, big_rows), big_rows)
        raw_gate[there, :] = inv_s[there, :] * jnp.dot(
            normed[there, :], gatew_ref[...], preferred_element_type=f32
        )

    def arrived_place(k, direction, item):
        source = lax.rem(pair - k + pairs, pairs) if direction == 0 else lax.rem(pair + k, pairs)
        return 2 * source + (half if item == 0 else 1 - half)

    add_product(sp)
    add_product(other)
    for k in range(1, steps):
        for direction in range(2):
            for item in range(2):
                add_product(arrived_place(k, direction, item))
    for direction in range(2):
        for item in range(2):
            if has(steps, direction, item):
                for copy in rings[steps, direction, item][:1]:
                    copy.wait_recv()
                add_product(arrived_place(steps, direction, item))

    @pl.loop(0, span // big_rows)
    def _(i):
        there = pl.ds(pl.multiple_of(i * big_rows, big_rows), big_rows)
        if by_item:
            product_here = acc[there, :]
        else:
            weights = wp_out[...].reshape(-1, wp_out.shape[2])
            product_here = jnp.dot(normed[there, :], weights, preferred_element_type=f32)
        pre_ref[there, :] = (product_here * inv_s[there, :1]).astype(bf16)

    gate_t = raw_gate[...].T
    keep = gate_t[1:2, :] + bias_ref[:, :1]
    small = jnp.exp(-jnp.abs(keep))
    ratio = small / (2.0 + small)
    square = ratio * ratio
    series = jnp.full_like(square, 1.0 / 17.0)
    for odd in (15, 13, 11, 9, 7, 5, 3, 1):
        series = series * square + 1.0 / odd
    log_keep_row = jnp.minimum(keep, 0.0) - 2.0 * ratio * series
    log_in_row = gate_t[0:1, :]

    following = (2 * lax.rem(pair + 1, pairs) + half, tp)
    edges = [
        remote(pre_ref.at[pl.ds(span - 16, 16), pl.ds(0, 2 * head)], edge_q,
               edge_sem.at[0], edge_sem.at[1], following),
        remote(pre_ref.at[pl.ds(span - 16, 16), pl.ds(4 * head, group)], edge_p,
               edge_sem.at[2], edge_sem.at[3], following),
    ]

    @pl.when(pair < pairs - 1)
    def _():
        for copy in edges:
            copy.start()

    @pl.when(pair == 0)
    def _():
        edge_q[...] = jnp.zeros_like(edge_q)
        edge_p[...] = jnp.zeros_like(edge_p)

    ext[pl.ds(16, span), :] = pre_ref[:, : 2 * head].astype(f32)
    ext_p[pl.ds(16, span), :] = pre_ref[:, 4 * head :].astype(f32)

    finals, tops, leads, gaps, cols = [], [], [], [], []
    for c in range(2):
        log_in = log_in_row[:, c * length : (c + 1) * length]
        cumulative = scanned(log_keep_row[:, c * length : (c + 1) * length], jnp.add, 0.0)
        gap = log_in - cumulative
        ceiling = scanned(gap, jnp.maximum, big_negative)
        final = cumulative[:, length - 1 :]
        top = final + ceiling[:, length - 1 :]
        share = jnp.exp(final + gap - top)
        finals.append(final)
        tops.append(top)
        gaps.append(gap)
        cols.append(columns_of([cumulative, ceiling, share]))

    @pl.when(pair > 0)
    def _():
        for copy in edges:
            copy.wait_recv()

    ext[pl.ds(0, 16), :] = edge_q[...].astype(f32)
    ext_p[pl.ds(0, 16), :] = edge_p[...].astype(f32)

    taps = taps_ref.shape[0]
    for c in range(2):
        running = None
        for j in range(taps):
            term = taps_ref[pl.ds(j, 1), :] * ext[pl.ds(16 + c * length - taps + 1 + j, length), :]
            running = term if running is None else running + term
        active = running * jax.nn.sigmoid(running)
        q_s[pl.ds(c * length, length), :] = (active[:, :head] * head ** (-0.5)).astype(bf16)
        k_s[pl.ds(c * length, length), :] = active[:, head:].astype(bf16)

    memories, normals = [], []
    for c in range(2):
        share = cols[c][:, 2:3]
        keys = k_s[pl.ds(c * length, length), :]
        values = pre_ref[pl.ds(c * length, length), pl.ds(2 * head, head)].astype(f32)
        memories.append(
            lax.dot_general(
                (values * share).astype(bf16), keys, (((0,), (0,)), ((), ())),
                preferred_element_type=f32,
            )
        )
        normals.append(jnp.sum(keys.astype(f32) * share, axis=0, keepdims=True))
    both = jnp.maximum(finals[1] + tops[0], tops[1])
    first, second = jnp.exp(finals[1] + tops[0] - both), jnp.exp(tops[1] - both)
    st[...] = (first * memories[0] + second * memories[1]).astype(bf16)
    st_low[...] = jnp.concatenate(
        [
            first * normals[0] + second * normals[1],
            jnp.broadcast_to(both, (1, head)),
            jnp.broadcast_to(finals[0] + finals[1], (1, head)),
            jnp.zeros((5, head), f32),
        ],
        axis=0,
    )
    states = []
    for d in range(1, pairs):
        to = (2 * lax.rem(pair + d, pairs) + half, tp)
        copies = [
            remote(st, st_in.at[d - 1], state_send.at[d - 1, 0], state_recv.at[d - 1, 0], to),
            remote(
                st_low, low_in.at[d - 1], state_send.at[d - 1, 1], state_recv.at[d - 1, 1], to
            ),
        ]
        states.append(copies)
        for copy in copies:
            pl.when(pair + d < pairs)(copy.start)

        @pl.when(pair < d)
        def _():
            st_in[d - 1] = jnp.zeros(st_in.shape[1:], bf16)
            low_in[d - 1] = jnp.zeros(low_in.shape[1:], f32)

    block = 128 if length % 128 == 0 else length
    for c in range(2):
        for t in range(0, length, block):
            reach = t + block
            scores = lax.dot_general(
                q_s[pl.ds(c * length + t, block), :], k_s[pl.ds(c * length, reach), :],
                (((1,), (1,)), ((), ())), preferred_element_type=f32,
            )
            weight = jnp.exp(
                jnp.minimum(gaps[c][:, :reach] - cols[c][t : t + block, 1:2], 0.0)
            )
            t_ids = t + lax.broadcasted_iota(jnp.int32, (block, reach), 0)
            s_ids = lax.broadcasted_iota(jnp.int32, (block, reach), 1)
            scores = jnp.where(t_ids >= s_ids, scores * weight, 0.0).astype(bf16)
            num_s[pl.ds(c * length + t, block), :] = jnp.dot(
                scores, pre_ref[pl.ds(c * length, reach), pl.ds(2 * head, head)],
                preferred_element_type=f32,
            )
            small_s[pl.ds(c * length + t, block), :] = jnp.broadcast_to(
                jnp.sum(scores.astype(f32), axis=1, keepdims=True), (block, 128)
            )

    level = (tp * 2 + half) % LEVELS
    window = None
    for step in range(LEVELS):
        low, high = (0, 2) if step == 0 else (2**step, 2 ** (step + 1))
        part = ext_p[pl.ds(16 - low, span), :]
        for lag in range(low + 1, high):
            part = part + ext_p[pl.ds(16 - lag, span), :]
        if window is None:
            window = part
        else:
            window = window + jnp.where(level >= step, part, 0.0)
    reach = lax.shift_left(jnp.int32(2), level.astype(jnp.int32))
    row_ids = pair * span + lax.broadcasted_iota(jnp.int32, (span, group), 0)
    counted = jnp.minimum(row_ids + 1, reach).astype(f32)
    pooled = (window / counted - ext_p[pl.ds(16, span), :]).astype(bf16)
    mix_s[:, head:] = (
        jnp.dot(pooled, group_ref[...], preferred_element_type=f32) * pool_gain_ref[...]
    ).astype(bf16)

    later = jnp.zeros((1, 1), f32)
    logs = []
    for d in range(1, pairs):
        for copy in states[d - 1]:
            pl.when(pair >= d)(copy.wait_recv)
        logs.append(jnp.where(pair >= d, low_in[d - 1, 1:2, :1] + later, big_negative))
        later = later + low_in[d - 1, 2:3, :1]
    ceiling_in = functools.reduce(jnp.maximum, logs)
    memory_in = jnp.zeros((head, head), f32)
    normal_in = jnp.zeros((1, head), f32)
    for d in range(1, pairs):
        factor = jnp.where(pair >= d, jnp.exp(logs[d - 1] - ceiling_in), 0.0)
        memory_in = memory_in + factor * st_in[d - 1].astype(f32)
        normal_in = normal_in + factor * low_in[d - 1, 0:1, :]
    for c in range(2):
        high = memory_in.astype(bf16)
        low = (memory_in - high.astype(f32)).astype(bf16)
        here = pl.ds(c * length, length)
        queries = q_s[here, :]
        over = (((1,), (1,)), ((), ()))
        far = lax.dot_general(queries, high, over, preferred_element_type=f32)
        far = far + lax.dot_general(queries, low, over, preferred_element_type=f32)
        far_sum = jnp.sum(queries.astype(f32) * normal_in, axis=1, keepdims=True)
        cum, near_top = cols[c][:, 0:1], cols[c][:, 1:2]
        near_log, far_log = cum + near_top, cum + ceiling_in
        ceiling = jnp.maximum(near_log, far_log)
        near_scale, far_scale = jnp.exp(near_log - ceiling), jnp.exp(far_log - ceiling)
        numerator = near_scale * num_s[here, :] + far_scale * far
        denominator = near_scale * small_s[here, :1] + far_scale * far_sum
        hidden = numerator / jnp.maximum(jnp.abs(denominator), jnp.exp(-ceiling))
        hidden = hidden * lax.rsqrt(jnp.mean(hidden * hidden, axis=1, keepdims=True) + epsilon)
        gate = jax.nn.sigmoid(pre_ref[here, pl.ds(3 * head, head)].astype(f32))
        mix_s[here, :head] = (hidden * gain_ref[...] * gate).astype(bf16)
        if c == 0:
            upper = jnp.maximum(finals[0] + ceiling_in, tops[0])
            kept, added = jnp.exp(finals[0] + ceiling_in - upper), jnp.exp(tops[0] - upper)
            memory_in = kept * memory_in + added * memories[0]
            normal_in = kept * normal_in + added * normals[0]
            ceiling_in = upper

    for direction in range(2):
        for item in range(2):
            if has(steps, direction, item):
                for copy in rings[steps, direction, item][1:]:
                    copy.wait_recv()
    columns = wo_out.shape[2]
    for s in range(wo_out.shape[0]):
        w_ref[:, s * columns : (s + 1) * columns] = wo_out[s]

    def product(a, b, s):
        h, r = target(a, b)
        start = pl.multiple_of(((h * tall + r) * 2 + s) * height, height)
        return jnp.dot(
            mix_s[pl.ds(start, height), :], w_ref[...], preferred_element_type=f32
        )

    crossed = []
    for i, (a, b) in enumerate(places):
        give[i] = product(a, b, 1 - side).astype(give.dtype)
        copy = remote(give.at[i], got.at[i], d_send.at[i], d_recv.at[i], sibling)
        copy.start()
        crossed.append(copy)
    sent = []
    for i, (a, b) in enumerate(places):
        mine = product(a, b, side)
        crossed[i].wait_recv()
        mine = mine + got[i].astype(f32)
        if i < count - 1:
            h, r = target(a, b)
            give[count + i] = mine.astype(give.dtype)
            copy = remote(
                give.at[count + i], got.at[count + i], send.at[i], recv.at[i],
                (2 * pair + h, 2 * r + side),
            )
            copy.start()
            sent.append(copy)
        else:
            total[...] = mine
    for i, copy in enumerate(sent):
        copy.wait_recv()
        total[...] += got[count + i].astype(f32)
    out_ref[...] = total[...].astype(out_ref.dtype)
    for copy in crossed + sent:
        copy.wait_send()
    for d in range(1, pairs):
        for copy in states[d - 1]:
            pl.when(pair + d < pairs)(copy.wait_send)

    @pl.when(pair < pairs - 1)
    def _():
        for copy in edges:
            copy.wait_send()

    for copy in swap + spread + passed + [c for copies in rings.values() for c in copies]:
        copy.wait_send()


def mixed_rows(rows_in, packed, packed_out, gate_weight, bias, taps, gain, own_group, pool_gain):
    pairs, n_tp = lax.axis_size("sp") // 2, lax.axis_size("tp")
    tall = n_tp // 2
    f32, bf16 = jnp.float32, jnp.bfloat16
    vmem = pl.BlockSpec(memory_space=pltpu.VMEM)
    dma = pltpu.SemaphoreType.DMA
    slots, steps = 4 * tall - 1, pairs // 2
    head, group = gain.shape[1], pool_gain.shape[1]
    tokens = rows_in.shape[0] - 16
    span, features, height = 2 * tokens, rows_in.shape[1] * n_tp, tokens // n_tp
    width = packed_out.shape[2] * 2 * pairs
    scratch = [
        ((2, rows_in.shape[0], features), bf16),
        ((2 * pairs,) + packed.shape[1:], bf16),
        ((2 * pairs,) + packed_out.shape[1:], bf16),
        ((span, features), bf16),
        ((span, 128), f32),
        ((span, 128), f32),
        ((span, packed.shape[2]), f32),
        ((span, packed.shape[2]), bf16),
        ((head + group, width), bf16),
        ((16, 2 * head), bf16),
        ((16, group), bf16),
        ((span + 16, 2 * head), f32),
        ((span + 16, group), f32),
        ((span, head), bf16),
        ((span, head), bf16),
        ((span, head), f32),
        ((span, 128), f32),
        ((span, head + group), bf16),
        ((head, head), bf16),
        ((8, head), f32),
        ((pairs - 1, head, head), bf16),
        ((pairs - 1, 8, head), f32),
        ((slots, height, width), bf16),
        ((slots, height, width), bf16),
        ((height, width), f32),
    ]
    return pl.pallas_call(
        functools.partial(mixer_kernel, pairs, tall, tokens, head, group),
        out_shape=jax.ShapeDtypeStruct((height, width), bf16),
        in_specs=[vmem] * 9,
        out_specs=vmem,
        scratch_shapes=[pltpu.VMEM(shape, kind) for shape, kind in scratch] + [
            dma((3,)),
            dma((2 * tall,)), dma((2 * tall,)),
            dma((2 * tall,)), dma((2 * tall,)),
            dma((2,)), dma((2,)),
            dma((steps * 4, 2)), dma((steps * 4, 2)),
            dma((4,)), dma((pairs - 1, 2)), dma((pairs - 1, 2)),
            dma((2 * tall,)), dma((2 * tall,)), dma((2 * tall,)), dma((2 * tall,)),
        ],
        compiler_params=pltpu.CompilerParams(
            collective_id=0, has_side_effects=True, vmem_limit_bytes=63 * 2**20
        ),
    )(rows_in, packed, packed_out, gate_weight, bias, taps, gain, own_group, pool_gain)


HALO = 16


def quad_kernel(
    quads, tokens, head, group,
    x_ref, key_ref, value_ref, query_ref, outgate_ref, pool_ref, cell_out_ref, pool_out_ref,
    norm_ref, in_ref, keep_ref, bias_ref, conv_query_ref, conv_key_ref, gain_ref, group_ref,
    pool_gain_ref,
    out_ref,
    x_all, gain_all, w_all, wo_all, gatew, normed, inv_s, raw_gate, acc, pre_ref, ext, ext_p,
    q_s, k_s, num_s, small_s, mix_s, st_own, low_own, st_near, low_near, st_quad, low_quad,
    st_far, low_far, give, got, give_y, got_y, give_z, got_z, total,
    local_sem, halo_sem, gain_send, gain_recv, xz_send, xz_recv, xy_send, xy_recv,
    xs_send, xs_recv, z_send, x_send, w_recv, near_send, near_recv, far_send, far_recv,
    c_send, c_recv, y_send, y_recv, t_send, t_recv,
):
    f32, bf16 = jnp.float32, jnp.bfloat16
    height = out_ref.shape[0]
    rows = tokens + HALO
    span = 2 * rows
    width = x_ref.shape[1]
    features = x_all.shape[2]
    depth, columns = key_ref.shape[0], cell_out_ref.shape[1]
    sp, tp = lax.axis_index("sp"), lax.axis_index("tp")
    q, l, x = sp // 4, (sp // 2) % 2, sp % 2
    y, side = tp // 2, tp % 2
    here = 2 * q + l
    n_sp = 4 * quads

    def device(plane, x_, y_, side_):
        return (2 * plane + x_, 2 * y_ + side_)

    partner_plane = 2 * q + 1 - l
    beside = device(here, 1 - x, y, side)
    partner = device(partner_plane, x, y, side)
    across = device(here, x, 1 - y, side)
    sibling = device(here, x, y, 1 - side)
    nears, fars = [], []
    for e in range(1, quads):
        other = lax.rem(q + e, quads)
        behind = (other < q).astype(jnp.int32)
        nears.append(2 * other + behind)
        fars.append(2 * other + 1 - behind)
    following = lax.rem(sp + 1, n_sp)
    crowd = [(0, 1), (1, 0), (1, 1)]

    def mate(a, b):
        return (sp, 2 * lax.rem(y + a, 2) + lax.rem(side + b, 2))

    barrier = pltpu.get_barrier_semaphore()
    greeted = [beside, partner, (following, tp), (lax.rem(sp + n_sp - 1, n_sp), tp)]
    greeted += [mate(a, b) for a, b in crowd]
    greeted += [device(plane, x, y, side) for plane in nears + fars]
    for to in greeted:
        pl.semaphore_signal(barrier, inc=1, device_id=to, device_id_type=MESH)
    pl.semaphore_wait(barrier, len(greeted))

    started = []

    def begin(copy):
        copy.start()
        started.append(copy)

    own_column = pl.ds(pl.multiple_of(tp * width, width), width)

    def column_of(y_, side_):
        return pl.ds(pl.multiple_of((2 * y_ + side_) * width, width), width)

    pieces = (tokens // 2) // HALO * HALO
    cuts = [(HALO, pieces), (HALO + pieces, tokens - pieces), (0, HALO)]

    def x_place(block, cut, column):
        start, size = cuts[cut]
        return x_all.at[block, pl.ds(start, size), column]

    def x_mine(cut):
        start, size = cuts[cut]
        if cut == 2:
            return x_place(l, cut, own_column)
        return x_ref.at[pl.ds(start - HALO, size), :]

    def partner_copy(cut):
        return remote(
            x_mine(cut), x_place(l, cut, own_column), xz_send.at[cut], xz_recv.at[cut], partner
        )

    def across_copy(which, cut):
        src = x_mine(cut) if which == 0 else x_place(1 - l, cut, own_column)
        block = l if which == 0 else 1 - l
        return remote(
            src, x_place(block, cut, own_column), xy_send.at[which, cut], xy_recv.at[which, cut],
            across,
        )

    def sibling_copy(which, cut):
        block = l if which % 2 == 0 else 1 - l
        place = x_place(block, cut, column_of(y if which < 2 else 1 - y, side))
        src = x_mine(cut) if which == 0 else place
        return remote(src, place, xs_send.at[which, cut], xs_recv.at[which, cut], sibling)

    halo = remote(
        x_ref.at[pl.ds(tokens - HALO, HALO), :],
        x_all.at[lax.rem(following // 2, 2), pl.ds(0, HALO), own_column],
        halo_sem.at[0], halo_sem.at[1], (following, tp),
    )
    halo_here = remote(
        x_ref.at[pl.ds(tokens - HALO, HALO), :], x_place(l, 2, own_column),
        halo_sem.at[0], halo_sem.at[1], (following, tp),
    )
    pl.when(sp < n_sp - 1)(halo.start)
    for cut in range(2):
        begin(partner_copy(cut))
        begin(across_copy(0, cut))
        begin(sibling_copy(0, cut))

    weights = [
        (key_ref, 0, head), (value_ref, head, head), (query_ref, 2 * head, head),
        (outgate_ref, 3 * head, head), (pool_ref, 4 * head, group),
        (cell_out_ref, 0, head), (pool_out_ref, head, group),
    ]
    classes = {"kv": (0, 1), "q": (2,), "op": (3, 4), "wo": (5, 6)}

    def weight_source(j, half):
        ref, start, size = weights[j]
        cut = pl.ds(pl.multiple_of(half * size, size), size)
        return ref.at[:, cut] if j < 5 else ref.at[cut, :]

    def weight_place(j, place):
        ref, start, size = weights[j]
        if j < 5:
            return w_all.at[pl.ds(pl.multiple_of(place * depth, depth), depth), pl.ds(start, size)]
        return wo_all.at[pl.ds(start, size), pl.ds(pl.multiple_of(place * columns, columns), columns)]

    def send_weight(name, plane):
        for j in classes[name]:
            begin(remote(
                weight_source(j, lax.rem(plane, 2)), weight_place(j, sp),
                z_send.at[plane, j], w_recv.at[sp, j], device(plane, x, y, side),
            ))

    def arrived(name, place):
        for j in classes[name]:
            there = weight_place(j, place)
            remote(there, there, x_send.at[0, j], w_recv.at[place, j], beside).wait_recv()

    def forward(name, plane):
        place = 2 * plane + x
        arrived(name, place)
        for j in classes[name]:
            there = weight_place(j, place)
            begin(remote(there, there, x_send.at[plane, j], w_recv.at[place, j], beside))

    planes = [partner_plane] + nears + fars
    for name in ("kv", "q", "op", "wo"):
        for j in classes[name]:
            begin(remote(
                weight_source(j, l), weight_place(j, sp), x_send.at[here, j], w_recv.at[sp, j],
                beside,
            ))
        for plane in planes:
            send_weight(name, plane)
    locals_ = [pltpu.make_async_copy(x_mine(c), x_place(l, c, own_column), local_sem.at[7 + c])
               for c in range(2)]
    locals_ += [
        pltpu.make_async_copy(weight_source(j, l), weight_place(j, sp), local_sem.at[j])
        for j in range(7)
    ]
    for copy in locals_:
        copy.start()

    gain_all[:, own_column] = jnp.broadcast_to(norm_ref[...], (HALO, width))
    gains = []
    for i, (a, b) in enumerate(crowd):
        there = gain_all.at[:, own_column]
        copy = remote(there, there, gain_send.at[i], gain_recv.at[i], mate(a, b))
        begin(copy)
        gains.append(copy)
    gatew[...] = jnp.zeros_like(gatew)
    gatew[0:16, :] = jnp.concatenate([in_ref[...], keep_ref[...]], axis=0)

    @pl.when(sp == 0)
    def _():
        x_all[0, 0:HALO, own_column] = jnp.zeros((HALO, width), bf16)

    pl.when(sp > 0)(halo_here.wait_recv)
    begin(partner_copy(2))
    begin(across_copy(0, 2))
    begin(sibling_copy(0, 2))

    for cut in (0, 1, 2):
        partner_copy(cut).wait_recv()
        begin(across_copy(1, cut))
        begin(sibling_copy(1, cut))
        across_copy(0, cut).wait_recv()
        begin(sibling_copy(2, cut))
    for plane in nears:
        forward("kv", plane)
    forward("kv", partner_plane)
    for plane in nears:
        forward("q", plane)
    for cut in (0, 1, 2):
        across_copy(1, cut).wait_recv()
        begin(sibling_copy(3, cut))
    forward("q", partner_plane)
    for copy in gains:
        copy.wait_recv()
    for copy in locals_:
        copy.wait()
    for which in range(4):
        for cut in range(3):
            sibling_copy(which, cut).wait_recv()

    whole_gain = gain_all[0:1, :].astype(f32)
    small_rows = HALO

    @pl.loop(0, rows // small_rows)
    def _(i):
        for b in range(2):
            start = pl.multiple_of(i * small_rows, small_rows)
            there = pl.ds(pl.multiple_of(b * rows + i * small_rows, small_rows), small_rows)
            wide = x_all[b, pl.ds(start, small_rows), :].astype(f32)
            squares = jnp.sum(wide * wide, axis=1, keepdims=True)
            normed[there, :] = (wide * whole_gain).astype(bf16)
            inverse = lax.rsqrt(squares / features + epsilon)
            inv_s[there, :] = jnp.broadcast_to(inverse, (small_rows, 128))

    for plane in fars:
        forward("kv", plane)

    big = 256
    parts = span // big
    left_over = span - parts * big

    def strips(body):
        @pl.loop(0, parts)
        def _(i):
            body(pl.ds(pl.multiple_of(i * big, big), big))

        if left_over:
            body(pl.ds(parts * big, left_over))

    spans = {"kv": (0, 2 * head), "q": (2 * head, head), "op": (3 * head, head + group)}

    def add_product(name, plane, first, last):
        start, size = spans[name]
        cut = pl.ds(start, size)
        deep = pl.ds(pl.multiple_of(plane * 2 * depth, 2 * depth), 2 * depth)

        def body(there):
            product = jnp.dot(
                normed[there, deep], w_all[deep, cut], preferred_element_type=f32
            )
            if not first:
                product = product + acc[there, cut]
            if last:
                pre_ref[there, cut] = (product * inv_s[there, :1]).astype(bf16)
            else:
                acc[there, cut] = product

        strips(body)

    half_rows = tokens // 2 if tokens % 32 == 0 else tokens

    for b in range(2):
        @pl.loop(0, tokens // half_rows)
        def _(i):
            there = pl.ds(pl.multiple_of(b * rows + HALO + i * half_rows, HALO), half_rows)
            to = pl.ds(pl.multiple_of(b * tokens + i * half_rows, HALO), half_rows)
            raw_gate[to, :] = inv_s[there, :] * lax.dot_general(
                normed[there, :], gatew[...], (((1,), (1,)), ((), ())),
                preferred_element_type=f32,
            )

    def both_arrived(name, plane):
        arrived(name, 2 * plane + 1 - x)

    both_arrived("kv", here)
    add_product("kv", here, True, False)
    for plane in nears:
        forward("op", plane)
        both_arrived("kv", plane)
        add_product("kv", plane, False, False)
    for plane in fars:
        forward("q", plane)
    both_arrived("kv", partner_plane)
    add_product("kv", partner_plane, False, quads == 1)
    forward("op", partner_plane)
    for i, plane in enumerate(fars):
        both_arrived("kv", plane)
        add_product("kv", plane, False, i == len(fars) - 1)
    for plane in fars:
        forward("op", plane)

    gate_t = raw_gate[...].T
    which_row = lax.broadcasted_iota(jnp.int32, (8, 2 * tokens), 0) == tp * 2 + l
    log_in_row = jnp.sum(jnp.where(which_row, gate_t[0:8, :], 0.0), axis=0, keepdims=True)
    keep = jnp.sum(jnp.where(which_row, gate_t[8:16, :], 0.0), axis=0, keepdims=True)
    keep = keep + (bias_ref[l] + math.log(tokens * n_sp))
    small = jnp.exp(-jnp.abs(keep))
    ratio = small / (2.0 + small)
    square = ratio * ratio
    series = jnp.full_like(square, 1.0 / 17.0)
    for odd in (15, 13, 11, 9, 7, 5, 3, 1):
        series = series * square + 1.0 / odd
    log_keep_row = jnp.minimum(keep, 0.0) - 2.0 * ratio * series

    finals, tops, gaps, cols = [], [], [], []
    for b in range(2):
        log_in = log_in_row[:, b * tokens : (b + 1) * tokens]
        cumulative = scanned(log_keep_row[:, b * tokens : (b + 1) * tokens], jnp.add, 0.0)
        gap = log_in - cumulative
        ceiling = scanned(gap, jnp.maximum, big_negative)
        final = cumulative[:, tokens - 1 :]
        top = final + ceiling[:, tokens - 1 :]
        share = jnp.exp(final + gap - top)
        finals.append(final)
        tops.append(top)
        gaps.append(gap)
        cols.append(columns_of([cumulative, ceiling, share]))

    taps = conv_key_ref.shape[0]
    own_head = pl.ds(pl.multiple_of(l * head, head), head)
    own_group = pl.ds(pl.multiple_of(l * group, group), group)

    def convolved(conv_ref, start):
        out = []
        for b in range(2):
            ext[...] = pre_ref[pl.ds(b * rows, rows), pl.ds(start, head)].astype(f32)
            running = None
            for j in range(taps):
                term = conv_ref[pl.ds(j, 1), own_head] * ext[pl.ds(HALO - taps + 1 + j, tokens), :]
                running = term if running is None else running + term
            out.append(running * jax.nn.sigmoid(running))
        return out

    for b, active in enumerate(convolved(conv_key_ref, 0)):
        k_s[pl.ds(b * tokens, tokens), :] = active.astype(bf16)

    def values_of(b, size):
        return pre_ref[pl.ds(b * rows + HALO, size), pl.ds(head, head)]

    memories, normals, nearby = [], [], []
    for b in range(2):
        share = cols[b][:, 2:3]
        keys = k_s[pl.ds(b * tokens, tokens), :]
        values = values_of(b, tokens).astype(f32)
        memories.append(
            lax.dot_general(
                (values * share).astype(bf16), keys, (((0,), (0,)), ((), ())),
                preferred_element_type=f32,
            )
        )
        normals.append(jnp.sum(keys.astype(f32) * share, axis=0, keepdims=True))
        st_own[b] = memories[b].astype(bf16)
        low_own[b] = jnp.concatenate(
            [
                normals[b],
                jnp.broadcast_to(tops[b], (1, head)),
                jnp.broadcast_to(finals[b], (1, head)),
                jnp.zeros((5, head), f32),
            ],
            axis=0,
        )
        nearby.append([
            remote(st_own.at[b], st_near.at[b], near_send.at[b, 0], near_recv.at[b, 0], beside),
            remote(low_own.at[b], low_near.at[b], near_send.at[b, 1], near_recv.at[b, 1], beside),
        ])
        for copy in nearby[b]:
            begin(copy)

    sequence = [here] + nears + [partner_plane] + fars
    for i, plane in enumerate(sequence):
        both_arrived("q", plane)
        add_product("q", plane, i == 0, i == len(sequence) - 1)
    for plane in nears:
        forward("wo", plane)

    for copies in nearby:
        for copy in copies:
            copy.wait_recv()
    near_tops = [low_near[b, 1:2, :1] for b in range(2)]
    near_finals = [low_near[b, 2:3, :1] for b in range(2)]
    nothing = jnp.full((1, 1), big_negative, f32)
    first, second = x == 0, x == 1

    def gathered(terms):
        ceiling = functools.reduce(jnp.maximum, [log for log, _, _ in terms])
        memory = jnp.zeros((head, head), f32)
        normal = jnp.zeros((1, head), f32)
        for log, block, line in terms:
            factor = jnp.exp(log - ceiling)
            memory = memory + factor * block().astype(f32)
            normal = normal + factor * line()
        return memory, normal, ceiling

    def near_block(b):
        return lambda: st_near[b]

    def near_line(b):
        return lambda: low_near[b, 0:1, :]

    def own_block(b):
        return lambda: memories[b]

    def own_line(b):
        return lambda: normals[b]

    zero = jnp.zeros((1, 1), f32)
    far_copies = []
    if quads > 1:
        after_near = [
            jnp.where(first, finals[1] + near_finals[1], finals[0] + near_finals[1] + finals[1]),
            jnp.where(first, zero, finals[1]),
        ]
        after_own = [
            jnp.where(first, near_finals[0] + finals[1] + near_finals[1],
                      near_finals[1] + finals[1]),
            jnp.where(first, near_finals[1], zero),
        ]
        quad_memory, quad_normal, quad_top = gathered(
            [(tops[b] + after_own[b], own_block(b), own_line(b)) for b in range(2)]
            + [(near_tops[b] + after_near[b], near_block(b), near_line(b)) for b in range(2)]
        )
        st_quad[...] = quad_memory.astype(bf16)
        low_quad[...] = jnp.concatenate(
            [
                quad_normal,
                jnp.broadcast_to(quad_top, (1, head)),
                jnp.broadcast_to(
                    finals[0] + finals[1] + near_finals[0] + near_finals[1], (1, head)
                ),
                jnp.zeros((5, head), f32),
            ],
            axis=0,
        )
        for d in range(1, quads):
            to = device(2 * lax.rem(q + d, quads) + l, x, y, side)
            copies = [
                remote(st_quad, st_far.at[d - 1], far_send.at[d - 1, 0], far_recv.at[d - 1, 0], to),
                remote(
                    low_quad, low_far.at[d - 1], far_send.at[d - 1, 1], far_recv.at[d - 1, 1], to
                ),
            ]
            far_copies.append(copies)
            for copy in copies:
                pl.when(q + d < quads)(copy.start)

            @pl.when(q < d)
            def _():
                st_far[d - 1] = jnp.zeros(st_far.shape[1:], bf16)
                low_far[d - 1] = jnp.zeros(low_far.shape[1:], f32)

    for b, active in enumerate(convolved(conv_query_ref, 2 * head)):
        q_s[pl.ds(b * tokens, tokens), :] = (active * head ** (-0.5)).astype(bf16)

    block = 128 if tokens % 128 == 0 else tokens
    for b in range(2):
        for t in range(0, tokens, block):
            reach = t + block
            scores = lax.dot_general(
                q_s[pl.ds(b * tokens + t, block), :], k_s[pl.ds(b * tokens, reach), :],
                (((1,), (1,)), ((), ())), preferred_element_type=f32,
            )
            weight = jnp.exp(
                jnp.minimum(gaps[b][:, :reach] - cols[b][t : t + block, 1:2], 0.0)
            )
            t_ids = t + lax.broadcasted_iota(jnp.int32, (block, reach), 0)
            s_ids = lax.broadcasted_iota(jnp.int32, (block, reach), 1)
            scores = jnp.where(t_ids >= s_ids, scores * weight, 0.0).astype(bf16)
            num_s[pl.ds(b * tokens + t, block), :] = jnp.dot(
                scores, values_of(b, reach), preferred_element_type=f32,
            )
            small_s[pl.ds(b * tokens + t, block), :] = jnp.broadcast_to(
                jnp.sum(scores.astype(f32), axis=1, keepdims=True), (block, 128)
            )

    forward("wo", partner_plane)
    for i, plane in enumerate(sequence):
        both_arrived("op", plane)
        add_product("op", plane, i == 0, i == len(sequence) - 1)
    for plane in fars:
        forward("wo", plane)

    level = (tp * 2 + l) % LEVELS
    ext_p[...] = pre_ref[:, 4 * head :].astype(f32)
    for b in range(2):
        base = b * rows + HALO
        window = None
        for step in range(LEVELS):
            low, high = (0, 2) if step == 0 else (2**step, 2 ** (step + 1))
            part = ext_p[pl.ds(base - low, tokens), :]
            for lag in range(low + 1, high):
                part = part + ext_p[pl.ds(base - lag, tokens), :]
            if window is None:
                window = part
            else:
                window = window + jnp.where(level >= step, part, 0.0)
        reach = lax.shift_left(jnp.int32(2), level.astype(jnp.int32))
        row_ids = (4 * q + 2 * b + x) * tokens + lax.broadcasted_iota(
            jnp.int32, (tokens, group), 0
        )
        counted = jnp.minimum(row_ids + 1, reach).astype(f32)
        pooled = (window / counted - ext_p[pl.ds(base, tokens), :]).astype(bf16)
        mix_s[pl.ds(b * tokens, tokens), head:] = (
            jnp.dot(pooled, group_ref[l], preferred_element_type=f32)
            * pool_gain_ref[:, own_group]
        ).astype(bf16)

    later = jnp.zeros((1, 1), f32)
    if quads > 1:
        logs = []
        for d in range(1, quads):
            for copy in far_copies[d - 1]:
                pl.when(q >= d)(copy.wait_recv)
            logs.append(jnp.where(q >= d, low_far[d - 1, 1:2, :1] + later, big_negative))
            later = later + low_far[d - 1, 2:3, :1]
        quad_ceiling = functools.reduce(jnp.maximum, logs)
        memory_in = jnp.zeros((head, head), f32)
        normal_in = jnp.zeros((1, head), f32)
        for d in range(1, quads):
            factor = jnp.where(q >= d, jnp.exp(logs[d - 1] - quad_ceiling), 0.0)
            memory_in = memory_in + factor * st_far[d - 1].astype(f32)
            normal_in = normal_in + factor * low_far[d - 1, 0:1, :]
    else:
        quad_ceiling = nothing
        memory_in = jnp.zeros((head, head), f32)
        normal_in = jnp.zeros((1, head), f32)
    come = (lambda: memory_in), (lambda: normal_in)
    entering = [
        gathered([
            (quad_ceiling + jnp.where(first, zero, near_finals[0]),) + come,
            (jnp.where(first, nothing, near_tops[0]), near_block(0), near_line(0)),
        ]),
        gathered([
            (quad_ceiling + finals[0] + near_finals[0] + jnp.where(first, zero, near_finals[1]),)
            + come,
            (tops[0] + jnp.where(first, near_finals[0], near_finals[1]),
             own_block(0), own_line(0)),
            (near_tops[0] + jnp.where(first, zero, finals[0] + near_finals[1]),
             near_block(0), near_line(0)),
            (jnp.where(first, nothing, near_tops[1]), near_block(1), near_line(1)),
        ]),
    ]
    for b in range(2):
        memory, normal, ceiling_in = entering[b]
        high = memory.astype(bf16)
        low = (memory - high.astype(f32)).astype(bf16)
        there = pl.ds(b * tokens, tokens)
        queries = q_s[there, :]
        over = (((1,), (1,)), ((), ()))
        far = lax.dot_general(queries, high, over, preferred_element_type=f32)
        far = far + lax.dot_general(queries, low, over, preferred_element_type=f32)
        far_sum = jnp.sum(queries.astype(f32) * normal, axis=1, keepdims=True)
        cum, near_top = cols[b][:, 0:1], cols[b][:, 1:2]
        near_log, far_log = cum + near_top, cum + ceiling_in
        ceiling = jnp.maximum(near_log, far_log)
        near_scale, far_scale = jnp.exp(near_log - ceiling), jnp.exp(far_log - ceiling)
        numerator = near_scale * num_s[there, :] + far_scale * far
        denominator = near_scale * small_s[there, :1] + far_scale * far_sum
        hidden = numerator / jnp.maximum(jnp.abs(denominator), jnp.exp(-ceiling))
        hidden = hidden * lax.rsqrt(jnp.mean(hidden * hidden, axis=1, keepdims=True) + epsilon)
        gate = jax.nn.sigmoid(
            pre_ref[pl.ds(b * rows + HALO, tokens), pl.ds(3 * head, head)].astype(f32)
        )
        mix_s[there, :head] = (hidden * gain_ref[:, own_head] * gate).astype(bf16)

    def product(block, y_, side_, place):
        start = pl.multiple_of(block * tokens + (2 * y_ + side_) * height, height)
        return jnp.dot(
            mix_s[pl.ds(start, height), :],
            wo_all[:, pl.ds(pl.multiple_of(place * columns, columns), columns)],
            preferred_element_type=f32,
        )

    chunks = []
    for plane in [here, partner_plane] + nears + fars:
        chunks += [(plane, 2 * plane + x), (plane, 2 * plane + 1 - x)]

    def sibling_part(place):
        return remote(give.at[place], got.at[place], c_send.at[place], c_recv.at[place], sibling)

    def across_part(place):
        return remote(
            give_y.at[place], got_y.at[place], y_send.at[place], y_recv.at[place], across
        )

    def partner_part(place):
        return remote(
            give_z.at[place], got_z.at[place], t_send.at[place], t_recv.at[place], partner
        )

    def stage_a(i):
        plane, place = chunks[i]
        if i % 2 == 1:
            arrived("wo", place)
        for s in range(2):
            for r in range(2):
                give[place, pl.ds((2 * s + r) * height, height), :] = product(
                    s, r, 1 - side, place
                ).astype(bf16)
        begin(sibling_part(place))

    def stage_b(i):
        plane, place = chunks[i]
        theirs, ours = [], []
        for s in range(2):
            theirs.append(product(s, 1 - y, side, place))
            ours.append(product(s, y, side, place))
        sibling_part(place).wait_recv()

        def from_sibling(s, r):
            start = pl.multiple_of((2 * s + r) * height, height)
            return got[place, pl.ds(start, height), :].astype(f32)

        for s in range(2):
            give_y[place, pl.ds(s * height, height), :] = (
                theirs[s] + from_sibling(s, 1 - y)
            ).astype(bf16)
        begin(across_part(place))
        for s in range(2):
            total[place, pl.ds(s * height, height), :] = ours[s] + from_sibling(s, y)

    def stage_c(i):
        plane, place = chunks[i]
        across_part(place).wait_recv()
        away = pl.ds(pl.multiple_of((1 - l) * height, height), height)
        give_z[place] = (total[place, away, :] + got_y[place, away, :].astype(f32)).astype(bf16)
        begin(partner_part(place))

    def stage_d(i):
        plane, place = chunks[i]
        partner_part(place).wait_recv()
        stay = pl.ds(pl.multiple_of(l * height, height), height)
        out_ref[:, pl.ds(pl.multiple_of(place * columns, columns), columns)] = (
            total[place, stay, :] + got_y[place, stay, :].astype(f32)
            + got_z[place].astype(f32)
        ).astype(out_ref.dtype)

    count = len(chunks)
    for i in range(count + 5):
        if i < count:
            stage_a(i)
        if 0 <= i - 1 < count:
            stage_b(i - 1)
        if 0 <= i - 3 < count:
            stage_c(i - 3)
        if 0 <= i - 5 < count:
            stage_d(i - 5)

    for copy in started:
        copy.wait_send()
    pl.when(sp < n_sp - 1)(halo.wait_send)
    for d, copies in enumerate(far_copies):
        for copy in copies:
            pl.when(q + d + 1 < quads)(copy.wait_send)


def mixed_quads(
    inputs, norm_gain, query_weight, key_weight, value_weight, outgate_weight, inputgate_weight,
    forget_weight, forget_bias, conv_query, conv_key, cell_gain, pool_weight, group_weight,
    pool_gain, cell_out_weight, pool_out_weight,
):
    n_sp, n_tp = lax.axis_size("sp"), lax.axis_size("tp")
    quads = n_sp // 4
    f32, bf16 = jnp.float32, jnp.bfloat16
    vmem = pl.BlockSpec(memory_space=pltpu.VMEM)
    anywhere = pl.BlockSpec(memory_space=pl.ANY)
    scalars = pl.BlockSpec(memory_space=pltpu.SMEM)
    dma = pltpu.SemaphoreType.DMA
    head, group = query_weight.shape[1] // 2, pool_weight.shape[1] // 2
    tokens = inputs.shape[0]
    rows = tokens + HALO
    features, height = inputs.shape[1] * n_tp, tokens // n_tp
    columns = cell_out_weight.shape[1]
    width = columns * n_sp
    wide = 4 * head + group
    scratch = [
        ((2, rows, features), bf16),
        ((HALO, features), bf16),
        ((features, wide), bf16),
        ((head + group, width), bf16),
        ((128, features), bf16),
        ((2 * rows, features), bf16),
        ((2 * rows, 128), f32),
        ((2 * tokens, 128), f32),
        ((2 * rows, wide), f32),
        ((2 * rows, wide), bf16),
        ((rows, head), f32),
        ((2 * rows, group), f32),
        ((2 * tokens, head), bf16),
        ((2 * tokens, head), bf16),
        ((2 * tokens, head), f32),
        ((2 * tokens, 128), f32),
        ((2 * tokens, head + group), bf16),
        ((2, head, head), bf16),
        ((2, 8, head), f32),
        ((2, head, head), bf16),
        ((2, 8, head), f32),
        ((head, head), bf16),
        ((8, head), f32),
        ((max(quads - 1, 1), head, head), bf16),
        ((max(quads - 1, 1), 8, head), f32),
        ((n_sp, 4 * height, columns), bf16),
        ((n_sp, 4 * height, columns), bf16),
        ((n_sp, 2 * height, columns), bf16),
        ((n_sp, 2 * height, columns), bf16),
        ((n_sp, height, columns), bf16),
        ((n_sp, height, columns), bf16),
        ((n_sp, 2 * height, columns), f32),
    ]
    far = (max(quads - 1, 1), 2)
    sems = [
        (9,), (2,), (3,), (3,), (3,), (3,), (2, 3), (2, 3), (4, 3), (4, 3),
        (2 * quads, 7), (2 * quads, 7), (n_sp, 7), (2, 2), (2, 2), far, far,
        (n_sp,), (n_sp,), (n_sp,), (n_sp,), (n_sp,), (n_sp,),
    ]
    return pl.pallas_call(
        functools.partial(quad_kernel, quads, tokens, head, group),
        out_shape=jax.ShapeDtypeStruct((height, width), bf16),
        in_specs=[anywhere] * 8 + [vmem] * 3 + [scalars] + [vmem] * 5,
        out_specs=vmem,
        scratch_shapes=[pltpu.VMEM(shape, kind) for shape, kind in scratch]
        + [dma(shape) for shape in sems],
        compiler_params=pltpu.CompilerParams(
            collective_id=0, has_side_effects=True, vmem_limit_bytes=63 * 2**20
        ),
    )(
        inputs, key_weight, value_weight, query_weight, outgate_weight, pool_weight,
        cell_out_weight, pool_out_weight, norm_gain[None], inputgate_weight.T, forget_weight.T,
        forget_bias, conv_query, conv_key, cell_gain[None], group_weight, pool_gain[None],
    )


def local(
    inputs,
    norm_gain,
    query_weight,
    key_weight,
    value_weight,
    outgate_weight,
    inputgate_weight,
    forget_weight,
    forget_bias,
    conv_query,
    conv_key,
    cell_gain,
    pool_weight,
    group_weight,
    pool_gain,
    cell_out_weight,
    pool_out_weight,
):
    narrow = query_weight.shape[0] % 128 or cell_out_weight.shape[1] % 128
    if not narrow and inputs.shape[0] % 32 == 0 and lax.axis_size("tp") == 4:
        return mixed_quads(
            inputs, norm_gain, query_weight, key_weight, value_weight, outgate_weight,
            inputgate_weight, forget_weight, forget_bias, conv_query, conv_key, cell_gain,
            pool_weight, group_weight, pool_gain, cell_out_weight, pool_out_weight,
        )
    f32, bf16 = jnp.float32, jnp.bfloat16
    sp_index, tp_index = lax.axis_index("sp"), lax.axis_index("tp")
    n_sp = lax.axis_size("sp")
    pairs = n_sp // 2
    pair, half = sp_index // 2, sp_index % 2
    tokens_here = inputs.shape[0]
    span = 2 * tokens_here
    local_heads = forget_bias.shape[0]
    head = query_weight.shape[1] // 2
    group = pool_weight.shape[1] // 2

    def halves(array, axis):
        return jnp.split(array, 2, axis=axis)

    ingredients = [
        halves(w, 1)
        for w in (query_weight, key_weight, value_weight, outgate_weight, pool_weight)
    ]
    packed = jnp.stack([jnp.concatenate([w[j] for w in ingredients], axis=1) for j in range(2)])
    cell_halves, pool_halves = halves(cell_out_weight, 0), halves(pool_out_weight, 0)
    packed_out = jnp.stack(
        [jnp.concatenate([cell_halves[j], pool_halves[j]], axis=0) for j in range(2)]
    )
    gain_rows = jnp.broadcast_to(norm_gain[None, :], (16, norm_gain.shape[0]))
    rows_in = jnp.concatenate([inputs, gain_rows], axis=0)
    head_index = tp_index * local_heads + half
    gate_cols = jnp.concatenate(
        [
            lax.dynamic_slice_in_dim(inputgate_weight, head_index, 1, 1),
            lax.dynamic_slice_in_dim(forget_weight, head_index, 1, 1),
        ],
        axis=1,
    )
    gate_weight = jnp.pad(gate_cols, ((0, 0), (0, 126)))
    sequence_log = math.log(tokens_here * n_sp)
    bias = jnp.broadcast_to(forget_bias[half] + sequence_log, (1, 128))

    def own(array, axis, width):
        return lax.dynamic_slice_in_dim(array, half * width, width, axis)

    taps = jnp.concatenate([own(conv_query, 1, head), own(conv_key, 1, head)], axis=1)
    own_group = lax.dynamic_index_in_dim(group_weight, half, 0, keepdims=False)
    return mixed_rows(
        rows_in,
        packed,
        packed_out,
        gate_weight,
        bias,
        taps,
        own(cell_gain, 0, head)[None],
        own_group,
        own(pool_gain, 0, group)[None],
    )


def solution(mesh):
    in_specs = (
        P("sp", "tp"),
        P("tp"),
        P("sp", "tp"),
        P("sp", "tp"),
        P("sp", "tp"),
        P("sp", "tp"),
        P(),
        P(),
        P("tp"),
        P(None, "tp"),
        P(None, "tp"),
        P("tp"),
        P("sp", "tp"),
        P("tp", None, None),
        P("tp"),
        P("tp", "sp"),
        P("tp", "sp"),
    )
    out_specs = P(("sp", "tp"), None)
    return jax.shard_map(local, mesh=mesh, in_specs=in_specs, out_specs=out_specs, check_vma=False)
```

```python
import functools
import math

import jax
import jax.numpy as jnp
from jax import lax
from jax.experimental import pallas as pl
from jax.experimental.pallas import tpu as pltpu
from jax.sharding import PartitionSpec as P

LEVELS = 4

epsilon = 1e-06
big_negative = -1e30
highest = lax.Precision.HIGHEST
MESH = pl.DeviceIdType.MESH


def remote(src, dst, send, recv, device):
    return pltpu.make_async_remote_copy(
        src_ref=src, dst_ref=dst, send_sem=send, recv_sem=recv,
        device_id=device, device_id_type=MESH,
    )


def columns_of(rows):
    filled = jnp.concatenate(
        rows + [jnp.zeros((128 - len(rows), rows[0].shape[1]), jnp.float32)], axis=0
    )
    return filled.T


def scanned(row, combine, fill):
    length = row.shape[1]
    lane = lax.broadcasted_iota(jnp.int32, (8, length), 1)
    value = jnp.broadcast_to(row, (8, length))
    step = 1
    while step < length:
        moved = pltpu.roll(value, step, 1)
        value = combine(value, jnp.where(lane >= step, moved, fill))
        step *= 2
    return value[:1]


def mixer_kernel(
    pairs, tall, tokens, head, group,
    x_ref, wp_ref, wo_ref, gatew_ref, bias_ref, taps_ref, gain_ref, group_ref, pool_gain_ref,
    out_ref,
    x_out, wp_out, wo_out, normed, inv_s, raw_gate, acc, pre_ref, w_ref,
    edge_q, edge_p, ext, ext_p, q_s, k_s, num_s, small_s, mix_s, st, st_low, st_in, low_in,
    give, got, total,
    local_sem, x_send, x_recv, s_send, s_recv, h_send, h_recv, r_send, r_recv,
    edge_sem, state_send, state_recv, send, recv, d_send, d_recv,
):
    f32, bf16 = jnp.float32, jnp.bfloat16
    height = out_ref.shape[0]
    span = 2 * tokens
    length = tokens
    features = x_out.shape[2]
    sp, tp = lax.axis_index("sp"), lax.axis_index("tp")
    pair, half = sp // 2, sp % 2
    row, side = tp // 2, tp % 2
    width = x_ref.shape[1]
    other = 2 * pair + 1 - half
    sibling = (sp, 2 * row + 1 - side)
    right = (2 * lax.rem(pair + 1, pairs) + half, tp)
    left = (2 * lax.rem(pair + pairs - 1, pairs) + half, tp)
    offsets = [(a, b) for a in range(2) for b in range(tall) if (a, b) != (0, 0)]
    peers = [
        (2 * pair + lax.rem(half + a, 2), 2 * lax.rem(row + b, tall) + side) for a, b in offsets
    ]

    places = [(a, b) for a in range(2) for b in range(tall)][::-1]
    count = len(places)

    def target(a, b):
        return (lax.rem(half + a, 2), lax.rem(row + b, tall))

    barrier = pltpu.get_barrier_semaphore()
    greeted = [sibling]
    for a, b in places[:-1]:
        h, r = target(a, b)
        greeted.append((2 * pair + h, 2 * r + side))
    for d in range(1, pairs):
        greeted.append((2 * lax.rem(pair + d, pairs) + half, tp))
    for device in greeted:
        pl.semaphore_signal(barrier, inc=1, device_id=device, device_id_type=MESH)
    pl.semaphore_wait(barrier, len(greeted))

    def x_block(h, r, s):
        column = pl.multiple_of((2 * r + s) * width, width)
        return x_out.at[h, :, pl.ds(column, width)]

    def ring_copies(k, direction, item):
        if direction == 0:
            source = lax.rem(pair - k + 1 + pairs, pairs)
        else:
            source = lax.rem(pair + k - 1, pairs)
        place = 2 * source + (half if item == 0 else 1 - half)
        target = right if direction == 0 else left
        own = k == 1 and item == 0
        index = ((k - 1) * 2 + direction) * 2 + item
        out = []
        for j, (whole, mine) in enumerate(((wp_out, wp_ref), (wo_out, wo_ref))):
            src = mine.at[half] if own else whole.at[place]
            out.append(
                remote(src, whole.at[place], r_send.at[index, j], r_recv.at[index, j], target)
            )
        return out

    steps = pairs // 2

    def has(k, direction, item):
        return k < steps or (k == steps and direction == item)

    swap = [
        remote(wp_ref.at[1 - half], wp_out.at[sp], h_send.at[0], h_recv.at[0], (other, tp)),
        remote(wo_ref.at[1 - half], wo_out.at[sp], h_send.at[1], h_recv.at[1], (other, tp)),
    ]
    for copy in swap:
        copy.start()
    rings = {}
    for direction in range(2):
        if has(1, direction, 0):
            rings[1, direction, 0] = ring_copies(1, direction, 0)
            for copy in rings[1, direction, 0]:
                copy.start()
    spread = []
    for i, device in enumerate(peers):
        copy = remote(x_ref, x_block(half, row, side), x_send.at[i], x_recv.at[i], device)
        copy.start()
        spread.append(copy)
    locals_ = [
        pltpu.make_async_copy(x_ref, x_block(half, row, side), local_sem.at[0]),
        pltpu.make_async_copy(wp_ref.at[half], wp_out.at[sp], local_sem.at[1]),
        pltpu.make_async_copy(wo_ref.at[half], wo_out.at[sp], local_sem.at[2]),
    ]
    for copy in locals_:
        copy.start()
    passed = [remote(x_ref, x_block(half, row, side), s_send.at[0], s_recv.at[0], sibling)]
    passed[0].start()

    acc[...] = jnp.zeros_like(acc)
    for copy in swap:
        copy.wait_recv()
    for direction in range(2):
        if has(1, direction, 1):
            rings[1, direction, 1] = ring_copies(1, direction, 1)
            for copy in rings[1, direction, 1]:
                copy.start()

    def advance(k):
        for item in range(2):
            for direction in range(2):
                if has(k, direction, item):
                    for copy in rings[k - 1, direction, item]:
                        copy.wait_recv()
                    rings[k, direction, item] = ring_copies(k, direction, item)
                    for copy in rings[k, direction, item]:
                        copy.start()
                elif has(k - 1, direction, item):
                    for copy in rings[k - 1, direction, item]:
                        copy.wait_recv()
            if k == 2 and item == 0:
                pass_on()

    def pass_on():
        for i, (a, b) in enumerate(offsets):
            spread[i].wait_recv()
            block = x_block(lax.rem(half + 2 - a, 2), lax.rem(row + tall - b, tall), side)
            copy = remote(block, block, s_send.at[i + 1], s_recv.at[i + 1], sibling)
            copy.start()
            passed.append(copy)

    for k in range(2, steps + 1):
        advance(k)
    if steps < 2:
        pass_on()
    for copy in passed:
        copy.wait_recv()
    for copy in locals_:
        copy.wait()

    whole_gain = x_out[0, tokens : tokens + 1, :].astype(f32)
    small_rows = 128 if tokens % 128 == 0 else tokens
    for h in range(2):
        @pl.loop(0, tokens // small_rows)
        def _(i):
            start = pl.multiple_of(i * small_rows, small_rows)
            wide = x_out[h, pl.ds(start, small_rows), :].astype(f32)
            squares = jnp.sum(wide * wide, axis=1, keepdims=True)
            there = pl.ds(h * tokens + start, small_rows)
            normed[there, :] = (wide * whole_gain).astype(bf16)
            inverse = lax.rsqrt(squares / features + epsilon)
            inv_s[there, :] = jnp.broadcast_to(inverse, (small_rows, 128))

    big_rows = 256 if span % 256 == 0 else span
    depth = wp_ref.shape[1]
    by_item = depth % 128 == 0

    def add_product(place):
        if by_item:
            @pl.loop(0, span // big_rows)
            def _(i):
                there = pl.ds(pl.multiple_of(i * big_rows, big_rows), big_rows)
                across = pl.ds(pl.multiple_of(place * depth, depth), depth)
                acc[there, :] += jnp.dot(
                    normed[there, across], wp_out[place], preferred_element_type=f32
                )

    @pl.loop(0, span // big_rows)
    def _(i):
        there = pl.ds(pl.multiple_of(i * big_rows, big_rows), big_rows)
        raw_gate[there, :] = inv_s[there, :] * jnp.dot(
            normed[there, :], gatew_ref[...], preferred_element_type=f32
        )

    def arrived_place(k, direction, item):
        source = lax.rem(pair - k + pairs, pairs) if direction == 0 else lax.rem(pair + k, pairs)
        return 2 * source + (half if item == 0 else 1 - half)

    add_product(sp)
    add_product(other)
    for k in range(1, steps):
        for direction in range(2):
            for item in range(2):
                add_product(arrived_place(k, direction, item))
    for direction in range(2):
        for item in range(2):
            if has(steps, direction, item):
                for copy in rings[steps, direction, item][:1]:
                    copy.wait_recv()
                add_product(arrived_place(steps, direction, item))

    @pl.loop(0, span // big_rows)
    def _(i):
        there = pl.ds(pl.multiple_of(i * big_rows, big_rows), big_rows)
        if by_item:
            product_here = acc[there, :]
        else:
            weights = wp_out[...].reshape(-1, wp_out.shape[2])
            product_here = jnp.dot(normed[there, :], weights, preferred_element_type=f32)
        pre_ref[there, :] = (product_here * inv_s[there, :1]).astype(bf16)

    gate_t = raw_gate[...].T
    keep = gate_t[1:2, :] + bias_ref[:, :1]
    small = jnp.exp(-jnp.abs(keep))
    ratio = small / (2.0 + small)
    square = ratio * ratio
    series = jnp.full_like(square, 1.0 / 17.0)
    for odd in (15, 13, 11, 9, 7, 5, 3, 1):
        series = series * square + 1.0 / odd
    log_keep_row = jnp.minimum(keep, 0.0) - 2.0 * ratio * series
    log_in_row = gate_t[0:1, :]

    following = (2 * lax.rem(pair + 1, pairs) + half, tp)
    edges = [
        remote(pre_ref.at[pl.ds(span - 16, 16), pl.ds(0, 2 * head)], edge_q,
               edge_sem.at[0], edge_sem.at[1], following),
        remote(pre_ref.at[pl.ds(span - 16, 16), pl.ds(4 * head, group)], edge_p,
               edge_sem.at[2], edge_sem.at[3], following),
    ]

    @pl.when(pair < pairs - 1)
    def _():
        for copy in edges:
            copy.start()

    @pl.when(pair == 0)
    def _():
        edge_q[...] = jnp.zeros_like(edge_q)
        edge_p[...] = jnp.zeros_like(edge_p)

    ext[pl.ds(16, span), :] = pre_ref[:, : 2 * head].astype(f32)
    ext_p[pl.ds(16, span), :] = pre_ref[:, 4 * head :].astype(f32)

    finals, tops, leads, gaps, cols = [], [], [], [], []
    for c in range(2):
        log_in = log_in_row[:, c * length : (c + 1) * length]
        cumulative = scanned(log_keep_row[:, c * length : (c + 1) * length], jnp.add, 0.0)
        gap = log_in - cumulative
        ceiling = scanned(gap, jnp.maximum, big_negative)
        final = cumulative[:, length - 1 :]
        top = final + ceiling[:, length - 1 :]
        share = jnp.exp(final + gap - top)
        finals.append(final)
        tops.append(top)
        gaps.append(gap)
        cols.append(columns_of([cumulative, ceiling, share]))

    @pl.when(pair > 0)
    def _():
        for copy in edges:
            copy.wait_recv()

    ext[pl.ds(0, 16), :] = edge_q[...].astype(f32)
    ext_p[pl.ds(0, 16), :] = edge_p[...].astype(f32)

    taps = taps_ref.shape[0]
    for c in range(2):
        running = None
        for j in range(taps):
            term = taps_ref[pl.ds(j, 1), :] * ext[pl.ds(16 + c * length - taps + 1 + j, length), :]
            running = term if running is None else running + term
        active = running * jax.nn.sigmoid(running)
        q_s[pl.ds(c * length, length), :] = (active[:, :head] * head ** (-0.5)).astype(bf16)
        k_s[pl.ds(c * length, length), :] = active[:, head:].astype(bf16)

    memories, normals = [], []
    for c in range(2):
        share = cols[c][:, 2:3]
        keys = k_s[pl.ds(c * length, length), :]
        values = pre_ref[pl.ds(c * length, length), pl.ds(2 * head, head)].astype(f32)
        memories.append(
            lax.dot_general(
                (values * share).astype(bf16), keys, (((0,), (0,)), ((), ())),
                preferred_element_type=f32,
            )
        )
        normals.append(jnp.sum(keys.astype(f32) * share, axis=0, keepdims=True))
    both = jnp.maximum(finals[1] + tops[0], tops[1])
    first, second = jnp.exp(finals[1] + tops[0] - both), jnp.exp(tops[1] - both)
    st[...] = (first * memories[0] + second * memories[1]).astype(bf16)
    st_low[...] = jnp.concatenate(
        [
            first * normals[0] + second * normals[1],
            jnp.broadcast_to(both, (1, head)),
            jnp.broadcast_to(finals[0] + finals[1], (1, head)),
            jnp.zeros((5, head), f32),
        ],
        axis=0,
    )
    states = []
    for d in range(1, pairs):
        to = (2 * lax.rem(pair + d, pairs) + half, tp)
        copies = [
            remote(st, st_in.at[d - 1], state_send.at[d - 1, 0], state_recv.at[d - 1, 0], to),
            remote(
                st_low, low_in.at[d - 1], state_send.at[d - 1, 1], state_recv.at[d - 1, 1], to
            ),
        ]
        states.append(copies)
        for copy in copies:
            pl.when(pair + d < pairs)(copy.start)

        @pl.when(pair < d)
        def _():
            st_in[d - 1] = jnp.zeros(st_in.shape[1:], bf16)
            low_in[d - 1] = jnp.zeros(low_in.shape[1:], f32)

    block = 128 if length % 128 == 0 else length
    for c in range(2):
        for t in range(0, length, block):
            reach = t + block
            scores = lax.dot_general(
                q_s[pl.ds(c * length + t, block), :], k_s[pl.ds(c * length, reach), :],
                (((1,), (1,)), ((), ())), preferred_element_type=f32,
            )
            weight = jnp.exp(
                jnp.minimum(gaps[c][:, :reach] - cols[c][t : t + block, 1:2], 0.0)
            )
            t_ids = t + lax.broadcasted_iota(jnp.int32, (block, reach), 0)
            s_ids = lax.broadcasted_iota(jnp.int32, (block, reach), 1)
            scores = jnp.where(t_ids >= s_ids, scores * weight, 0.0).astype(bf16)
            num_s[pl.ds(c * length + t, block), :] = jnp.dot(
                scores, pre_ref[pl.ds(c * length, reach), pl.ds(2 * head, head)],
                preferred_element_type=f32,
            )
            small_s[pl.ds(c * length + t, block), :] = jnp.broadcast_to(
                jnp.sum(scores.astype(f32), axis=1, keepdims=True), (block, 128)
            )

    level = (tp * 2 + half) % LEVELS
    window = None
    for step in range(LEVELS):
        low, high = (0, 2) if step == 0 else (2**step, 2 ** (step + 1))
        part = ext_p[pl.ds(16 - low, span), :]
        for lag in range(low + 1, high):
            part = part + ext_p[pl.ds(16 - lag, span), :]
        if window is None:
            window = part
        else:
            window = window + jnp.where(level >= step, part, 0.0)
    reach = lax.shift_left(jnp.int32(2), level.astype(jnp.int32))
    row_ids = pair * span + lax.broadcasted_iota(jnp.int32, (span, group), 0)
    counted = jnp.minimum(row_ids + 1, reach).astype(f32)
    pooled = (window / counted - ext_p[pl.ds(16, span), :]).astype(bf16)
    mix_s[:, head:] = (
        jnp.dot(pooled, group_ref[...], preferred_element_type=f32) * pool_gain_ref[...]
    ).astype(bf16)

    later = jnp.zeros((1, 1), f32)
    logs = []
    for d in range(1, pairs):
        for copy in states[d - 1]:
            pl.when(pair >= d)(copy.wait_recv)
        logs.append(jnp.where(pair >= d, low_in[d - 1, 1:2, :1] + later, big_negative))
        later = later + low_in[d - 1, 2:3, :1]
    ceiling_in = functools.reduce(jnp.maximum, logs)
    memory_in = jnp.zeros((head, head), f32)
    normal_in = jnp.zeros((1, head), f32)
    for d in range(1, pairs):
        factor = jnp.where(pair >= d, jnp.exp(logs[d - 1] - ceiling_in), 0.0)
        memory_in = memory_in + factor * st_in[d - 1].astype(f32)
        normal_in = normal_in + factor * low_in[d - 1, 0:1, :]
    for c in range(2):
        high = memory_in.astype(bf16)
        low = (memory_in - high.astype(f32)).astype(bf16)
        here = pl.ds(c * length, length)
        queries = q_s[here, :]
        over = (((1,), (1,)), ((), ()))
        far = lax.dot_general(queries, high, over, preferred_element_type=f32)
        far = far + lax.dot_general(queries, low, over, preferred_element_type=f32)
        far_sum = jnp.sum(queries.astype(f32) * normal_in, axis=1, keepdims=True)
        cum, near_top = cols[c][:, 0:1], cols[c][:, 1:2]
        near_log, far_log = cum + near_top, cum + ceiling_in
        ceiling = jnp.maximum(near_log, far_log)
        near_scale, far_scale = jnp.exp(near_log - ceiling), jnp.exp(far_log - ceiling)
        numerator = near_scale * num_s[here, :] + far_scale * far
        denominator = near_scale * small_s[here, :1] + far_scale * far_sum
        hidden = numerator / jnp.maximum(jnp.abs(denominator), jnp.exp(-ceiling))
        hidden = hidden * lax.rsqrt(jnp.mean(hidden * hidden, axis=1, keepdims=True) + epsilon)
        gate = jax.nn.sigmoid(pre_ref[here, pl.ds(3 * head, head)].astype(f32))
        mix_s[here, :head] = (hidden * gain_ref[...] * gate).astype(bf16)
        if c == 0:
            upper = jnp.maximum(finals[0] + ceiling_in, tops[0])
            kept, added = jnp.exp(finals[0] + ceiling_in - upper), jnp.exp(tops[0] - upper)
            memory_in = kept * memory_in + added * memories[0]
            normal_in = kept * normal_in + added * normals[0]
            ceiling_in = upper

    for direction in range(2):
        for item in range(2):
            if has(steps, direction, item):
                for copy in rings[steps, direction, item][1:]:
                    copy.wait_recv()
    columns = wo_out.shape[2]
    for s in range(wo_out.shape[0]):
        w_ref[:, s * columns : (s + 1) * columns] = wo_out[s]

    def product(a, b, s):
        h, r = target(a, b)
        start = pl.multiple_of(((h * tall + r) * 2 + s) * height, height)
        return jnp.dot(
            mix_s[pl.ds(start, height), :], w_ref[...], preferred_element_type=f32
        )

    crossed = []
    for i, (a, b) in enumerate(places):
        give[i] = product(a, b, 1 - side).astype(give.dtype)
        copy = remote(give.at[i], got.at[i], d_send.at[i], d_recv.at[i], sibling)
        copy.start()
        crossed.append(copy)
    sent = []
    for i, (a, b) in enumerate(places):
        mine = product(a, b, side)
        crossed[i].wait_recv()
        mine = mine + got[i].astype(f32)
        if i < count - 1:
            h, r = target(a, b)
            give[count + i] = mine.astype(give.dtype)
            copy = remote(
                give.at[count + i], got.at[count + i], send.at[i], recv.at[i],
                (2 * pair + h, 2 * r + side),
            )
            copy.start()
            sent.append(copy)
        else:
            total[...] = mine
    for i, copy in enumerate(sent):
        copy.wait_recv()
        total[...] += got[count + i].astype(f32)
    out_ref[...] = total[...].astype(out_ref.dtype)
    for copy in crossed + sent:
        copy.wait_send()
    for d in range(1, pairs):
        for copy in states[d - 1]:
            pl.when(pair + d < pairs)(copy.wait_send)

    @pl.when(pair < pairs - 1)
    def _():
        for copy in edges:
            copy.wait_send()

    for copy in swap + spread + passed + [c for copies in rings.values() for c in copies]:
        copy.wait_send()


def mixed_rows(rows_in, packed, packed_out, gate_weight, bias, taps, gain, own_group, pool_gain):
    pairs, n_tp = lax.axis_size("sp") // 2, lax.axis_size("tp")
    tall = n_tp // 2
    f32, bf16 = jnp.float32, jnp.bfloat16
    vmem = pl.BlockSpec(memory_space=pltpu.VMEM)
    dma = pltpu.SemaphoreType.DMA
    slots, steps = 4 * tall - 1, pairs // 2
    head, group = gain.shape[1], pool_gain.shape[1]
    tokens = rows_in.shape[0] - 16
    span, features, height = 2 * tokens, rows_in.shape[1] * n_tp, tokens // n_tp
    width = packed_out.shape[2] * 2 * pairs
    scratch = [
        ((2, rows_in.shape[0], features), bf16),
        ((2 * pairs,) + packed.shape[1:], bf16),
        ((2 * pairs,) + packed_out.shape[1:], bf16),
        ((span, features), bf16),
        ((span, 128), f32),
        ((span, 128), f32),
        ((span, packed.shape[2]), f32),
        ((span, packed.shape[2]), bf16),
        ((head + group, width), bf16),
        ((16, 2 * head), bf16),
        ((16, group), bf16),
        ((span + 16, 2 * head), f32),
        ((span + 16, group), f32),
        ((span, head), bf16),
        ((span, head), bf16),
        ((span, head), f32),
        ((span, 128), f32),
        ((span, head + group), bf16),
        ((head, head), bf16),
        ((8, head), f32),
        ((pairs - 1, head, head), bf16),
        ((pairs - 1, 8, head), f32),
        ((slots, height, width), bf16),
        ((slots, height, width), bf16),
        ((height, width), f32),
    ]
    return pl.pallas_call(
        functools.partial(mixer_kernel, pairs, tall, tokens, head, group),
        out_shape=jax.ShapeDtypeStruct((height, width), bf16),
        in_specs=[vmem] * 9,
        out_specs=vmem,
        scratch_shapes=[pltpu.VMEM(shape, kind) for shape, kind in scratch] + [
            dma((3,)),
            dma((2 * tall,)), dma((2 * tall,)),
            dma((2 * tall,)), dma((2 * tall,)),
            dma((2,)), dma((2,)),
            dma((steps * 4, 2)), dma((steps * 4, 2)),
            dma((4,)), dma((pairs - 1, 2)), dma((pairs - 1, 2)),
            dma((2 * tall,)), dma((2 * tall,)), dma((2 * tall,)), dma((2 * tall,)),
        ],
        compiler_params=pltpu.CompilerParams(
            collective_id=0, has_side_effects=True, vmem_limit_bytes=63 * 2**20
        ),
    )(rows_in, packed, packed_out, gate_weight, bias, taps, gain, own_group, pool_gain)


HALO = 16


def quad_kernel(
    quads, tokens, head, group,
    x_ref, key_ref, value_ref, query_ref, outgate_ref, pool_ref, cell_out_ref, pool_out_ref,
    norm_ref, in_ref, keep_ref, bias_ref, conv_query_ref, conv_key_ref, gain_ref, group_ref,
    pool_gain_ref,
    out_ref,
    x_all, gain_all, w_all, wo_all, gatew, normed, inv_s, raw_gate, acc, pre_ref, ext, ext_p,
    q_s, k_s, num_s, small_s, mix_s, st_own, low_own, st_near, low_near, st_quad, low_quad,
    st_far, low_far, give, got, give_y, got_y, give_z, got_z, total,
    local_sem, halo_sem, gain_send, gain_recv, xz_send, xz_recv, xy_send, xy_recv,
    xs_send, xs_recv, z_send, x_send, w_recv, near_send, near_recv, far_send, far_recv,
    c_send, c_recv, y_send, y_recv, t_send, t_recv,
):
    f32, bf16 = jnp.float32, jnp.bfloat16
    height = out_ref.shape[0]
    rows = tokens + HALO
    span = 2 * rows
    width = x_ref.shape[1]
    features = x_all.shape[2]
    depth, columns = key_ref.shape[0], cell_out_ref.shape[1]
    sp, tp = lax.axis_index("sp"), lax.axis_index("tp")
    q, l, x = sp // 4, (sp // 2) % 2, sp % 2
    y, side = tp // 2, tp % 2
    here = 2 * q + l
    n_sp = 4 * quads

    def device(plane, x_, y_, side_):
        return (2 * plane + x_, 2 * y_ + side_)

    partner_plane = 2 * q + 1 - l
    beside = device(here, 1 - x, y, side)
    partner = device(partner_plane, x, y, side)
    across = device(here, x, 1 - y, side)
    sibling = device(here, x, y, 1 - side)
    nears, fars = [], []
    for e in range(1, quads):
        other = lax.rem(q + e, quads)
        behind = (other < q).astype(jnp.int32)
        nears.append(2 * other + behind)
        fars.append(2 * other + 1 - behind)
    following = lax.rem(sp + 1, n_sp)
    crowd = [(0, 1), (1, 0), (1, 1)]

    def mate(a, b):
        return (sp, 2 * lax.rem(y + a, 2) + lax.rem(side + b, 2))

    barrier = pltpu.get_barrier_semaphore()
    def flipped(place):
        return place + 2 - 4 * lax.rem(place // 2, 2)

    greeted = [beside, partner, (following, tp), (lax.rem(sp + n_sp - 1, n_sp), tp)]
    greeted += [(flipped(following), tp), (lax.rem(flipped(sp) + n_sp - 1, n_sp), tp)]
    greeted += [mate(a, b) for a, b in crowd]
    greeted += [device(plane, x, y, side) for plane in nears + fars]
    for to in greeted:
        pl.semaphore_signal(barrier, inc=1, device_id=to, device_id_type=MESH)
    pl.semaphore_wait(barrier, len(greeted))

    started = []

    def begin(copy):
        copy.start()
        started.append(copy)

    own_column = pl.ds(pl.multiple_of(tp * width, width), width)

    def column_of(y_, side_):
        return pl.ds(pl.multiple_of((2 * y_ + side_) * width, width), width)

    pieces = (tokens // 2) // HALO * HALO
    cuts = [(HALO, pieces), (HALO + pieces, tokens - pieces), (0, HALO)]

    def x_place(block, cut, column):
        start, size = cuts[cut]
        return x_all.at[block, pl.ds(start, size), column]

    def x_mine(cut):
        start, size = cuts[cut]
        if cut == 2:
            return x_place(l, cut, own_column)
        return x_ref.at[pl.ds(start - HALO, size), :]

    def partner_copy(cut):
        return remote(
            x_mine(cut), x_place(l, cut, own_column), xz_send.at[cut], xz_recv.at[cut], partner
        )

    def across_copy(which, cut):
        src = x_mine(cut) if which == 0 else x_place(1 - l, cut, own_column)
        block = l if which == 0 else 1 - l
        return remote(
            src, x_place(block, cut, own_column), xy_send.at[which, cut], xy_recv.at[which, cut],
            across,
        )

    def sibling_copy(which, cut):
        block = l if which % 2 == 0 else 1 - l
        place = x_place(block, cut, column_of(y if which < 2 else 1 - y, side))
        src = x_mine(cut) if which == 0 else place
        return remote(src, place, xs_send.at[which, cut], xs_recv.at[which, cut], sibling)

    halos, halos_here = [], []
    for i, to in enumerate((following, flipped(following))):
        halos.append(remote(
            x_ref.at[pl.ds(tokens - HALO, HALO), :],
            x_all.at[lax.rem(following // 2, 2), pl.ds(0, HALO), own_column],
            halo_sem.at[i, 0], halo_sem.at[i, 1], (to, tp),
        ))
        place = x_place(l if i == 0 else 1 - l, 2, own_column)
        halos_here.append(remote(place, place, halo_sem.at[i, 0], halo_sem.at[i, 1], (to, tp)))
    for copy in halos:
        pl.when(sp < n_sp - 1)(copy.start)
    for cut in range(2):
        begin(partner_copy(cut))
        begin(across_copy(0, cut))
        begin(sibling_copy(0, cut))

    weights = [
        (key_ref, 0, head), (value_ref, head, head), (query_ref, 2 * head, head),
        (outgate_ref, 3 * head, head), (pool_ref, 4 * head, group),
        (cell_out_ref, 0, head), (pool_out_ref, head, group),
    ]
    classes = {"kv": (0, 1), "q": (2,), "op": (3, 4), "wo": (5, 6)}

    def weight_source(j, half):
        ref, start, size = weights[j]
        cut = pl.ds(pl.multiple_of(half * size, size), size)
        return ref.at[:, cut] if j < 5 else ref.at[cut, :]

    def weight_place(j, place):
        ref, start, size = weights[j]
        if j < 5:
            return w_all.at[pl.ds(pl.multiple_of(place * depth, depth), depth), pl.ds(start, size)]
        return wo_all.at[pl.ds(start, size), pl.ds(pl.multiple_of(place * columns, columns), columns)]

    def send_weight(name, plane):
        for j in classes[name]:
            begin(remote(
                weight_source(j, lax.rem(plane, 2)), weight_place(j, sp),
                z_send.at[plane, j], w_recv.at[sp, j], device(plane, x, y, side),
            ))

    def arrived(name, place):
        for j in classes[name]:
            there = weight_place(j, place)
            remote(there, there, x_send.at[0, j], w_recv.at[place, j], beside).wait_recv()

    def forward(name, plane):
        place = 2 * plane + x
        arrived(name, place)
        for j in classes[name]:
            there = weight_place(j, place)
            begin(remote(there, there, x_send.at[plane, j], w_recv.at[place, j], beside))

    planes = [partner_plane] + nears + fars
    for name in ("kv", "q", "op", "wo"):
        for j in classes[name]:
            begin(remote(
                weight_source(j, l), weight_place(j, sp), x_send.at[here, j], w_recv.at[sp, j],
                beside,
            ))
        for plane in planes:
            send_weight(name, plane)
    locals_ = [pltpu.make_async_copy(x_mine(c), x_place(l, c, own_column), local_sem.at[7 + c])
               for c in range(2)]
    locals_ += [
        pltpu.make_async_copy(weight_source(j, l), weight_place(j, sp), local_sem.at[j])
        for j in range(7)
    ]
    for copy in locals_:
        copy.start()

    gain_all[:, own_column] = jnp.broadcast_to(norm_ref[...], (HALO, width))
    gains = []
    for i, (a, b) in enumerate(crowd):
        there = gain_all.at[:, own_column]
        copy = remote(there, there, gain_send.at[i], gain_recv.at[i], mate(a, b))
        begin(copy)
        gains.append(copy)
    gatew[...] = jnp.zeros_like(gatew)
    gatew[0:16, :] = jnp.concatenate([in_ref[...], keep_ref[...]], axis=0)

    @pl.when((sp == 0) | (flipped(sp) == 0))
    def _():
        x_all[0, 0:HALO, own_column] = jnp.zeros((HALO, width), bf16)

    for copy, place in zip(halos_here, (sp, flipped(sp))):
        pl.when(place > 0)(copy.wait_recv)
    for which in range(2):
        begin(across_copy(which, 2))
        begin(sibling_copy(which, 2))

    for cut in (2, 0, 1):
        across_copy(0, cut).wait_recv()
        begin(sibling_copy(2, cut))
    for copy in gains:
        copy.wait_recv()
    for copy in locals_:
        copy.wait()
    for which in (0, 2):
        for cut in range(3):
            sibling_copy(which, cut).wait_recv()
    whole_gain = gain_all[0:1, :].astype(f32)

    def strips(size, most, body):
        for start in range(0, size, most):
            body(start, min(most, size - start))

    def normalize(b):
        def body(start, size):
            wide = x_all[b, pl.ds(start, size), :].astype(f32)
            squares = jnp.sum(wide * wide, axis=1, keepdims=True)
            there = pl.ds(pl.multiple_of(b * rows + start, HALO), size)
            normed[there, :] = (wide * whole_gain).astype(bf16)
            inverse = lax.rsqrt(squares / features + epsilon)
            inv_s[there, :] = jnp.broadcast_to(inverse, (size, 128))

        full = rows // 128

        @pl.loop(0, full)
        def _(i):
            body(pl.multiple_of(i * 128, 128), 128)

        if rows % 128:
            body(full * 128, rows % 128)

    def gate_rows(b):
        def body(start, size):
            there = pl.ds(pl.multiple_of(b * rows + HALO + start, HALO), size)
            to = pl.ds(pl.multiple_of(b * tokens + start, HALO), size)
            raw_gate[to, :] = inv_s[there, :] * lax.dot_general(
                normed[there, :], gatew[...], (((1,), (1,)), ((), ())),
                preferred_element_type=f32,
            )

        strips(tokens, 320, body)

    spans = {
        "kv": (0, 2 * head), "q": (2 * head, head), "op": (3 * head, head + group),
        "kvq": (0, 3 * head), "all": (0, 4 * head + group),
    }

    def add_product(name, plane, b, first=False, last=False):
        start, size = spans[name]
        cut = pl.ds(start, size)
        deep = pl.ds(pl.multiple_of(plane * 2 * depth, 2 * depth), 2 * depth)

        def body(row, count):
            there = pl.ds(pl.multiple_of(b * rows + row, HALO), count)
            product = jnp.dot(
                normed[there, deep], w_all[deep, cut], preferred_element_type=f32
            )
            if not first:
                product = product + acc[there, cut]
            if last:
                pre_ref[there, cut] = (product * inv_s[there, :1]).astype(bf16)
            else:
                acc[there, cut] = product

        strips(rows, 256, body)

    def beside_arrived(name, plane):
        arrived(name, 2 * plane + 1 - x)

    normalize(l)

    def relay(cut):
        partner_copy(cut).wait_recv()
        begin(across_copy(1, cut))
        begin(sibling_copy(1, cut))

    relay(0)
    gate_rows(l)
    for name in ("kv", "q", "op"):
        beside_arrived(name, here)
    relay(1)
    for plane in nears:
        forward("kv", plane)
    add_product("all", here, l, first=True)
    for cut in (2, 0, 1):
        across_copy(1, cut).wait_recv()
        begin(sibling_copy(3, cut))
    for plane in nears:
        forward("q", plane)
    for which in (1, 3):
        for cut in range(3):
            sibling_copy(which, cut).wait_recv()
    normalize(1 - l)
    gate_rows(1 - l)
    add_product("all", here, 1 - l, first=True)
    forward("kv", partner_plane)
    for plane in nears:
        beside_arrived("kv", plane)
        beside_arrived("q", plane)
        for b in range(2):
            add_product("kvq", plane, b)
    gate_t = raw_gate[...].T
    which_row = lax.broadcasted_iota(jnp.int32, (8, 2 * tokens), 0) == tp * 2 + l
    log_in_row = jnp.sum(jnp.where(which_row, gate_t[0:8, :], 0.0), axis=0, keepdims=True)
    keep = jnp.sum(jnp.where(which_row, gate_t[8:16, :], 0.0), axis=0, keepdims=True)
    keep = keep + (bias_ref[l] + math.log(tokens * n_sp))
    small = jnp.exp(-jnp.abs(keep))
    ratio = small / (2.0 + small)
    square = ratio * ratio
    series = jnp.full_like(square, 1.0 / 17.0)
    for odd in (15, 13, 11, 9, 7, 5, 3, 1):
        series = series * square + 1.0 / odd
    log_keep_row = jnp.minimum(keep, 0.0) - 2.0 * ratio * series

    finals, tops, gaps, cols = [], [], [], []
    for b in range(2):
        log_in = log_in_row[:, b * tokens : (b + 1) * tokens]
        cumulative = scanned(log_keep_row[:, b * tokens : (b + 1) * tokens], jnp.add, 0.0)
        gap = log_in - cumulative
        ceiling = scanned(gap, jnp.maximum, big_negative)
        final = cumulative[:, tokens - 1 :]
        top = final + ceiling[:, tokens - 1 :]
        share = jnp.exp(final + gap - top)
        finals.append(final)
        tops.append(top)
        gaps.append(gap)
        cols.append(columns_of([cumulative, ceiling, share]))

    for plane in nears:
        forward("op", plane)
    forward("q", partner_plane)
    beside_arrived("kv", partner_plane)
    for b in range(2):
        add_product("kv", partner_plane, b, last=quads == 1)
    for plane in fars:
        forward("kv", plane)
    forward("op", partner_plane)
    for i, plane in enumerate(fars):
        beside_arrived("kv", plane)
        for b in range(2):
            add_product("kv", plane, b, last=i == len(fars) - 1)

    taps = conv_key_ref.shape[0]
    own_head = pl.ds(pl.multiple_of(l * head, head), head)
    own_group = pl.ds(pl.multiple_of(l * group, group), group)

    def convolved(conv_ref, start):
        out = []
        for b in range(2):
            ext[...] = pre_ref[pl.ds(b * rows, rows), pl.ds(start, head)].astype(f32)
            running = None
            for j in range(taps):
                term = conv_ref[pl.ds(j, 1), own_head] * ext[pl.ds(HALO - taps + 1 + j, tokens), :]
                running = term if running is None else running + term
            out.append(running * jax.nn.sigmoid(running))
        return out

    for b, active in enumerate(convolved(conv_key_ref, 0)):
        k_s[pl.ds(b * tokens, tokens), :] = active.astype(bf16)

    def values_of(b, size):
        return pre_ref[pl.ds(b * rows + HALO, size), pl.ds(head, head)]

    memories, normals, nearby = [], [], []
    for b in range(2):
        share = cols[b][:, 2:3]
        keys = k_s[pl.ds(b * tokens, tokens), :]
        values = values_of(b, tokens).astype(f32)
        memories.append(
            lax.dot_general(
                (values * share).astype(bf16), keys, (((0,), (0,)), ((), ())),
                preferred_element_type=f32,
            )
        )
        normals.append(jnp.sum(keys.astype(f32) * share, axis=0, keepdims=True))
        st_own[b] = memories[b].astype(bf16)
        low_own[b] = jnp.concatenate(
            [
                normals[b],
                jnp.broadcast_to(tops[b], (1, head)),
                jnp.broadcast_to(finals[b], (1, head)),
                jnp.zeros((5, head), f32),
            ],
            axis=0,
        )
        nearby.append([
            remote(st_own.at[b], st_near.at[b], near_send.at[b, 0], near_recv.at[b, 0], beside),
            remote(low_own.at[b], low_near.at[b], near_send.at[b, 1], near_recv.at[b, 1], beside),
        ])
        for copy in nearby[b]:
            begin(copy)

    for plane in fars:
        forward("q", plane)
    tail = [partner_plane] + fars
    for i, plane in enumerate(tail):
        beside_arrived("q", plane)
        for b in range(2):
            add_product("q", plane, b, last=i == len(tail) - 1)
    for plane in fars:
        forward("op", plane)
    for b, active in enumerate(convolved(conv_query_ref, 2 * head)):
        q_s[pl.ds(b * tokens, tokens), :] = (active * head ** (-0.5)).astype(bf16)

    block = 128 if tokens % 128 == 0 else tokens
    for b in range(2):
        for t in range(0, tokens, block):
            reach = t + block
            scores = lax.dot_general(
                q_s[pl.ds(b * tokens + t, block), :], k_s[pl.ds(b * tokens, reach), :],
                (((1,), (1,)), ((), ())), preferred_element_type=f32,
            )
            weight = jnp.exp(
                jnp.minimum(gaps[b][:, :reach] - cols[b][t : t + block, 1:2], 0.0)
            )
            t_ids = t + lax.broadcasted_iota(jnp.int32, (block, reach), 0)
            s_ids = lax.broadcasted_iota(jnp.int32, (block, reach), 1)
            scores = jnp.where(t_ids >= s_ids, scores * weight, 0.0).astype(bf16)
            num_s[pl.ds(b * tokens + t, block), :] = jnp.dot(
                scores, values_of(b, reach), preferred_element_type=f32,
            )
            small_s[pl.ds(b * tokens + t, block), :] = jnp.broadcast_to(
                jnp.sum(scores.astype(f32), axis=1, keepdims=True), (block, 128)
            )

    for plane in nears:
        forward("wo", plane)
        beside_arrived("op", plane)
        for b in range(2):
            add_product("op", plane, b)
    beside_arrived("op", partner_plane)
    for b in range(2):
        add_product("op", partner_plane, b, last=quads == 1)
    for copies in nearby:
        for copy in copies:
            copy.wait_recv()
    near_tops = [low_near[b, 1:2, :1] for b in range(2)]
    near_finals = [low_near[b, 2:3, :1] for b in range(2)]
    nothing = jnp.full((1, 1), big_negative, f32)
    first, second = x == 0, x == 1

    def gathered(terms):
        ceiling = functools.reduce(jnp.maximum, [log for log, _, _ in terms])
        memory = jnp.zeros((head, head), f32)
        normal = jnp.zeros((1, head), f32)
        for log, block, line in terms:
            factor = jnp.exp(log - ceiling)
            memory = memory + factor * block().astype(f32)
            normal = normal + factor * line()
        return memory, normal, ceiling

    def near_block(b):
        return lambda: st_near[b]

    def near_line(b):
        return lambda: low_near[b, 0:1, :]

    def own_block(b):
        return lambda: memories[b]

    def own_line(b):
        return lambda: normals[b]

    zero = jnp.zeros((1, 1), f32)
    far_copies = []
    if quads > 1:
        after_near = [
            jnp.where(first, finals[1] + near_finals[1], finals[0] + near_finals[1] + finals[1]),
            jnp.where(first, zero, finals[1]),
        ]
        after_own = [
            jnp.where(first, near_finals[0] + finals[1] + near_finals[1],
                      near_finals[1] + finals[1]),
            jnp.where(first, near_finals[1], zero),
        ]
        quad_memory, quad_normal, quad_top = gathered(
            [(tops[b] + after_own[b], own_block(b), own_line(b)) for b in range(2)]
            + [(near_tops[b] + after_near[b], near_block(b), near_line(b)) for b in range(2)]
        )
        st_quad[...] = quad_memory.astype(bf16)
        low_quad[...] = jnp.concatenate(
            [
                quad_normal,
                jnp.broadcast_to(quad_top, (1, head)),
                jnp.broadcast_to(
                    finals[0] + finals[1] + near_finals[0] + near_finals[1], (1, head)
                ),
                jnp.zeros((5, head), f32),
            ],
            axis=0,
        )
        for d in range(1, quads):
            to = device(2 * lax.rem(q + d, quads) + l, x, y, side)
            copies = [
                remote(st_quad, st_far.at[d - 1], far_send.at[d - 1, 0], far_recv.at[d - 1, 0], to),
                remote(
                    low_quad, low_far.at[d - 1], far_send.at[d - 1, 1], far_recv.at[d - 1, 1], to
                ),
            ]
            far_copies.append(copies)
            for copy in copies:
                pl.when(q + d < quads)(copy.start)

            @pl.when(q < d)
            def _():
                st_far[d - 1] = jnp.zeros(st_far.shape[1:], bf16)
                low_far[d - 1] = jnp.zeros(low_far.shape[1:], f32)

    forward("wo", partner_plane)
    for i, plane in enumerate(fars):
        beside_arrived("op", plane)
        for b in range(2):
            add_product("op", plane, b, last=i == len(fars) - 1)
    for plane in fars:
        forward("wo", plane)
    level = (tp * 2 + l) % LEVELS
    ext_p[...] = pre_ref[:, 4 * head :].astype(f32)
    for b in range(2):
        base = b * rows + HALO
        window = None
        for step in range(LEVELS):
            low, high = (0, 2) if step == 0 else (2**step, 2 ** (step + 1))
            part = ext_p[pl.ds(base - low, tokens), :]
            for lag in range(low + 1, high):
                part = part + ext_p[pl.ds(base - lag, tokens), :]
            if window is None:
                window = part
            else:
                window = window + jnp.where(level >= step, part, 0.0)
        reach = lax.shift_left(jnp.int32(2), level.astype(jnp.int32))
        row_ids = (4 * q + 2 * b + x) * tokens + lax.broadcasted_iota(
            jnp.int32, (tokens, group), 0
        )
        counted = jnp.minimum(row_ids + 1, reach).astype(f32)
        pooled = (window / counted - ext_p[pl.ds(base, tokens), :]).astype(bf16)
        mix_s[pl.ds(b * tokens, tokens), head:] = (
            jnp.dot(pooled, group_ref[l], preferred_element_type=f32)
            * pool_gain_ref[:, own_group]
        ).astype(bf16)

    later = jnp.zeros((1, 1), f32)
    if quads > 1:
        logs = []
        for d in range(1, quads):
            for copy in far_copies[d - 1]:
                pl.when(q >= d)(copy.wait_recv)
            logs.append(jnp.where(q >= d, low_far[d - 1, 1:2, :1] + later, big_negative))
            later = later + low_far[d - 1, 2:3, :1]
        quad_ceiling = functools.reduce(jnp.maximum, logs)
        memory_in = jnp.zeros((head, head), f32)
        normal_in = jnp.zeros((1, head), f32)
        for d in range(1, quads):
            factor = jnp.where(q >= d, jnp.exp(logs[d - 1] - quad_ceiling), 0.0)
            memory_in = memory_in + factor * st_far[d - 1].astype(f32)
            normal_in = normal_in + factor * low_far[d - 1, 0:1, :]
    else:
        quad_ceiling = nothing
        memory_in = jnp.zeros((head, head), f32)
        normal_in = jnp.zeros((1, head), f32)
    come = (lambda: memory_in), (lambda: normal_in)
    entering = [
        gathered([
            (quad_ceiling + jnp.where(first, zero, near_finals[0]),) + come,
            (jnp.where(first, nothing, near_tops[0]), near_block(0), near_line(0)),
        ]),
        gathered([
            (quad_ceiling + finals[0] + near_finals[0] + jnp.where(first, zero, near_finals[1]),)
            + come,
            (tops[0] + jnp.where(first, near_finals[0], near_finals[1]),
             own_block(0), own_line(0)),
            (near_tops[0] + jnp.where(first, zero, finals[0] + near_finals[1]),
             near_block(0), near_line(0)),
            (jnp.where(first, nothing, near_tops[1]), near_block(1), near_line(1)),
        ]),
    ]
    for b in range(2):
        memory, normal, ceiling_in = entering[b]
        high = memory.astype(bf16)
        low = (memory - high.astype(f32)).astype(bf16)
        there = pl.ds(b * tokens, tokens)
        queries = q_s[there, :]
        over = (((1,), (1,)), ((), ()))
        far = lax.dot_general(queries, high, over, preferred_element_type=f32)
        far = far + lax.dot_general(queries, low, over, preferred_element_type=f32)
        far_sum = jnp.sum(queries.astype(f32) * normal, axis=1, keepdims=True)
        cum, near_top = cols[b][:, 0:1], cols[b][:, 1:2]
        near_log, far_log = cum + near_top, cum + ceiling_in
        ceiling = jnp.maximum(near_log, far_log)
        near_scale, far_scale = jnp.exp(near_log - ceiling), jnp.exp(far_log - ceiling)
        numerator = near_scale * num_s[there, :] + far_scale * far
        denominator = near_scale * small_s[there, :1] + far_scale * far_sum
        hidden = numerator / jnp.maximum(jnp.abs(denominator), jnp.exp(-ceiling))
        hidden = hidden * lax.rsqrt(jnp.mean(hidden * hidden, axis=1, keepdims=True) + epsilon)
        gate = jax.nn.sigmoid(
            pre_ref[pl.ds(b * rows + HALO, tokens), pl.ds(3 * head, head)].astype(f32)
        )
        mix_s[there, :head] = (hidden * gain_ref[:, own_head] * gate).astype(bf16)

    def product(block, y_, side_, place):
        start = pl.multiple_of(block * tokens + (2 * y_ + side_) * height, height)
        return jnp.dot(
            mix_s[pl.ds(start, height), :],
            wo_all[:, pl.ds(pl.multiple_of(place * columns, columns), columns)],
            preferred_element_type=f32,
        )

    chunks = []
    for plane in [here, partner_plane] + nears + fars:
        chunks += [(plane, 2 * plane + x), (plane, 2 * plane + 1 - x)]

    def sibling_part(place):
        return remote(give.at[place], got.at[place], c_send.at[place], c_recv.at[place], sibling)

    def first_part(i, place):
        return remote(
            give_y.at[place], got_y.at[place], y_send.at[place], y_recv.at[place],
            partner if i % 2 else across,
        )

    def second_part(i, place):
        return remote(
            give_z.at[place], got_z.at[place], t_send.at[place], t_recv.at[place],
            across if i % 2 else partner,
        )

    def stage_a(i):
        plane, place = chunks[i]
        if i % 2 == 1:
            arrived("wo", place)
        for s in range(2):
            for r in range(2):
                give[place, pl.ds((2 * s + r) * height, height), :] = product(
                    s, r, 1 - side, place
                ).astype(bf16)
        begin(sibling_part(place))

    def stage_b(i):
        plane, place = chunks[i]

        def slot(k, away):
            if i % 2:
                return (1 - l if away else l), k
            return k, (1 - y if away else y)

        away = [product(*slot(k, True), side, place) for k in range(2)]
        stay = [product(*slot(k, False), side, place) for k in range(2)]
        sibling_part(place).wait_recv()

        def from_sibling(s, r):
            start = pl.multiple_of((2 * s + r) * height, height)
            return got[place, pl.ds(start, height), :].astype(f32)

        for k in range(2):
            give_y[place, pl.ds(k * height, height), :] = (
                away[k] + from_sibling(*slot(k, True))
            ).astype(bf16)
        begin(first_part(i, place))
        for k in range(2):
            total[place, pl.ds(k * height, height), :] = stay[k] + from_sibling(*slot(k, False))

    def kept(i, away):
        own = y if i % 2 else l
        return pl.ds(pl.multiple_of((1 - own if away else own) * height, height), height)

    def stage_c(i):
        plane, place = chunks[i]
        first_part(i, place).wait_recv()
        there = kept(i, True)
        give_z[place] = (total[place, there, :] + got_y[place, there, :].astype(f32)).astype(bf16)
        begin(second_part(i, place))

    def stage_d(i):
        plane, place = chunks[i]
        second_part(i, place).wait_recv()
        there = kept(i, False)
        out_ref[:, pl.ds(pl.multiple_of(place * columns, columns), columns)] = (
            total[place, there, :] + got_y[place, there, :].astype(f32)
            + got_z[place].astype(f32)
        ).astype(out_ref.dtype)

    count = len(chunks)
    for i in range(count + 4):
        if i < count:
            stage_a(i)
        if 0 <= i - 1 < count:
            stage_b(i - 1)
        if 0 <= i - 4 < count:
            stage_c(i - 4)
    for i in [2, 3, 0, 1] + list(range(4, count)):
        stage_d(i)
    for copy in started:
        copy.wait_send()
    for copy in halos:
        pl.when(sp < n_sp - 1)(copy.wait_send)
    for d, copies in enumerate(far_copies):
        for copy in copies:
            pl.when(q + d + 1 < quads)(copy.wait_send)


def mixed_quads(
    inputs, norm_gain, query_weight, key_weight, value_weight, outgate_weight, inputgate_weight,
    forget_weight, forget_bias, conv_query, conv_key, cell_gain, pool_weight, group_weight,
    pool_gain, cell_out_weight, pool_out_weight,
):
    n_sp, n_tp = lax.axis_size("sp"), lax.axis_size("tp")
    quads = n_sp // 4
    f32, bf16 = jnp.float32, jnp.bfloat16
    vmem = pl.BlockSpec(memory_space=pltpu.VMEM)
    anywhere = pl.BlockSpec(memory_space=pl.ANY)
    scalars = pl.BlockSpec(memory_space=pltpu.SMEM)
    dma = pltpu.SemaphoreType.DMA
    head, group = query_weight.shape[1] // 2, pool_weight.shape[1] // 2
    tokens = inputs.shape[0]
    rows = tokens + HALO
    features, height = inputs.shape[1] * n_tp, tokens // n_tp
    columns = cell_out_weight.shape[1]
    width = columns * n_sp
    wide = 4 * head + group
    scratch = [
        ((2, rows, features), bf16),
        ((HALO, features), bf16),
        ((features, wide), bf16),
        ((head + group, width), bf16),
        ((128, features), bf16),
        ((2 * rows, features), bf16),
        ((2 * rows, 128), f32),
        ((2 * tokens, 128), f32),
        ((2 * rows, wide), f32),
        ((2 * rows, wide), bf16),
        ((rows, head), f32),
        ((2 * rows, group), f32),
        ((2 * tokens, head), bf16),
        ((2 * tokens, head), bf16),
        ((2 * tokens, head), f32),
        ((2 * tokens, 128), f32),
        ((2 * tokens, head + group), bf16),
        ((2, head, head), bf16),
        ((2, 8, head), f32),
        ((2, head, head), bf16),
        ((2, 8, head), f32),
        ((head, head), bf16),
        ((8, head), f32),
        ((max(quads - 1, 1), head, head), bf16),
        ((max(quads - 1, 1), 8, head), f32),
        ((n_sp, 4 * height, columns), bf16),
        ((n_sp, 4 * height, columns), bf16),
        ((n_sp, 2 * height, columns), bf16),
        ((n_sp, 2 * height, columns), bf16),
        ((n_sp, height, columns), bf16),
        ((n_sp, height, columns), bf16),
        ((n_sp, 2 * height, columns), f32),
    ]
    far = (max(quads - 1, 1), 2)
    sems = [
        (9,), (2, 2), (3,), (3,), (2,), (2,), (2, 3), (2, 3), (4, 3), (4, 3),
        (2 * quads, 7), (2 * quads, 7), (n_sp, 7), (2, 2), (2, 2), far, far,
        (n_sp,), (n_sp,), (n_sp,), (n_sp,), (n_sp,), (n_sp,),
    ]
    return pl.pallas_call(
        functools.partial(quad_kernel, quads, tokens, head, group),
        out_shape=jax.ShapeDtypeStruct((height, width), bf16),
        in_specs=[anywhere] * 8 + [vmem] * 3 + [scalars] + [vmem] * 5,
        out_specs=vmem,
        scratch_shapes=[pltpu.VMEM(shape, kind) for shape, kind in scratch]
        + [dma(shape) for shape in sems],
        compiler_params=pltpu.CompilerParams(
            collective_id=0, has_side_effects=True, vmem_limit_bytes=63 * 2**20
        ),
    )(
        inputs, key_weight, value_weight, query_weight, outgate_weight, pool_weight,
        cell_out_weight, pool_out_weight, norm_gain[None], inputgate_weight.T, forget_weight.T,
        forget_bias, conv_query, conv_key, cell_gain[None], group_weight, pool_gain[None],
    )


def local(
    inputs,
    norm_gain,
    query_weight,
    key_weight,
    value_weight,
    outgate_weight,
    inputgate_weight,
    forget_weight,
    forget_bias,
    conv_query,
    conv_key,
    cell_gain,
    pool_weight,
    group_weight,
    pool_gain,
    cell_out_weight,
    pool_out_weight,
):
    narrow = query_weight.shape[0] % 128 or cell_out_weight.shape[1] % 128
    if not narrow and inputs.shape[0] % 32 == 0 and lax.axis_size("tp") == 4:
        return mixed_quads(
            inputs, norm_gain, query_weight, key_weight, value_weight, outgate_weight,
            inputgate_weight, forget_weight, forget_bias, conv_query, conv_key, cell_gain,
            pool_weight, group_weight, pool_gain, cell_out_weight, pool_out_weight,
        )
    f32, bf16 = jnp.float32, jnp.bfloat16
    sp_index, tp_index = lax.axis_index("sp"), lax.axis_index("tp")
    n_sp = lax.axis_size("sp")
    pairs = n_sp // 2
    pair, half = sp_index // 2, sp_index % 2
    tokens_here = inputs.shape[0]
    span = 2 * tokens_here
    local_heads = forget_bias.shape[0]
    head = query_weight.shape[1] // 2
    group = pool_weight.shape[1] // 2

    def halves(array, axis):
        return jnp.split(array, 2, axis=axis)

    ingredients = [
        halves(w, 1)
        for w in (query_weight, key_weight, value_weight, outgate_weight, pool_weight)
    ]
    packed = jnp.stack([jnp.concatenate([w[j] for w in ingredients], axis=1) for j in range(2)])
    cell_halves, pool_halves = halves(cell_out_weight, 0), halves(pool_out_weight, 0)
    packed_out = jnp.stack(
        [jnp.concatenate([cell_halves[j], pool_halves[j]], axis=0) for j in range(2)]
    )
    gain_rows = jnp.broadcast_to(norm_gain[None, :], (16, norm_gain.shape[0]))
    rows_in = jnp.concatenate([inputs, gain_rows], axis=0)
    head_index = tp_index * local_heads + half
    gate_cols = jnp.concatenate(
        [
            lax.dynamic_slice_in_dim(inputgate_weight, head_index, 1, 1),
            lax.dynamic_slice_in_dim(forget_weight, head_index, 1, 1),
        ],
        axis=1,
    )
    gate_weight = jnp.pad(gate_cols, ((0, 0), (0, 126)))
    sequence_log = math.log(tokens_here * n_sp)
    bias = jnp.broadcast_to(forget_bias[half] + sequence_log, (1, 128))

    def own(array, axis, width):
        return lax.dynamic_slice_in_dim(array, half * width, width, axis)

    taps = jnp.concatenate([own(conv_query, 1, head), own(conv_key, 1, head)], axis=1)
    own_group = lax.dynamic_index_in_dim(group_weight, half, 0, keepdims=False)
    return mixed_rows(
        rows_in,
        packed,
        packed_out,
        gate_weight,
        bias,
        taps,
        own(cell_gain, 0, head)[None],
        own_group,
        own(pool_gain, 0, group)[None],
    )


def solution(mesh):
    in_specs = (
        P("sp", "tp"),
        P("tp"),
        P("sp", "tp"),
        P("sp", "tp"),
        P("sp", "tp"),
        P("sp", "tp"),
        P(),
        P(),
        P("tp"),
        P(None, "tp"),
        P(None, "tp"),
        P("tp"),
        P("sp", "tp"),
        P("tp", None, None),
        P("tp"),
        P("tp", "sp"),
        P("tp", "sp"),
    )
    out_specs = P(("sp", "tp"), None)
    return jax.shard_map(local, mesh=mesh, in_specs=in_specs, out_specs=out_specs, check_vma=False)
```

```python
import functools
import math

import jax
import jax.numpy as jnp
from jax import lax
from jax.experimental import pallas as pl
from jax.experimental.pallas import tpu as pltpu
from jax.sharding import PartitionSpec as P

LEVELS = 4

epsilon = 1e-06
big_negative = -1e30
highest = lax.Precision.HIGHEST
MESH = pl.DeviceIdType.MESH


def remote(src, dst, send, recv, device):
    return pltpu.make_async_remote_copy(
        src_ref=src, dst_ref=dst, send_sem=send, recv_sem=recv,
        device_id=device, device_id_type=MESH,
    )


def columns_of(rows):
    filled = jnp.concatenate(
        rows + [jnp.zeros((128 - len(rows), rows[0].shape[1]), jnp.float32)], axis=0
    )
    return filled.T


def scanned(row, combine, fill):
    length = row.shape[1]
    lane = lax.broadcasted_iota(jnp.int32, (8, length), 1)
    value = jnp.broadcast_to(row, (8, length))
    step = 1
    while step < length:
        moved = pltpu.roll(value, step, 1)
        value = combine(value, jnp.where(lane >= step, moved, fill))
        step *= 2
    return value[:1]


def mixer_kernel(
    pairs, tall, tokens, head, group,
    x_ref, wp_ref, wo_ref, gatew_ref, bias_ref, taps_ref, gain_ref, group_ref, pool_gain_ref,
    out_ref,
    x_out, wp_out, wo_out, normed, inv_s, raw_gate, acc, pre_ref, w_ref,
    edge_q, edge_p, ext, ext_p, q_s, k_s, num_s, small_s, mix_s, st, st_low, st_in, low_in,
    give, got, total,
    local_sem, x_send, x_recv, s_send, s_recv, h_send, h_recv, r_send, r_recv,
    edge_sem, state_send, state_recv, send, recv, d_send, d_recv,
):
    f32, bf16 = jnp.float32, jnp.bfloat16
    height = out_ref.shape[0]
    span = 2 * tokens
    length = tokens
    features = x_out.shape[2]
    sp, tp = lax.axis_index("sp"), lax.axis_index("tp")
    pair, half = sp // 2, sp % 2
    row, side = tp // 2, tp % 2
    width = x_ref.shape[1]
    other = 2 * pair + 1 - half
    sibling = (sp, 2 * row + 1 - side)
    right = (2 * lax.rem(pair + 1, pairs) + half, tp)
    left = (2 * lax.rem(pair + pairs - 1, pairs) + half, tp)
    offsets = [(a, b) for a in range(2) for b in range(tall) if (a, b) != (0, 0)]
    peers = [
        (2 * pair + lax.rem(half + a, 2), 2 * lax.rem(row + b, tall) + side) for a, b in offsets
    ]

    places = [(a, b) for a in range(2) for b in range(tall)][::-1]
    count = len(places)

    def target(a, b):
        return (lax.rem(half + a, 2), lax.rem(row + b, tall))

    barrier = pltpu.get_barrier_semaphore()
    greeted = [sibling]
    for a, b in places[:-1]:
        h, r = target(a, b)
        greeted.append((2 * pair + h, 2 * r + side))
    for d in range(1, pairs):
        greeted.append((2 * lax.rem(pair + d, pairs) + half, tp))
    for device in greeted:
        pl.semaphore_signal(barrier, inc=1, device_id=device, device_id_type=MESH)
    pl.semaphore_wait(barrier, len(greeted))

    def x_block(h, r, s):
        column = pl.multiple_of((2 * r + s) * width, width)
        return x_out.at[h, :, pl.ds(column, width)]

    def ring_copies(k, direction, item):
        if direction == 0:
            source = lax.rem(pair - k + 1 + pairs, pairs)
        else:
            source = lax.rem(pair + k - 1, pairs)
        place = 2 * source + (half if item == 0 else 1 - half)
        target = right if direction == 0 else left
        own = k == 1 and item == 0
        index = ((k - 1) * 2 + direction) * 2 + item
        out = []
        for j, (whole, mine) in enumerate(((wp_out, wp_ref), (wo_out, wo_ref))):
            src = mine.at[half] if own else whole.at[place]
            out.append(
                remote(src, whole.at[place], r_send.at[index, j], r_recv.at[index, j], target)
            )
        return out

    steps = pairs // 2

    def has(k, direction, item):
        return k < steps or (k == steps and direction == item)

    swap = [
        remote(wp_ref.at[1 - half], wp_out.at[sp], h_send.at[0], h_recv.at[0], (other, tp)),
        remote(wo_ref.at[1 - half], wo_out.at[sp], h_send.at[1], h_recv.at[1], (other, tp)),
    ]
    for copy in swap:
        copy.start()
    rings = {}
    for direction in range(2):
        if has(1, direction, 0):
            rings[1, direction, 0] = ring_copies(1, direction, 0)
            for copy in rings[1, direction, 0]:
                copy.start()
    spread = []
    for i, device in enumerate(peers):
        copy = remote(x_ref, x_block(half, row, side), x_send.at[i], x_recv.at[i], device)
        copy.start()
        spread.append(copy)
    locals_ = [
        pltpu.make_async_copy(x_ref, x_block(half, row, side), local_sem.at[0]),
        pltpu.make_async_copy(wp_ref.at[half], wp_out.at[sp], local_sem.at[1]),
        pltpu.make_async_copy(wo_ref.at[half], wo_out.at[sp], local_sem.at[2]),
    ]
    for copy in locals_:
        copy.start()
    passed = [remote(x_ref, x_block(half, row, side), s_send.at[0], s_recv.at[0], sibling)]
    passed[0].start()

    acc[...] = jnp.zeros_like(acc)
    for copy in swap:
        copy.wait_recv()
    for direction in range(2):
        if has(1, direction, 1):
            rings[1, direction, 1] = ring_copies(1, direction, 1)
            for copy in rings[1, direction, 1]:
                copy.start()

    def advance(k):
        for item in range(2):
            for direction in range(2):
                if has(k, direction, item):
                    for copy in rings[k - 1, direction, item]:
                        copy.wait_recv()
                    rings[k, direction, item] = ring_copies(k, direction, item)
                    for copy in rings[k, direction, item]:
                        copy.start()
                elif has(k - 1, direction, item):
                    for copy in rings[k - 1, direction, item]:
                        copy.wait_recv()
            if k == 2 and item == 0:
                pass_on()

    def pass_on():
        for i, (a, b) in enumerate(offsets):
            spread[i].wait_recv()
            block = x_block(lax.rem(half + 2 - a, 2), lax.rem(row + tall - b, tall), side)
            copy = remote(block, block, s_send.at[i + 1], s_recv.at[i + 1], sibling)
            copy.start()
            passed.append(copy)

    for k in range(2, steps + 1):
        advance(k)
    if steps < 2:
        pass_on()
    for copy in passed:
        copy.wait_recv()
    for copy in locals_:
        copy.wait()

    whole_gain = x_out[0, tokens : tokens + 1, :].astype(f32)
    small_rows = 128 if tokens % 128 == 0 else tokens
    for h in range(2):
        @pl.loop(0, tokens // small_rows)
        def _(i):
            start = pl.multiple_of(i * small_rows, small_rows)
            wide = x_out[h, pl.ds(start, small_rows), :].astype(f32)
            squares = jnp.sum(wide * wide, axis=1, keepdims=True)
            there = pl.ds(h * tokens + start, small_rows)
            normed[there, :] = (wide * whole_gain).astype(bf16)
            inverse = lax.rsqrt(squares / features + epsilon)
            inv_s[there, :] = jnp.broadcast_to(inverse, (small_rows, 128))

    big_rows = 256 if span % 256 == 0 else span
    depth = wp_ref.shape[1]
    by_item = depth % 128 == 0

    def add_product(place):
        if by_item:
            @pl.loop(0, span // big_rows)
            def _(i):
                there = pl.ds(pl.multiple_of(i * big_rows, big_rows), big_rows)
                across = pl.ds(pl.multiple_of(place * depth, depth), depth)
                acc[there, :] += jnp.dot(
                    normed[there, across], wp_out[place], preferred_element_type=f32
                )

    @pl.loop(0, span // big_rows)
    def _(i):
        there = pl.ds(pl.multiple_of(i * big_rows, big_rows), big_rows)
        raw_gate[there, :] = inv_s[there, :] * jnp.dot(
            normed[there, :], gatew_ref[...], preferred_element_type=f32
        )

    def arrived_place(k, direction, item):
        source = lax.rem(pair - k + pairs, pairs) if direction == 0 else lax.rem(pair + k, pairs)
        return 2 * source + (half if item == 0 else 1 - half)

    add_product(sp)
    add_product(other)
    for k in range(1, steps):
        for direction in range(2):
            for item in range(2):
                add_product(arrived_place(k, direction, item))
    for direction in range(2):
        for item in range(2):
            if has(steps, direction, item):
                for copy in rings[steps, direction, item][:1]:
                    copy.wait_recv()
                add_product(arrived_place(steps, direction, item))

    @pl.loop(0, span // big_rows)
    def _(i):
        there = pl.ds(pl.multiple_of(i * big_rows, big_rows), big_rows)
        if by_item:
            product_here = acc[there, :]
        else:
            weights = wp_out[...].reshape(-1, wp_out.shape[2])
            product_here = jnp.dot(normed[there, :], weights, preferred_element_type=f32)
        pre_ref[there, :] = (product_here * inv_s[there, :1]).astype(bf16)

    gate_t = raw_gate[...].T
    keep = gate_t[1:2, :] + bias_ref[:, :1]
    small = jnp.exp(-jnp.abs(keep))
    ratio = small / (2.0 + small)
    square = ratio * ratio
    series = jnp.full_like(square, 1.0 / 17.0)
    for odd in (15, 13, 11, 9, 7, 5, 3, 1):
        series = series * square + 1.0 / odd
    log_keep_row = jnp.minimum(keep, 0.0) - 2.0 * ratio * series
    log_in_row = gate_t[0:1, :]

    following = (2 * lax.rem(pair + 1, pairs) + half, tp)
    edges = [
        remote(pre_ref.at[pl.ds(span - 16, 16), pl.ds(0, 2 * head)], edge_q,
               edge_sem.at[0], edge_sem.at[1], following),
        remote(pre_ref.at[pl.ds(span - 16, 16), pl.ds(4 * head, group)], edge_p,
               edge_sem.at[2], edge_sem.at[3], following),
    ]

    @pl.when(pair < pairs - 1)
    def _():
        for copy in edges:
            copy.start()

    @pl.when(pair == 0)
    def _():
        edge_q[...] = jnp.zeros_like(edge_q)
        edge_p[...] = jnp.zeros_like(edge_p)

    ext[pl.ds(16, span), :] = pre_ref[:, : 2 * head].astype(f32)
    ext_p[pl.ds(16, span), :] = pre_ref[:, 4 * head :].astype(f32)

    finals, tops, leads, gaps, cols = [], [], [], [], []
    for c in range(2):
        log_in = log_in_row[:, c * length : (c + 1) * length]
        cumulative = scanned(log_keep_row[:, c * length : (c + 1) * length], jnp.add, 0.0)
        gap = log_in - cumulative
        ceiling = scanned(gap, jnp.maximum, big_negative)
        final = cumulative[:, length - 1 :]
        top = final + ceiling[:, length - 1 :]
        share = jnp.exp(final + gap - top)
        finals.append(final)
        tops.append(top)
        gaps.append(gap)
        cols.append(columns_of([cumulative, ceiling, share]))

    @pl.when(pair > 0)
    def _():
        for copy in edges:
            copy.wait_recv()

    ext[pl.ds(0, 16), :] = edge_q[...].astype(f32)
    ext_p[pl.ds(0, 16), :] = edge_p[...].astype(f32)

    taps = taps_ref.shape[0]
    for c in range(2):
        running = None
        for j in range(taps):
            term = taps_ref[pl.ds(j, 1), :] * ext[pl.ds(16 + c * length - taps + 1 + j, length), :]
            running = term if running is None else running + term
        active = running * jax.nn.sigmoid(running)
        q_s[pl.ds(c * length, length), :] = (active[:, :head] * head ** (-0.5)).astype(bf16)
        k_s[pl.ds(c * length, length), :] = active[:, head:].astype(bf16)

    memories, normals = [], []
    for c in range(2):
        share = cols[c][:, 2:3]
        keys = k_s[pl.ds(c * length, length), :]
        values = pre_ref[pl.ds(c * length, length), pl.ds(2 * head, head)].astype(f32)
        memories.append(
            lax.dot_general(
                (values * share).astype(bf16), keys, (((0,), (0,)), ((), ())),
                preferred_element_type=f32,
            )
        )
        normals.append(jnp.sum(keys.astype(f32) * share, axis=0, keepdims=True))
    both = jnp.maximum(finals[1] + tops[0], tops[1])
    first, second = jnp.exp(finals[1] + tops[0] - both), jnp.exp(tops[1] - both)
    st[...] = (first * memories[0] + second * memories[1]).astype(bf16)
    st_low[...] = jnp.concatenate(
        [
            first * normals[0] + second * normals[1],
            jnp.broadcast_to(both, (1, head)),
            jnp.broadcast_to(finals[0] + finals[1], (1, head)),
            jnp.zeros((5, head), f32),
        ],
        axis=0,
    )
    states = []
    for d in range(1, pairs):
        to = (2 * lax.rem(pair + d, pairs) + half, tp)
        copies = [
            remote(st, st_in.at[d - 1], state_send.at[d - 1, 0], state_recv.at[d - 1, 0], to),
            remote(
                st_low, low_in.at[d - 1], state_send.at[d - 1, 1], state_recv.at[d - 1, 1], to
            ),
        ]
        states.append(copies)
        for copy in copies:
            pl.when(pair + d < pairs)(copy.start)

        @pl.when(pair < d)
        def _():
            st_in[d - 1] = jnp.zeros(st_in.shape[1:], bf16)
            low_in[d - 1] = jnp.zeros(low_in.shape[1:], f32)

    block = 128 if length % 128 == 0 else length
    for c in range(2):
        for t in range(0, length, block):
            reach = t + block
            scores = lax.dot_general(
                q_s[pl.ds(c * length + t, block), :], k_s[pl.ds(c * length, reach), :],
                (((1,), (1,)), ((), ())), preferred_element_type=f32,
            )
            weight = jnp.exp(
                jnp.minimum(gaps[c][:, :reach] - cols[c][t : t + block, 1:2], 0.0)
            )
            t_ids = t + lax.broadcasted_iota(jnp.int32, (block, reach), 0)
            s_ids = lax.broadcasted_iota(jnp.int32, (block, reach), 1)
            scores = jnp.where(t_ids >= s_ids, scores * weight, 0.0).astype(bf16)
            num_s[pl.ds(c * length + t, block), :] = jnp.dot(
                scores, pre_ref[pl.ds(c * length, reach), pl.ds(2 * head, head)],
                preferred_element_type=f32,
            )
            small_s[pl.ds(c * length + t, block), :] = jnp.broadcast_to(
                jnp.sum(scores.astype(f32), axis=1, keepdims=True), (block, 128)
            )

    level = (tp * 2 + half) % LEVELS
    window = None
    for step in range(LEVELS):
        low, high = (0, 2) if step == 0 else (2**step, 2 ** (step + 1))
        part = ext_p[pl.ds(16 - low, span), :]
        for lag in range(low + 1, high):
            part = part + ext_p[pl.ds(16 - lag, span), :]
        if window is None:
            window = part
        else:
            window = window + jnp.where(level >= step, part, 0.0)
    reach = lax.shift_left(jnp.int32(2), level.astype(jnp.int32))
    row_ids = pair * span + lax.broadcasted_iota(jnp.int32, (span, group), 0)
    counted = jnp.minimum(row_ids + 1, reach).astype(f32)
    pooled = (window / counted - ext_p[pl.ds(16, span), :]).astype(bf16)
    mix_s[:, head:] = (
        jnp.dot(pooled, group_ref[...], preferred_element_type=f32) * pool_gain_ref[...]
    ).astype(bf16)

    later = jnp.zeros((1, 1), f32)
    logs = []
    for d in range(1, pairs):
        for copy in states[d - 1]:
            pl.when(pair >= d)(copy.wait_recv)
        logs.append(jnp.where(pair >= d, low_in[d - 1, 1:2, :1] + later, big_negative))
        later = later + low_in[d - 1, 2:3, :1]
    ceiling_in = functools.reduce(jnp.maximum, logs)
    memory_in = jnp.zeros((head, head), f32)
    normal_in = jnp.zeros((1, head), f32)
    for d in range(1, pairs):
        factor = jnp.where(pair >= d, jnp.exp(logs[d - 1] - ceiling_in), 0.0)
        memory_in = memory_in + factor * st_in[d - 1].astype(f32)
        normal_in = normal_in + factor * low_in[d - 1, 0:1, :]
    for c in range(2):
        high = memory_in.astype(bf16)
        low = (memory_in - high.astype(f32)).astype(bf16)
        here = pl.ds(c * length, length)
        queries = q_s[here, :]
        over = (((1,), (1,)), ((), ()))
        far = lax.dot_general(queries, high, over, preferred_element_type=f32)
        far = far + lax.dot_general(queries, low, over, preferred_element_type=f32)
        far_sum = jnp.sum(queries.astype(f32) * normal_in, axis=1, keepdims=True)
        cum, near_top = cols[c][:, 0:1], cols[c][:, 1:2]
        near_log, far_log = cum + near_top, cum + ceiling_in
        ceiling = jnp.maximum(near_log, far_log)
        near_scale, far_scale = jnp.exp(near_log - ceiling), jnp.exp(far_log - ceiling)
        numerator = near_scale * num_s[here, :] + far_scale * far
        denominator = near_scale * small_s[here, :1] + far_scale * far_sum
        hidden = numerator / jnp.maximum(jnp.abs(denominator), jnp.exp(-ceiling))
        hidden = hidden * lax.rsqrt(jnp.mean(hidden * hidden, axis=1, keepdims=True) + epsilon)
        gate = jax.nn.sigmoid(pre_ref[here, pl.ds(3 * head, head)].astype(f32))
        mix_s[here, :head] = (hidden * gain_ref[...] * gate).astype(bf16)
        if c == 0:
            upper = jnp.maximum(finals[0] + ceiling_in, tops[0])
            kept, added = jnp.exp(finals[0] + ceiling_in - upper), jnp.exp(tops[0] - upper)
            memory_in = kept * memory_in + added * memories[0]
            normal_in = kept * normal_in + added * normals[0]
            ceiling_in = upper

    for direction in range(2):
        for item in range(2):
            if has(steps, direction, item):
                for copy in rings[steps, direction, item][1:]:
                    copy.wait_recv()
    columns = wo_out.shape[2]
    for s in range(wo_out.shape[0]):
        w_ref[:, s * columns : (s + 1) * columns] = wo_out[s]

    def product(a, b, s):
        h, r = target(a, b)
        start = pl.multiple_of(((h * tall + r) * 2 + s) * height, height)
        return jnp.dot(
            mix_s[pl.ds(start, height), :], w_ref[...], preferred_element_type=f32
        )

    crossed = []
    for i, (a, b) in enumerate(places):
        give[i] = product(a, b, 1 - side).astype(give.dtype)
        copy = remote(give.at[i], got.at[i], d_send.at[i], d_recv.at[i], sibling)
        copy.start()
        crossed.append(copy)
    sent = []
    for i, (a, b) in enumerate(places):
        mine = product(a, b, side)
        crossed[i].wait_recv()
        mine = mine + got[i].astype(f32)
        if i < count - 1:
            h, r = target(a, b)
            give[count + i] = mine.astype(give.dtype)
            copy = remote(
                give.at[count + i], got.at[count + i], send.at[i], recv.at[i],
                (2 * pair + h, 2 * r + side),
            )
            copy.start()
            sent.append(copy)
        else:
            total[...] = mine
    for i, copy in enumerate(sent):
        copy.wait_recv()
        total[...] += got[count + i].astype(f32)
    out_ref[...] = total[...].astype(out_ref.dtype)
    for copy in crossed + sent:
        copy.wait_send()
    for d in range(1, pairs):
        for copy in states[d - 1]:
            pl.when(pair + d < pairs)(copy.wait_send)

    @pl.when(pair < pairs - 1)
    def _():
        for copy in edges:
            copy.wait_send()

    for copy in swap + spread + passed + [c for copies in rings.values() for c in copies]:
        copy.wait_send()


def mixed_rows(rows_in, packed, packed_out, gate_weight, bias, taps, gain, own_group, pool_gain):
    pairs, n_tp = lax.axis_size("sp") // 2, lax.axis_size("tp")
    tall = n_tp // 2
    f32, bf16 = jnp.float32, jnp.bfloat16
    vmem = pl.BlockSpec(memory_space=pltpu.VMEM)
    dma = pltpu.SemaphoreType.DMA
    slots, steps = 4 * tall - 1, pairs // 2
    head, group = gain.shape[1], pool_gain.shape[1]
    tokens = rows_in.shape[0] - 16
    span, features, height = 2 * tokens, rows_in.shape[1] * n_tp, tokens // n_tp
    width = packed_out.shape[2] * 2 * pairs
    scratch = [
        ((2, rows_in.shape[0], features), bf16),
        ((2 * pairs,) + packed.shape[1:], bf16),
        ((2 * pairs,) + packed_out.shape[1:], bf16),
        ((span, features), bf16),
        ((span, 128), f32),
        ((span, 128), f32),
        ((span, packed.shape[2]), f32),
        ((span, packed.shape[2]), bf16),
        ((head + group, width), bf16),
        ((16, 2 * head), bf16),
        ((16, group), bf16),
        ((span + 16, 2 * head), f32),
        ((span + 16, group), f32),
        ((span, head), bf16),
        ((span, head), bf16),
        ((span, head), f32),
        ((span, 128), f32),
        ((span, head + group), bf16),
        ((head, head), bf16),
        ((8, head), f32),
        ((pairs - 1, head, head), bf16),
        ((pairs - 1, 8, head), f32),
        ((slots, height, width), bf16),
        ((slots, height, width), bf16),
        ((height, width), f32),
    ]
    return pl.pallas_call(
        functools.partial(mixer_kernel, pairs, tall, tokens, head, group),
        out_shape=jax.ShapeDtypeStruct((height, width), bf16),
        in_specs=[vmem] * 9,
        out_specs=vmem,
        scratch_shapes=[pltpu.VMEM(shape, kind) for shape, kind in scratch] + [
            dma((3,)),
            dma((2 * tall,)), dma((2 * tall,)),
            dma((2 * tall,)), dma((2 * tall,)),
            dma((2,)), dma((2,)),
            dma((steps * 4, 2)), dma((steps * 4, 2)),
            dma((4,)), dma((pairs - 1, 2)), dma((pairs - 1, 2)),
            dma((2 * tall,)), dma((2 * tall,)), dma((2 * tall,)), dma((2 * tall,)),
        ],
        compiler_params=pltpu.CompilerParams(
            collective_id=0, has_side_effects=True, vmem_limit_bytes=63 * 2**20
        ),
    )(rows_in, packed, packed_out, gate_weight, bias, taps, gain, own_group, pool_gain)


HALO = 16
ISSUE = ("kv_P", "kv_N", "q_N", "kv_F", "q_F", "q_P", "op_N", "op_P", "op_F")
ISSUE_WO = ("wo_P", "wo_N", "wo_F")


def quad_kernel(
    quads, tokens, head, group,
    x_ref, key_ref, value_ref, query_ref, outgate_ref, pool_ref, cell_out_ref, pool_out_ref,
    norm_ref, in_ref, keep_ref, bias_ref, conv_query_ref, conv_key_ref, gain_ref, group_ref,
    pool_gain_ref,
    out_ref,
    x_all, gain_all, w_all, wo_all, gatew, normed, inv_s, raw_gate, acc, pre_ref, ext, ext_p,
    q_s, k_s, num_s, small_s, mix_s, st_own, low_own, st_near, low_near, st_quad, low_quad,
    st_far, low_far, give, got, give_y, got_y, give_z, got_z, total, out_s,
    local_sem, halo_sem, gain_send, gain_recv, xz_send, xz_recv, xy_send, xy_recv,
    xs_send, xs_recv, z_send, x_send, w_recv, near_send, near_recv, far_send, far_recv,
    c_send, c_recv, y_send, y_recv, t_send, t_recv, out_sem,
):
    f32, bf16 = jnp.float32, jnp.bfloat16
    height = out_ref.shape[0]
    rows = tokens + HALO
    span = 2 * rows
    width = x_ref.shape[1]
    features = x_all.shape[2]
    depth, columns = key_ref.shape[0], cell_out_ref.shape[1]
    sp, tp = lax.axis_index("sp"), lax.axis_index("tp")
    q, l, x = sp // 4, (sp // 2) % 2, sp % 2
    y, side = tp // 2, tp % 2
    here = 2 * q + l
    n_sp = 4 * quads

    def device(plane, x_, y_, side_):
        return (2 * plane + x_, 2 * y_ + side_)

    partner_plane = 2 * q + 1 - l
    beside = device(here, 1 - x, y, side)
    partner = device(partner_plane, x, y, side)
    across = device(here, x, 1 - y, side)
    sibling = device(here, x, y, 1 - side)
    nears, fars = [], []
    for e in range(1, quads):
        other = lax.rem(q + e, quads)
        behind = (other < q).astype(jnp.int32)
        nears.append(2 * other + behind)
        fars.append(2 * other + 1 - behind)
    following = lax.rem(sp + 1, n_sp)
    crowd = [(0, 1), (1, 0), (1, 1)]

    def mate(a, b):
        return (sp, 2 * lax.rem(y + a, 2) + lax.rem(side + b, 2))

    barrier = pltpu.get_barrier_semaphore()
    def flipped(place):
        return place + 2 - 4 * lax.rem(place // 2, 2)

    greeted = [beside, partner, (following, tp), (lax.rem(sp + n_sp - 1, n_sp), tp)]
    greeted += [(flipped(following), tp), (lax.rem(flipped(sp) + n_sp - 1, n_sp), tp)]
    greeted += [mate(a, b) for a, b in crowd]
    greeted += [device(plane, x, y, side) for plane in nears + fars]
    for to in greeted:
        pl.semaphore_signal(barrier, inc=1, device_id=to, device_id_type=MESH)
    pl.semaphore_wait(barrier, len(greeted))

    started = []

    def begin(copy):
        copy.start()
        started.append(copy)

    own_column = pl.ds(pl.multiple_of(tp * width, width), width)

    def column_of(y_, side_):
        return pl.ds(pl.multiple_of((2 * y_ + side_) * width, width), width)

    pieces = (tokens // 2) // HALO * HALO
    cuts = [(HALO, pieces), (HALO + pieces, tokens - pieces), (0, HALO)]

    def x_place(block, cut, column):
        start, size = cuts[cut]
        return x_all.at[block, pl.ds(start, size), column]

    def x_mine(cut):
        start, size = cuts[cut]
        if cut == 2:
            return x_place(l, cut, own_column)
        return x_ref.at[pl.ds(start - HALO, size), :]

    def partner_copy(cut):
        return remote(
            x_mine(cut), x_place(l, cut, own_column), xz_send.at[cut], xz_recv.at[cut], partner
        )

    def across_copy(which, cut):
        src = x_mine(cut) if which == 0 else x_place(1 - l, cut, own_column)
        block = l if which == 0 else 1 - l
        return remote(
            src, x_place(block, cut, own_column), xy_send.at[which, cut], xy_recv.at[which, cut],
            across,
        )

    def sibling_copy(which, cut):
        block = l if which % 2 == 0 else 1 - l
        place = x_place(block, cut, column_of(y if which < 2 else 1 - y, side))
        src = x_mine(cut) if which == 0 else place
        return remote(src, place, xs_send.at[which, cut], xs_recv.at[which, cut], sibling)

    halos, halos_here = [], []
    for i, to in enumerate((following, flipped(following))):
        halos.append(remote(
            x_ref.at[pl.ds(tokens - HALO, HALO), :],
            x_all.at[lax.rem(following // 2, 2), pl.ds(0, HALO), own_column],
            halo_sem.at[i, 0], halo_sem.at[i, 1], (to, tp),
        ))
        place = x_place(l if i == 0 else 1 - l, 2, own_column)
        halos_here.append(remote(place, place, halo_sem.at[i, 0], halo_sem.at[i, 1], (to, tp)))
    for copy in halos:
        pl.when(sp < n_sp - 1)(copy.start)
    for cut in range(2):
        begin(partner_copy(cut))
        begin(across_copy(0, cut))
        begin(sibling_copy(0, cut))

    weights = [
        (key_ref, 0, head), (value_ref, head, head), (query_ref, 2 * head, head),
        (outgate_ref, 3 * head, head), (pool_ref, 4 * head, group),
        (cell_out_ref, 0, head), (pool_out_ref, head, group),
    ]
    classes = {"kv": (0, 1), "q": (2,), "op": (3, 4), "wo": (5, 6)}

    def weight_source(j, half):
        ref, start, size = weights[j]
        cut = pl.ds(pl.multiple_of(half * size, size), size)
        return ref.at[:, cut] if j < 5 else ref.at[cut, :]

    def weight_place(j, place):
        ref, start, size = weights[j]
        if j < 5:
            return w_all.at[pl.ds(pl.multiple_of(place * depth, depth), depth), pl.ds(start, size)]
        return wo_all.at[pl.ds(start, size), pl.ds(pl.multiple_of(place * columns, columns), columns)]

    def send_weight(name, plane):
        for j in classes[name]:
            begin(remote(
                weight_source(j, lax.rem(plane, 2)), weight_place(j, sp),
                z_send.at[plane, j], w_recv.at[sp, j], device(plane, x, y, side),
            ))

    def arrived(name, place):
        for j in classes[name]:
            there = weight_place(j, place)
            remote(there, there, x_send.at[0, j], w_recv.at[place, j], beside).wait_recv()

    def forward(name, plane):
        place = 2 * plane + x
        arrived(name, place)
        for j in classes[name]:
            there = weight_place(j, place)
            begin(remote(there, there, x_send.at[plane, j], w_recv.at[place, j], beside))

    groups = {"P": [partner_plane], "N": nears, "F": fars}

    def send_own(name):
        for j in classes[name]:
            begin(remote(
                weight_source(j, l), weight_place(j, sp), x_send.at[here, j], w_recv.at[sp, j],
                beside,
            ))

    def issue(steps):
        for step in steps:
            name, group_name = step.split("_")
            for plane in groups[group_name]:
                send_weight(name, plane)

    for name in ("kv", "q", "op", "wo"):
        send_own(name)
    issue(ISSUE)
    locals_ = [pltpu.make_async_copy(x_mine(c), x_place(l, c, own_column), local_sem.at[7 + c])
               for c in range(2)]
    locals_ += [
        pltpu.make_async_copy(weight_source(j, l), weight_place(j, sp), local_sem.at[j])
        for j in range(7)
    ]
    for copy in locals_:
        copy.start()

    gain_all[:, own_column] = jnp.broadcast_to(norm_ref[...].reshape(1, width), (HALO, width))
    gains = []
    for i, (a, b) in enumerate(crowd):
        there = gain_all.at[:, own_column]
        copy = remote(there, there, gain_send.at[i], gain_recv.at[i], mate(a, b))
        begin(copy)
        gains.append(copy)
    gatew[...] = jnp.zeros_like(gatew)
    gatew[0:16, :] = jnp.concatenate([in_ref[...], keep_ref[...]], axis=0)

    @pl.when((sp == 0) | (flipped(sp) == 0))
    def _():
        x_all[0, 0:HALO, own_column] = jnp.zeros((HALO, width), bf16)

    for copy, place in zip(halos_here, (sp, flipped(sp))):
        pl.when(place > 0)(copy.wait_recv)
    for which in range(2):
        begin(across_copy(which, 2))
        begin(sibling_copy(which, 2))

    def relay(cut):
        partner_copy(cut).wait_recv()
        begin(across_copy(1, cut))
        begin(sibling_copy(1, cut))

    def from_across(which, cut):
        across_copy(which, cut).wait_recv()
        begin(sibling_copy(2 + which, cut))

    def from_sibling_core(which):
        for block in (which, which + 2):
            for cut in range(3):
                sibling_copy(block, cut).wait_recv()

    def forwards(name, group_name):
        for plane in groups[group_name]:
            forward(name, plane)

    from_across(0, 0)
    relay(0)
    from_across(0, 1)
    from_across(0, 2)
    forwards("kv", "N")
    for copy in gains:
        copy.wait_recv()
    for copy in locals_:
        copy.wait()
    from_sibling_core(0)
    whole_gain = gain_all[0:1, :].astype(f32)

    def strips(size, most, body):
        for start in range(0, size, most):
            body(start, min(most, size - start))

    def normalize(b):
        def body(start, size):
            wide = x_all[b, pl.ds(start, size), :].astype(f32)
            squares = jnp.sum(wide * wide, axis=1, keepdims=True)
            there = pl.ds(pl.multiple_of(b * rows + start, HALO), size)
            normed[there, :] = (wide * whole_gain).astype(bf16)
            inverse = lax.rsqrt(squares / features + epsilon)
            inv_s[there, :] = jnp.broadcast_to(inverse, (size, 128))

        full = rows // 128

        @pl.loop(0, full)
        def _(i):
            body(pl.multiple_of(i * 128, 128), 128)

        if rows % 128:
            body(full * 128, rows % 128)

    def gate_rows(b):
        def body(start, size):
            there = pl.ds(pl.multiple_of(b * rows + HALO + start, HALO), size)
            to = pl.ds(pl.multiple_of(b * tokens + start, HALO), size)
            raw_gate[to, :] = inv_s[there, :] * lax.dot_general(
                normed[there, :], gatew[...], (((1,), (1,)), ((), ())),
                preferred_element_type=f32,
            )

        strips(tokens, 320, body)

    spans = {
        "kv": (0, 2 * head), "q": (2 * head, head), "op": (3 * head, head + group),
        "kvq": (0, 3 * head), "all": (0, 4 * head + group),
    }

    def add_product(name, plane, b, first=False, last=False):
        start, size = spans[name]
        cut = pl.ds(start, size)
        deep = pl.ds(pl.multiple_of(plane * 2 * depth, 2 * depth), 2 * depth)

        def body(row, count):
            there = pl.ds(pl.multiple_of(b * rows + row, HALO), count)
            product = jnp.dot(
                normed[there, deep], w_all[deep, cut], preferred_element_type=f32
            )
            if not first:
                product = product + acc[there, cut]
            if last:
                pre_ref[there, cut] = (product * inv_s[there, :1]).astype(bf16)
            else:
                acc[there, cut] = product

        strips(rows, 256, body)

    def beside_arrived(name, plane):
        arrived(name, 2 * plane + 1 - x)

    normalize(l)
    relay(1)
    gate_rows(l)
    for name in ("kv", "q", "op"):
        beside_arrived(name, here)
    forwards("q", "N")
    add_product("all", here, l, first=True)
    for cut in (2, 0, 1):
        from_across(1, cut)
    forwards("kv", "P")
    from_sibling_core(1)
    normalize(1 - l)
    gate_rows(1 - l)
    add_product("all", here, 1 - l, first=True)
    issue(ISSUE_WO)
    for plane in nears:
        beside_arrived("kv", plane)
        beside_arrived("q", plane)
        for b in range(2):
            add_product("kvq", plane, b)
    gate_t = raw_gate[...].T
    which_row = lax.broadcasted_iota(jnp.int32, (8, 2 * tokens), 0) == tp * 2 + l
    log_in_row = jnp.sum(jnp.where(which_row, gate_t[0:8, :], 0.0), axis=0, keepdims=True)
    keep = jnp.sum(jnp.where(which_row, gate_t[8:16, :], 0.0), axis=0, keepdims=True)
    keep = keep + (bias_ref[l] + math.log(tokens * n_sp))
    small = jnp.exp(-jnp.abs(keep))
    ratio = small / (2.0 + small)
    square = ratio * ratio
    series = jnp.full_like(square, 1.0 / 17.0)
    for odd in (15, 13, 11, 9, 7, 5, 3, 1):
        series = series * square + 1.0 / odd
    log_keep_row = jnp.minimum(keep, 0.0) - 2.0 * ratio * series

    finals, tops, gaps, cols = [], [], [], []
    for b in range(2):
        log_in = log_in_row[:, b * tokens : (b + 1) * tokens]
        cumulative = scanned(log_keep_row[:, b * tokens : (b + 1) * tokens], jnp.add, 0.0)
        gap = log_in - cumulative
        ceiling = scanned(gap, jnp.maximum, big_negative)
        final = cumulative[:, tokens - 1 :]
        top = final + ceiling[:, tokens - 1 :]
        share = jnp.exp(final + gap - top)
        finals.append(final)
        tops.append(top)
        gaps.append(gap)
        cols.append(columns_of([cumulative, ceiling, share]))

    forwards("kv", "F")
    forwards("q", "P")
    for plane in [partner_plane]:
        beside_arrived("kv", plane)
        for b in range(2):
            add_product("kv", plane, b, last=quads == 1)
    forwards("op", "N")
    forwards("q", "F")
    for i, plane in enumerate(fars):
        beside_arrived("kv", plane)
        for b in range(2):
            add_product("kv", plane, b, last=i == len(fars) - 1)

    taps = conv_key_ref.shape[0]
    own_head = pl.ds(pl.multiple_of(l * head, head), head)
    own_group = pl.ds(pl.multiple_of(l * group, group), group)

    def convolved(conv_ref, start):
        out = []
        for b in range(2):
            ext[...] = pre_ref[pl.ds(b * rows, rows), pl.ds(start, head)].astype(f32)
            running = None
            for j in range(taps):
                term = conv_ref[pl.ds(j, 1), own_head] * ext[pl.ds(HALO - taps + 1 + j, tokens), :]
                running = term if running is None else running + term
            out.append(running * jax.nn.sigmoid(running))
        return out

    for b, active in enumerate(convolved(conv_key_ref, 0)):
        k_s[pl.ds(b * tokens, tokens), :] = active.astype(bf16)

    def values_of(b, size):
        return pre_ref[pl.ds(b * rows + HALO, size), pl.ds(head, head)]

    memories, normals, nearby = [], [], []
    for b in range(2):
        share = cols[b][:, 2:3]
        keys = k_s[pl.ds(b * tokens, tokens), :]
        values = values_of(b, tokens).astype(f32)
        memories.append(
            lax.dot_general(
                (values * share).astype(bf16), keys, (((0,), (0,)), ((), ())),
                preferred_element_type=f32,
            )
        )
        normals.append(jnp.sum(keys.astype(f32) * share, axis=0, keepdims=True))
        st_own[b] = memories[b].astype(bf16)
        low_own[b] = jnp.concatenate(
            [
                normals[b],
                jnp.broadcast_to(tops[b], (1, head)),
                jnp.broadcast_to(finals[b], (1, head)),
                jnp.zeros((5, head), f32),
            ],
            axis=0,
        )
        nearby.append([
            remote(st_own.at[b], st_near.at[b], near_send.at[b, 0], near_recv.at[b, 0], beside),
            remote(low_own.at[b], low_near.at[b], near_send.at[b, 1], near_recv.at[b, 1], beside),
        ])
        for copy in nearby[b]:
            begin(copy)

    forwards("op", "P")
    tail = [partner_plane] + fars
    for i, plane in enumerate(tail):
        beside_arrived("q", plane)
        for b in range(2):
            add_product("q", plane, b, last=i == len(tail) - 1)
    forwards("op", "F")
    for b, active in enumerate(convolved(conv_query_ref, 2 * head)):
        q_s[pl.ds(b * tokens, tokens), :] = (active * head ** (-0.5)).astype(bf16)

    block = 128 if tokens % 128 == 0 else tokens
    for b in range(2):
        for t in range(0, tokens, block):
            reach = t + block
            scores = lax.dot_general(
                q_s[pl.ds(b * tokens + t, block), :], k_s[pl.ds(b * tokens, reach), :],
                (((1,), (1,)), ((), ())), preferred_element_type=f32,
            )
            weight = jnp.exp(
                jnp.minimum(gaps[b][:, :reach] - cols[b][t : t + block, 1:2], 0.0)
            )
            t_ids = t + lax.broadcasted_iota(jnp.int32, (block, reach), 0)
            s_ids = lax.broadcasted_iota(jnp.int32, (block, reach), 1)
            scores = jnp.where(t_ids >= s_ids, scores * weight, 0.0).astype(bf16)
            num_s[pl.ds(b * tokens + t, block), :] = jnp.dot(
                scores, values_of(b, reach), preferred_element_type=f32,
            )
            small_s[pl.ds(b * tokens + t, block), :] = jnp.broadcast_to(
                jnp.sum(scores.astype(f32), axis=1, keepdims=True), (block, 128)
            )

    for copies in nearby:
        for copy in copies:
            copy.wait_recv()
    near_tops = [low_near[b, 1:2, :1] for b in range(2)]
    near_finals = [low_near[b, 2:3, :1] for b in range(2)]
    nothing = jnp.full((1, 1), big_negative, f32)
    first, second = x == 0, x == 1

    def gathered(terms):
        ceiling = functools.reduce(jnp.maximum, [log for log, _, _ in terms])
        memory = jnp.zeros((head, head), f32)
        normal = jnp.zeros((1, head), f32)
        for log, block, line in terms:
            factor = jnp.exp(log - ceiling)
            memory = memory + factor * block().astype(f32)
            normal = normal + factor * line()
        return memory, normal, ceiling

    def near_block(b):
        return lambda: st_near[b]

    def near_line(b):
        return lambda: low_near[b, 0:1, :]

    def own_block(b):
        return lambda: memories[b]

    def own_line(b):
        return lambda: normals[b]

    zero = jnp.zeros((1, 1), f32)
    far_copies = []
    if quads > 1:
        after_near = [
            jnp.where(first, finals[1] + near_finals[1], finals[0] + near_finals[1] + finals[1]),
            jnp.where(first, zero, finals[1]),
        ]
        after_own = [
            jnp.where(first, near_finals[0] + finals[1] + near_finals[1],
                      near_finals[1] + finals[1]),
            jnp.where(first, near_finals[1], zero),
        ]
        quad_memory, quad_normal, quad_top = gathered(
            [(tops[b] + after_own[b], own_block(b), own_line(b)) for b in range(2)]
            + [(near_tops[b] + after_near[b], near_block(b), near_line(b)) for b in range(2)]
        )
        st_quad[...] = quad_memory.astype(bf16)
        low_quad[...] = jnp.concatenate(
            [
                quad_normal,
                jnp.broadcast_to(quad_top, (1, head)),
                jnp.broadcast_to(
                    finals[0] + finals[1] + near_finals[0] + near_finals[1], (1, head)
                ),
                jnp.zeros((5, head), f32),
            ],
            axis=0,
        )
        for d in range(1, quads):
            to = device(2 * lax.rem(q + d, quads) + l, x, y, side)
            copies = [
                remote(st_quad, st_far.at[d - 1], far_send.at[d - 1, 0], far_recv.at[d - 1, 0], to),
                remote(
                    low_quad, low_far.at[d - 1], far_send.at[d - 1, 1], far_recv.at[d - 1, 1], to
                ),
            ]
            far_copies.append(copies)
            for copy in copies:
                pl.when(q + d < quads)(copy.start)

            @pl.when(q < d)
            def _():
                st_far[d - 1] = jnp.zeros(st_far.shape[1:], bf16)
                low_far[d - 1] = jnp.zeros(low_far.shape[1:], f32)

    for plane in nears:
        beside_arrived("op", plane)
        for b in range(2):
            add_product("op", plane, b)
    forwards("wo", "P")
    beside_arrived("op", partner_plane)
    for b in range(2):
        add_product("op", partner_plane, b, last=quads == 1)
    def remember():
        later = jnp.zeros((1, 1), f32)
        if quads > 1:
            logs = []
            for d in range(1, quads):
                for copy in far_copies[d - 1]:
                    pl.when(q >= d)(copy.wait_recv)
                logs.append(jnp.where(q >= d, low_far[d - 1, 1:2, :1] + later, big_negative))
                later = later + low_far[d - 1, 2:3, :1]
            quad_ceiling = functools.reduce(jnp.maximum, logs)
            memory_in = jnp.zeros((head, head), f32)
            normal_in = jnp.zeros((1, head), f32)
            for d in range(1, quads):
                factor = jnp.where(q >= d, jnp.exp(logs[d - 1] - quad_ceiling), 0.0)
                memory_in = memory_in + factor * st_far[d - 1].astype(f32)
                normal_in = normal_in + factor * low_far[d - 1, 0:1, :]
        else:
            quad_ceiling = nothing
            memory_in = jnp.zeros((head, head), f32)
            normal_in = jnp.zeros((1, head), f32)
        come = (lambda: memory_in), (lambda: normal_in)
        entering = [
            gathered([
                (quad_ceiling + jnp.where(first, zero, near_finals[0]),) + come,
                (jnp.where(first, nothing, near_tops[0]), near_block(0), near_line(0)),
            ]),
            gathered([
                (quad_ceiling + finals[0] + near_finals[0] + jnp.where(first, zero, near_finals[1]),)
                + come,
                (tops[0] + jnp.where(first, near_finals[0], near_finals[1]),
                 own_block(0), own_line(0)),
                (near_tops[0] + jnp.where(first, zero, finals[0] + near_finals[1]),
                 near_block(0), near_line(0)),
                (jnp.where(first, nothing, near_tops[1]), near_block(1), near_line(1)),
            ]),
        ]
        for b in range(2):
            memory, normal, ceiling_in = entering[b]
            high = memory.astype(bf16)
            low = (memory - high.astype(f32)).astype(bf16)
            there = pl.ds(b * tokens, tokens)
            queries = q_s[there, :]
            over = (((1,), (1,)), ((), ()))
            far = lax.dot_general(queries, high, over, preferred_element_type=f32)
            far = far + lax.dot_general(queries, low, over, preferred_element_type=f32)
            far_sum = jnp.sum(queries.astype(f32) * normal, axis=1, keepdims=True)
            cum, near_top = cols[b][:, 0:1], cols[b][:, 1:2]
            near_log, far_log = cum + near_top, cum + ceiling_in
            ceiling = jnp.maximum(near_log, far_log)
            near_scale, far_scale = jnp.exp(near_log - ceiling), jnp.exp(far_log - ceiling)
            numerator = near_scale * num_s[there, :] + far_scale * far
            denominator = near_scale * small_s[there, :1] + far_scale * far_sum
            hidden = numerator / jnp.maximum(jnp.abs(denominator), jnp.exp(-ceiling))
            hidden = hidden * lax.rsqrt(jnp.mean(hidden * hidden, axis=1, keepdims=True) + epsilon)
            num_s[there, :] = hidden

    pl.when(q == 0)(remember)
    forwards("wo", "F")
    for i, plane in enumerate(fars):
        beside_arrived("op", plane)
        for b in range(2):
            add_product("op", plane, b, last=i == len(fars) - 1)
    level = (tp * 2 + l) % LEVELS
    ext_p[...] = pre_ref[:, 4 * head :].astype(f32)
    for b in range(2):
        base = b * rows + HALO
        window = None
        for step in range(LEVELS):
            low, high = (0, 2) if step == 0 else (2**step, 2 ** (step + 1))
            part = ext_p[pl.ds(base - low, tokens), :]
            for lag in range(low + 1, high):
                part = part + ext_p[pl.ds(base - lag, tokens), :]
            if window is None:
                window = part
            else:
                window = window + jnp.where(level >= step, part, 0.0)
        reach = lax.shift_left(jnp.int32(2), level.astype(jnp.int32))
        row_ids = (4 * q + 2 * b + x) * tokens + lax.broadcasted_iota(
            jnp.int32, (tokens, group), 0
        )
        counted = jnp.minimum(row_ids + 1, reach).astype(f32)
        pooled = (window / counted - ext_p[pl.ds(base, tokens), :]).astype(bf16)
        mix_s[pl.ds(b * tokens, tokens), head:] = (
            jnp.dot(pooled, group_ref[l], preferred_element_type=f32)
            * pool_gain_ref[:, own_group]
        ).astype(bf16)

    forwards("wo", "N")
    pl.when(q > 0)(remember)
    for b in range(2):
        there = pl.ds(b * tokens, tokens)
        gate = jax.nn.sigmoid(
            pre_ref[pl.ds(b * rows + HALO, tokens), pl.ds(3 * head, head)].astype(f32)
        )
        mix_s[there, :head] = (num_s[there, :] * gain_ref[:, own_head] * gate).astype(bf16)

    def product(block, y_, side_, place):
        start = pl.multiple_of(block * tokens + (2 * y_ + side_) * height, height)
        return jnp.dot(
            mix_s[pl.ds(start, height), :],
            wo_all[:, pl.ds(pl.multiple_of(place * columns, columns), columns)],
            preferred_element_type=f32,
        )

    chunks = [(0, 0, here)] + [(0, 1, plane) for plane in nears]
    chunks += [(0, 0, partner_plane)] + [(0, 1, plane) for plane in fars]
    chunks += [(1, 1, here), (1, 1, partner_plane)] + [(1, 0, plane) for plane in fars + nears]
    chunks = [
        (other, turned, 2 * plane + (1 - x if other else x)) for other, turned, plane in chunks
    ]

    def sibling_part(place):
        return remote(give.at[place], got.at[place], c_send.at[place], c_recv.at[place], sibling)

    def first_part(i, place):
        return remote(
            give_y.at[place], got_y.at[place], y_send.at[place], y_recv.at[place],
            partner if chunks[i][1] else across,
        )

    def second_part(i, place):
        return remote(
            give_z.at[place], got_z.at[place], t_send.at[place], t_recv.at[place],
            across if chunks[i][1] else partner,
        )

    def stage_a(i):
        other, turned, place = chunks[i]
        if other:
            arrived("wo", place)
        for s in range(2):
            for r in range(2):
                give[place, pl.ds((2 * s + r) * height, height), :] = product(
                    s, r, 1 - side, place
                ).astype(bf16)
        begin(sibling_part(place))

    def stage_b(i):
        other, turned, place = chunks[i]

        def slot(k, away):
            if turned:
                return (1 - l if away else l), k
            return k, (1 - y if away else y)

        away = [product(*slot(k, True), side, place) for k in range(2)]
        stay = [product(*slot(k, False), side, place) for k in range(2)]
        sibling_part(place).wait_recv()

        def from_sibling(s, r):
            start = pl.multiple_of((2 * s + r) * height, height)
            return got[place, pl.ds(start, height), :].astype(f32)

        for k in range(2):
            give_y[place, pl.ds(k * height, height), :] = (
                away[k] + from_sibling(*slot(k, True))
            ).astype(bf16)
        begin(first_part(i, place))
        for k in range(2):
            total[place, pl.ds(k * height, height), :] = stay[k] + from_sibling(*slot(k, False))

    def kept(i, away):
        own = y if chunks[i][1] else l
        return pl.ds(pl.multiple_of((1 - own if away else own) * height, height), height)

    def stage_c(i):
        other, turned, place = chunks[i]
        first_part(i, place).wait_recv()
        there = kept(i, True)
        give_z[place] = (total[place, there, :] + got_y[place, there, :].astype(f32)).astype(bf16)
        begin(second_part(i, place))

    def stage_d(i):
        other, turned, place = chunks[i]
        second_part(i, place).wait_recv()
        there = kept(i, False)
        out_s[place] = (
            total[place, there, :] + got_y[place, there, :].astype(f32)
            + got_z[place].astype(f32)
        ).astype(out_ref.dtype)
        store = pltpu.make_async_copy(
            out_s.at[place],
            out_ref.at[:, pl.ds(pl.multiple_of(place * columns, columns), columns)],
            out_sem.at[i],
        )
        store.start()
        stores.append(store)

    count = len(chunks)
    stores = []
    for i in range(count + 1):
        if i < count:
            stage_a(i)
        if i > 0:
            stage_b(i - 1)
    for i in range(count):
        stage_c(i)
        if i == 0:
            sent = len(started) - 1
            for copy in started[:sent - 2 * count]:
                copy.wait_send()
            early = sent - 2 * count
    for i in range(count):
        stage_d(i)
    for copy in stores:
        copy.wait()
    for copy in started[early:]:
        copy.wait_send()
    for copy in halos:
        pl.when(sp < n_sp - 1)(copy.wait_send)
    for d, copies in enumerate(far_copies):
        for copy in copies:
            pl.when(q + d + 1 < quads)(copy.wait_send)


def mixed_quads(
    inputs, norm_gain, query_weight, key_weight, value_weight, outgate_weight, inputgate_weight,
    forget_weight, forget_bias, conv_query, conv_key, cell_gain, pool_weight, group_weight,
    pool_gain, cell_out_weight, pool_out_weight,
):
    n_sp, n_tp = lax.axis_size("sp"), lax.axis_size("tp")
    quads = n_sp // 4
    f32, bf16 = jnp.float32, jnp.bfloat16
    vmem = pl.BlockSpec(memory_space=pltpu.VMEM)
    anywhere = pl.BlockSpec(memory_space=pl.ANY)
    scalars = pl.BlockSpec(memory_space=pltpu.SMEM)
    dma = pltpu.SemaphoreType.DMA
    head, group = query_weight.shape[1] // 2, pool_weight.shape[1] // 2
    tokens = inputs.shape[0]
    rows = tokens + HALO
    features, height = inputs.shape[1] * n_tp, tokens // n_tp
    columns = cell_out_weight.shape[1]
    width = columns * n_sp
    wide = 4 * head + group
    scratch = [
        ((2, rows, features), bf16),
        ((HALO, features), bf16),
        ((features, wide), bf16),
        ((head + group, width), bf16),
        ((128, features), bf16),
        ((2 * rows, features), bf16),
        ((2 * rows, 128), f32),
        ((2 * tokens, 128), f32),
        ((2 * rows, wide), f32),
        ((2 * rows, wide), bf16),
        ((rows, head), f32),
        ((2 * rows, group), f32),
        ((2 * tokens, head), bf16),
        ((2 * tokens, head), bf16),
        ((2 * tokens, head), f32),
        ((2 * tokens, 128), f32),
        ((2 * tokens, head + group), bf16),
        ((2, head, head), bf16),
        ((2, 8, head), f32),
        ((2, head, head), bf16),
        ((2, 8, head), f32),
        ((head, head), bf16),
        ((8, head), f32),
        ((max(quads - 1, 1), head, head), bf16),
        ((max(quads - 1, 1), 8, head), f32),
        ((n_sp, 4 * height, columns), bf16),
        ((n_sp, 4 * height, columns), bf16),
        ((n_sp, 2 * height, columns), bf16),
        ((n_sp, 2 * height, columns), bf16),
        ((n_sp, height, columns), bf16),
        ((n_sp, height, columns), bf16),
        ((n_sp, 2 * height, columns), f32),
        ((n_sp, height, columns), bf16),
    ]
    far = (max(quads - 1, 1), 2)
    sems = [
        (9,), (2, 2), (3,), (3,), (2,), (2,), (2, 3), (2, 3), (4, 3), (4, 3),
        (2 * quads, 7), (2 * quads, 7), (n_sp, 7), (2, 2), (2, 2), far, far,
        (n_sp,), (n_sp,), (n_sp,), (n_sp,), (n_sp,), (n_sp,), (n_sp,),
    ]
    return pl.pallas_call(
        functools.partial(quad_kernel, quads, tokens, head, group),
        out_shape=jax.ShapeDtypeStruct((height, width), bf16),
        in_specs=[anywhere] * 8 + [vmem] * 3 + [scalars] + [vmem] * 5,
        out_specs=anywhere,
        scratch_shapes=[pltpu.VMEM(shape, kind) for shape, kind in scratch]
        + [dma(shape) for shape in sems],
        compiler_params=pltpu.CompilerParams(
            collective_id=0, has_side_effects=True, vmem_limit_bytes=63 * 2**20
        ),
    )(
        inputs, key_weight, value_weight, query_weight, outgate_weight, pool_weight,
        cell_out_weight, pool_out_weight, norm_gain, inputgate_weight.T, forget_weight.T,
        forget_bias, conv_query, conv_key, cell_gain[None], group_weight, pool_gain[None],
    )


def local(
    inputs,
    norm_gain,
    query_weight,
    key_weight,
    value_weight,
    outgate_weight,
    inputgate_weight,
    forget_weight,
    forget_bias,
    conv_query,
    conv_key,
    cell_gain,
    pool_weight,
    group_weight,
    pool_gain,
    cell_out_weight,
    pool_out_weight,
):
    narrow = query_weight.shape[0] % 128 or cell_out_weight.shape[1] % 128
    if not narrow and inputs.shape[0] % 32 == 0 and lax.axis_size("tp") == 4:
        return mixed_quads(
            inputs, norm_gain, query_weight, key_weight, value_weight, outgate_weight,
            inputgate_weight, forget_weight, forget_bias, conv_query, conv_key, cell_gain,
            pool_weight, group_weight, pool_gain, cell_out_weight, pool_out_weight,
        )
    f32, bf16 = jnp.float32, jnp.bfloat16
    sp_index, tp_index = lax.axis_index("sp"), lax.axis_index("tp")
    n_sp = lax.axis_size("sp")
    pairs = n_sp // 2
    pair, half = sp_index // 2, sp_index % 2
    tokens_here = inputs.shape[0]
    span = 2 * tokens_here
    local_heads = forget_bias.shape[0]
    head = query_weight.shape[1] // 2
    group = pool_weight.shape[1] // 2

    def halves(array, axis):
        return jnp.split(array, 2, axis=axis)

    ingredients = [
        halves(w, 1)
        for w in (query_weight, key_weight, value_weight, outgate_weight, pool_weight)
    ]
    packed = jnp.stack([jnp.concatenate([w[j] for w in ingredients], axis=1) for j in range(2)])
    cell_halves, pool_halves = halves(cell_out_weight, 0), halves(pool_out_weight, 0)
    packed_out = jnp.stack(
        [jnp.concatenate([cell_halves[j], pool_halves[j]], axis=0) for j in range(2)]
    )
    gain_rows = jnp.broadcast_to(norm_gain[None, :], (16, norm_gain.shape[0]))
    rows_in = jnp.concatenate([inputs, gain_rows], axis=0)
    head_index = tp_index * local_heads + half
    gate_cols = jnp.concatenate(
        [
            lax.dynamic_slice_in_dim(inputgate_weight, head_index, 1, 1),
            lax.dynamic_slice_in_dim(forget_weight, head_index, 1, 1),
        ],
        axis=1,
    )
    gate_weight = jnp.pad(gate_cols, ((0, 0), (0, 126)))
    sequence_log = math.log(tokens_here * n_sp)
    bias = jnp.broadcast_to(forget_bias[half] + sequence_log, (1, 128))

    def own(array, axis, width):
        return lax.dynamic_slice_in_dim(array, half * width, width, axis)

    taps = jnp.concatenate([own(conv_query, 1, head), own(conv_key, 1, head)], axis=1)
    own_group = lax.dynamic_index_in_dim(group_weight, half, 0, keepdims=False)
    return mixed_rows(
        rows_in,
        packed,
        packed_out,
        gate_weight,
        bias,
        taps,
        own(cell_gain, 0, head)[None],
        own_group,
        own(pool_gain, 0, group)[None],
    )


def solution(mesh):
    in_specs = (
        P("sp", "tp"),
        P("tp"),
        P("sp", "tp"),
        P("sp", "tp"),
        P("sp", "tp"),
        P("sp", "tp"),
        P(),
        P(),
        P("tp"),
        P(None, "tp"),
        P(None, "tp"),
        P("tp"),
        P("sp", "tp"),
        P("tp", None, None),
        P("tp"),
        P("tp", "sp"),
        P("tp", "sp"),
    )
    out_specs = P(("sp", "tp"), None)
    return jax.shard_map(local, mesh=mesh, in_specs=in_specs, out_specs=out_specs, check_vma=False)
```

```python
import functools
import math

import jax
import jax.numpy as jnp
from jax import lax
from jax.experimental import pallas as pl
from jax.experimental.pallas import tpu as pltpu
from jax.sharding import PartitionSpec as P

LEVELS = 4

epsilon = 1e-06
big_negative = -1e30
highest = lax.Precision.HIGHEST
MESH = pl.DeviceIdType.MESH


def remote(src, dst, send, recv, device):
    return pltpu.make_async_remote_copy(
        src_ref=src, dst_ref=dst, send_sem=send, recv_sem=recv,
        device_id=device, device_id_type=MESH,
    )


def columns_of(rows):
    filled = jnp.concatenate(
        rows + [jnp.zeros((128 - len(rows), rows[0].shape[1]), jnp.float32)], axis=0
    )
    return filled.T


def scanned(row, combine, fill):
    length = row.shape[1]
    lane = lax.broadcasted_iota(jnp.int32, (8, length), 1)
    value = jnp.broadcast_to(row, (8, length))
    step = 1
    while step < length:
        moved = pltpu.roll(value, step, 1)
        value = combine(value, jnp.where(lane >= step, moved, fill))
        step *= 2
    return value[:1]


def mixer_kernel(
    pairs, tall, tokens, head, group,
    x_ref, wp_ref, wo_ref, gatew_ref, bias_ref, taps_ref, gain_ref, group_ref, pool_gain_ref,
    out_ref,
    x_out, wp_out, wo_out, normed, inv_s, raw_gate, acc, pre_ref, w_ref,
    edge_q, edge_p, ext, ext_p, q_s, k_s, num_s, small_s, mix_s, st, st_low, st_in, low_in,
    give, got, total,
    local_sem, x_send, x_recv, s_send, s_recv, h_send, h_recv, r_send, r_recv,
    edge_sem, state_send, state_recv, send, recv, d_send, d_recv,
):
    f32, bf16 = jnp.float32, jnp.bfloat16
    height = out_ref.shape[0]
    span = 2 * tokens
    length = tokens
    features = x_out.shape[2]
    sp, tp = lax.axis_index("sp"), lax.axis_index("tp")
    pair, half = sp // 2, sp % 2
    row, side = tp // 2, tp % 2
    width = x_ref.shape[1]
    other = 2 * pair + 1 - half
    sibling = (sp, 2 * row + 1 - side)
    right = (2 * lax.rem(pair + 1, pairs) + half, tp)
    left = (2 * lax.rem(pair + pairs - 1, pairs) + half, tp)
    offsets = [(a, b) for a in range(2) for b in range(tall) if (a, b) != (0, 0)]
    peers = [
        (2 * pair + lax.rem(half + a, 2), 2 * lax.rem(row + b, tall) + side) for a, b in offsets
    ]

    places = [(a, b) for a in range(2) for b in range(tall)][::-1]
    count = len(places)

    def target(a, b):
        return (lax.rem(half + a, 2), lax.rem(row + b, tall))

    barrier = pltpu.get_barrier_semaphore()
    greeted = [sibling]
    for a, b in places[:-1]:
        h, r = target(a, b)
        greeted.append((2 * pair + h, 2 * r + side))
    for d in range(1, pairs):
        greeted.append((2 * lax.rem(pair + d, pairs) + half, tp))
    for device in greeted:
        pl.semaphore_signal(barrier, inc=1, device_id=device, device_id_type=MESH)
    pl.semaphore_wait(barrier, len(greeted))

    def x_block(h, r, s):
        column = pl.multiple_of((2 * r + s) * width, width)
        return x_out.at[h, :, pl.ds(column, width)]

    def ring_copies(k, direction, item):
        if direction == 0:
            source = lax.rem(pair - k + 1 + pairs, pairs)
        else:
            source = lax.rem(pair + k - 1, pairs)
        place = 2 * source + (half if item == 0 else 1 - half)
        target = right if direction == 0 else left
        own = k == 1 and item == 0
        index = ((k - 1) * 2 + direction) * 2 + item
        out = []
        for j, (whole, mine) in enumerate(((wp_out, wp_ref), (wo_out, wo_ref))):
            src = mine.at[half] if own else whole.at[place]
            out.append(
                remote(src, whole.at[place], r_send.at[index, j], r_recv.at[index, j], target)
            )
        return out

    steps = pairs // 2

    def has(k, direction, item):
        return k < steps or (k == steps and direction == item)

    swap = [
        remote(wp_ref.at[1 - half], wp_out.at[sp], h_send.at[0], h_recv.at[0], (other, tp)),
        remote(wo_ref.at[1 - half], wo_out.at[sp], h_send.at[1], h_recv.at[1], (other, tp)),
    ]
    for copy in swap:
        copy.start()
    rings = {}
    for direction in range(2):
        if has(1, direction, 0):
            rings[1, direction, 0] = ring_copies(1, direction, 0)
            for copy in rings[1, direction, 0]:
                copy.start()
    spread = []
    for i, device in enumerate(peers):
        copy = remote(x_ref, x_block(half, row, side), x_send.at[i], x_recv.at[i], device)
        copy.start()
        spread.append(copy)
    locals_ = [
        pltpu.make_async_copy(x_ref, x_block(half, row, side), local_sem.at[0]),
        pltpu.make_async_copy(wp_ref.at[half], wp_out.at[sp], local_sem.at[1]),
        pltpu.make_async_copy(wo_ref.at[half], wo_out.at[sp], local_sem.at[2]),
    ]
    for copy in locals_:
        copy.start()
    passed = [remote(x_ref, x_block(half, row, side), s_send.at[0], s_recv.at[0], sibling)]
    passed[0].start()

    acc[...] = jnp.zeros_like(acc)
    for copy in swap:
        copy.wait_recv()
    for direction in range(2):
        if has(1, direction, 1):
            rings[1, direction, 1] = ring_copies(1, direction, 1)
            for copy in rings[1, direction, 1]:
                copy.start()

    def advance(k):
        for item in range(2):
            for direction in range(2):
                if has(k, direction, item):
                    for copy in rings[k - 1, direction, item]:
                        copy.wait_recv()
                    rings[k, direction, item] = ring_copies(k, direction, item)
                    for copy in rings[k, direction, item]:
                        copy.start()
                elif has(k - 1, direction, item):
                    for copy in rings[k - 1, direction, item]:
                        copy.wait_recv()
            if k == 2 and item == 0:
                pass_on()

    def pass_on():
        for i, (a, b) in enumerate(offsets):
            spread[i].wait_recv()
            block = x_block(lax.rem(half + 2 - a, 2), lax.rem(row + tall - b, tall), side)
            copy = remote(block, block, s_send.at[i + 1], s_recv.at[i + 1], sibling)
            copy.start()
            passed.append(copy)

    for k in range(2, steps + 1):
        advance(k)
    if steps < 2:
        pass_on()
    for copy in passed:
        copy.wait_recv()
    for copy in locals_:
        copy.wait()

    whole_gain = x_out[0, tokens : tokens + 1, :].astype(f32)
    small_rows = 128 if tokens % 128 == 0 else tokens
    for h in range(2):
        @pl.loop(0, tokens // small_rows)
        def _(i):
            start = pl.multiple_of(i * small_rows, small_rows)
            wide = x_out[h, pl.ds(start, small_rows), :].astype(f32)
            squares = jnp.sum(wide * wide, axis=1, keepdims=True)
            there = pl.ds(h * tokens + start, small_rows)
            normed[there, :] = (wide * whole_gain).astype(bf16)
            inverse = lax.rsqrt(squares / features + epsilon)
            inv_s[there, :] = jnp.broadcast_to(inverse, (small_rows, 128))

    big_rows = 256 if span % 256 == 0 else span
    depth = wp_ref.shape[1]
    by_item = depth % 128 == 0

    def add_product(place):
        if by_item:
            @pl.loop(0, span // big_rows)
            def _(i):
                there = pl.ds(pl.multiple_of(i * big_rows, big_rows), big_rows)
                across = pl.ds(pl.multiple_of(place * depth, depth), depth)
                acc[there, :] += jnp.dot(
                    normed[there, across], wp_out[place], preferred_element_type=f32
                )

    @pl.loop(0, span // big_rows)
    def _(i):
        there = pl.ds(pl.multiple_of(i * big_rows, big_rows), big_rows)
        raw_gate[there, :] = inv_s[there, :] * jnp.dot(
            normed[there, :], gatew_ref[...], preferred_element_type=f32
        )

    def arrived_place(k, direction, item):
        source = lax.rem(pair - k + pairs, pairs) if direction == 0 else lax.rem(pair + k, pairs)
        return 2 * source + (half if item == 0 else 1 - half)

    add_product(sp)
    add_product(other)
    for k in range(1, steps):
        for direction in range(2):
            for item in range(2):
                add_product(arrived_place(k, direction, item))
    for direction in range(2):
        for item in range(2):
            if has(steps, direction, item):
                for copy in rings[steps, direction, item][:1]:
                    copy.wait_recv()
                add_product(arrived_place(steps, direction, item))

    @pl.loop(0, span // big_rows)
    def _(i):
        there = pl.ds(pl.multiple_of(i * big_rows, big_rows), big_rows)
        if by_item:
            product_here = acc[there, :]
        else:
            weights = wp_out[...].reshape(-1, wp_out.shape[2])
            product_here = jnp.dot(normed[there, :], weights, preferred_element_type=f32)
        pre_ref[there, :] = (product_here * inv_s[there, :1]).astype(bf16)

    gate_t = raw_gate[...].T
    keep = gate_t[1:2, :] + bias_ref[:, :1]
    small = jnp.exp(-jnp.abs(keep))
    ratio = small / (2.0 + small)
    square = ratio * ratio
    series = jnp.full_like(square, 1.0 / 17.0)
    for odd in (15, 13, 11, 9, 7, 5, 3, 1):
        series = series * square + 1.0 / odd
    log_keep_row = jnp.minimum(keep, 0.0) - 2.0 * ratio * series
    log_in_row = gate_t[0:1, :]

    following = (2 * lax.rem(pair + 1, pairs) + half, tp)
    edges = [
        remote(pre_ref.at[pl.ds(span - 16, 16), pl.ds(0, 2 * head)], edge_q,
               edge_sem.at[0], edge_sem.at[1], following),
        remote(pre_ref.at[pl.ds(span - 16, 16), pl.ds(4 * head, group)], edge_p,
               edge_sem.at[2], edge_sem.at[3], following),
    ]

    @pl.when(pair < pairs - 1)
    def _():
        for copy in edges:
            copy.start()

    @pl.when(pair == 0)
    def _():
        edge_q[...] = jnp.zeros_like(edge_q)
        edge_p[...] = jnp.zeros_like(edge_p)

    ext[pl.ds(16, span), :] = pre_ref[:, : 2 * head].astype(f32)
    ext_p[pl.ds(16, span), :] = pre_ref[:, 4 * head :].astype(f32)

    finals, tops, leads, gaps, cols = [], [], [], [], []
    for c in range(2):
        log_in = log_in_row[:, c * length : (c + 1) * length]
        cumulative = scanned(log_keep_row[:, c * length : (c + 1) * length], jnp.add, 0.0)
        gap = log_in - cumulative
        ceiling = scanned(gap, jnp.maximum, big_negative)
        final = cumulative[:, length - 1 :]
        top = final + ceiling[:, length - 1 :]
        share = jnp.exp(final + gap - top)
        finals.append(final)
        tops.append(top)
        gaps.append(gap)
        cols.append(columns_of([cumulative, ceiling, share]))

    @pl.when(pair > 0)
    def _():
        for copy in edges:
            copy.wait_recv()

    ext[pl.ds(0, 16), :] = edge_q[...].astype(f32)
    ext_p[pl.ds(0, 16), :] = edge_p[...].astype(f32)

    taps = taps_ref.shape[0]
    for c in range(2):
        running = None
        for j in range(taps):
            term = taps_ref[pl.ds(j, 1), :] * ext[pl.ds(16 + c * length - taps + 1 + j, length), :]
            running = term if running is None else running + term
        active = running * jax.nn.sigmoid(running)
        q_s[pl.ds(c * length, length), :] = (active[:, :head] * head ** (-0.5)).astype(bf16)
        k_s[pl.ds(c * length, length), :] = active[:, head:].astype(bf16)

    memories, normals = [], []
    for c in range(2):
        share = cols[c][:, 2:3]
        keys = k_s[pl.ds(c * length, length), :]
        values = pre_ref[pl.ds(c * length, length), pl.ds(2 * head, head)].astype(f32)
        memories.append(
            lax.dot_general(
                (values * share).astype(bf16), keys, (((0,), (0,)), ((), ())),
                preferred_element_type=f32,
            )
        )
        normals.append(jnp.sum(keys.astype(f32) * share, axis=0, keepdims=True))
    both = jnp.maximum(finals[1] + tops[0], tops[1])
    first, second = jnp.exp(finals[1] + tops[0] - both), jnp.exp(tops[1] - both)
    st[...] = (first * memories[0] + second * memories[1]).astype(bf16)
    st_low[...] = jnp.concatenate(
        [
            first * normals[0] + second * normals[1],
            jnp.broadcast_to(both, (1, head)),
            jnp.broadcast_to(finals[0] + finals[1], (1, head)),
            jnp.zeros((5, head), f32),
        ],
        axis=0,
    )
    states = []
    for d in range(1, pairs):
        to = (2 * lax.rem(pair + d, pairs) + half, tp)
        copies = [
            remote(st, st_in.at[d - 1], state_send.at[d - 1, 0], state_recv.at[d - 1, 0], to),
            remote(
                st_low, low_in.at[d - 1], state_send.at[d - 1, 1], state_recv.at[d - 1, 1], to
            ),
        ]
        states.append(copies)
        for copy in copies:
            pl.when(pair + d < pairs)(copy.start)

        @pl.when(pair < d)
        def _():
            st_in[d - 1] = jnp.zeros(st_in.shape[1:], bf16)
            low_in[d - 1] = jnp.zeros(low_in.shape[1:], f32)

    block = 128 if length % 128 == 0 else length
    for c in range(2):
        for t in range(0, length, block):
            reach = t + block
            scores = lax.dot_general(
                q_s[pl.ds(c * length + t, block), :], k_s[pl.ds(c * length, reach), :],
                (((1,), (1,)), ((), ())), preferred_element_type=f32,
            )
            weight = jnp.exp(
                jnp.minimum(gaps[c][:, :reach] - cols[c][t : t + block, 1:2], 0.0)
            )
            t_ids = t + lax.broadcasted_iota(jnp.int32, (block, reach), 0)
            s_ids = lax.broadcasted_iota(jnp.int32, (block, reach), 1)
            scores = jnp.where(t_ids >= s_ids, scores * weight, 0.0).astype(bf16)
            num_s[pl.ds(c * length + t, block), :] = jnp.dot(
                scores, pre_ref[pl.ds(c * length, reach), pl.ds(2 * head, head)],
                preferred_element_type=f32,
            )
            small_s[pl.ds(c * length + t, block), :] = jnp.broadcast_to(
                jnp.sum(scores.astype(f32), axis=1, keepdims=True), (block, 128)
            )

    level = (tp * 2 + half) % LEVELS
    window = None
    for step in range(LEVELS):
        low, high = (0, 2) if step == 0 else (2**step, 2 ** (step + 1))
        part = ext_p[pl.ds(16 - low, span), :]
        for lag in range(low + 1, high):
            part = part + ext_p[pl.ds(16 - lag, span), :]
        if window is None:
            window = part
        else:
            window = window + jnp.where(level >= step, part, 0.0)
    reach = lax.shift_left(jnp.int32(2), level.astype(jnp.int32))
    row_ids = pair * span + lax.broadcasted_iota(jnp.int32, (span, group), 0)
    counted = jnp.minimum(row_ids + 1, reach).astype(f32)
    pooled = (window / counted - ext_p[pl.ds(16, span), :]).astype(bf16)
    mix_s[:, head:] = (
        jnp.dot(pooled, group_ref[...], preferred_element_type=f32) * pool_gain_ref[...]
    ).astype(bf16)

    later = jnp.zeros((1, 1), f32)
    logs = []
    for d in range(1, pairs):
        for copy in states[d - 1]:
            pl.when(pair >= d)(copy.wait_recv)
        logs.append(jnp.where(pair >= d, low_in[d - 1, 1:2, :1] + later, big_negative))
        later = later + low_in[d - 1, 2:3, :1]
    ceiling_in = functools.reduce(jnp.maximum, logs)
    memory_in = jnp.zeros((head, head), f32)
    normal_in = jnp.zeros((1, head), f32)
    for d in range(1, pairs):
        factor = jnp.where(pair >= d, jnp.exp(logs[d - 1] - ceiling_in), 0.0)
        memory_in = memory_in + factor * st_in[d - 1].astype(f32)
        normal_in = normal_in + factor * low_in[d - 1, 0:1, :]
    for c in range(2):
        high = memory_in.astype(bf16)
        low = (memory_in - high.astype(f32)).astype(bf16)
        here = pl.ds(c * length, length)
        queries = q_s[here, :]
        over = (((1,), (1,)), ((), ()))
        far = lax.dot_general(queries, high, over, preferred_element_type=f32)
        far = far + lax.dot_general(queries, low, over, preferred_element_type=f32)
        far_sum = jnp.sum(queries.astype(f32) * normal_in, axis=1, keepdims=True)
        cum, near_top = cols[c][:, 0:1], cols[c][:, 1:2]
        near_log, far_log = cum + near_top, cum + ceiling_in
        ceiling = jnp.maximum(near_log, far_log)
        near_scale, far_scale = jnp.exp(near_log - ceiling), jnp.exp(far_log - ceiling)
        numerator = near_scale * num_s[here, :] + far_scale * far
        denominator = near_scale * small_s[here, :1] + far_scale * far_sum
        hidden = numerator / jnp.maximum(jnp.abs(denominator), jnp.exp(-ceiling))
        hidden = hidden * lax.rsqrt(jnp.mean(hidden * hidden, axis=1, keepdims=True) + epsilon)
        gate = jax.nn.sigmoid(pre_ref[here, pl.ds(3 * head, head)].astype(f32))
        mix_s[here, :head] = (hidden * gain_ref[...] * gate).astype(bf16)
        if c == 0:
            upper = jnp.maximum(finals[0] + ceiling_in, tops[0])
            kept, added = jnp.exp(finals[0] + ceiling_in - upper), jnp.exp(tops[0] - upper)
            memory_in = kept * memory_in + added * memories[0]
            normal_in = kept * normal_in + added * normals[0]
            ceiling_in = upper

    for direction in range(2):
        for item in range(2):
            if has(steps, direction, item):
                for copy in rings[steps, direction, item][1:]:
                    copy.wait_recv()
    columns = wo_out.shape[2]
    for s in range(wo_out.shape[0]):
        w_ref[:, s * columns : (s + 1) * columns] = wo_out[s]

    def product(a, b, s):
        h, r = target(a, b)
        start = pl.multiple_of(((h * tall + r) * 2 + s) * height, height)
        return jnp.dot(
            mix_s[pl.ds(start, height), :], w_ref[...], preferred_element_type=f32
        )

    crossed = []
    for i, (a, b) in enumerate(places):
        give[i] = product(a, b, 1 - side).astype(give.dtype)
        copy = remote(give.at[i], got.at[i], d_send.at[i], d_recv.at[i], sibling)
        copy.start()
        crossed.append(copy)
    sent = []
    for i, (a, b) in enumerate(places):
        mine = product(a, b, side)
        crossed[i].wait_recv()
        mine = mine + got[i].astype(f32)
        if i < count - 1:
            h, r = target(a, b)
            give[count + i] = mine.astype(give.dtype)
            copy = remote(
                give.at[count + i], got.at[count + i], send.at[i], recv.at[i],
                (2 * pair + h, 2 * r + side),
            )
            copy.start()
            sent.append(copy)
        else:
            total[...] = mine
    for i, copy in enumerate(sent):
        copy.wait_recv()
        total[...] += got[count + i].astype(f32)
    out_ref[...] = total[...].astype(out_ref.dtype)
    for copy in crossed + sent:
        copy.wait_send()
    for d in range(1, pairs):
        for copy in states[d - 1]:
            pl.when(pair + d < pairs)(copy.wait_send)

    @pl.when(pair < pairs - 1)
    def _():
        for copy in edges:
            copy.wait_send()

    for copy in swap + spread + passed + [c for copies in rings.values() for c in copies]:
        copy.wait_send()


def mixed_rows(rows_in, packed, packed_out, gate_weight, bias, taps, gain, own_group, pool_gain):
    pairs, n_tp = lax.axis_size("sp") // 2, lax.axis_size("tp")
    tall = n_tp // 2
    f32, bf16 = jnp.float32, jnp.bfloat16
    vmem = pl.BlockSpec(memory_space=pltpu.VMEM)
    dma = pltpu.SemaphoreType.DMA
    slots, steps = 4 * tall - 1, pairs // 2
    head, group = gain.shape[1], pool_gain.shape[1]
    tokens = rows_in.shape[0] - 16
    span, features, height = 2 * tokens, rows_in.shape[1] * n_tp, tokens // n_tp
    width = packed_out.shape[2] * 2 * pairs
    scratch = [
        ((2, rows_in.shape[0], features), bf16),
        ((2 * pairs,) + packed.shape[1:], bf16),
        ((2 * pairs,) + packed_out.shape[1:], bf16),
        ((span, features), bf16),
        ((span, 128), f32),
        ((span, 128), f32),
        ((span, packed.shape[2]), f32),
        ((span, packed.shape[2]), bf16),
        ((head + group, width), bf16),
        ((16, 2 * head), bf16),
        ((16, group), bf16),
        ((span + 16, 2 * head), f32),
        ((span + 16, group), f32),
        ((span, head), bf16),
        ((span, head), bf16),
        ((span, head), f32),
        ((span, 128), f32),
        ((span, head + group), bf16),
        ((head, head), bf16),
        ((8, head), f32),
        ((pairs - 1, head, head), bf16),
        ((pairs - 1, 8, head), f32),
        ((slots, height, width), bf16),
        ((slots, height, width), bf16),
        ((height, width), f32),
    ]
    return pl.pallas_call(
        functools.partial(mixer_kernel, pairs, tall, tokens, head, group),
        out_shape=jax.ShapeDtypeStruct((height, width), bf16),
        in_specs=[vmem] * 9,
        out_specs=vmem,
        scratch_shapes=[pltpu.VMEM(shape, kind) for shape, kind in scratch] + [
            dma((3,)),
            dma((2 * tall,)), dma((2 * tall,)),
            dma((2 * tall,)), dma((2 * tall,)),
            dma((2,)), dma((2,)),
            dma((steps * 4, 2)), dma((steps * 4, 2)),
            dma((4,)), dma((pairs - 1, 2)), dma((pairs - 1, 2)),
            dma((2 * tall,)), dma((2 * tall,)), dma((2 * tall,)), dma((2 * tall,)),
        ],
        compiler_params=pltpu.CompilerParams(
            collective_id=0, has_side_effects=True, vmem_limit_bytes=63 * 2**20
        ),
    )(rows_in, packed, packed_out, gate_weight, bias, taps, gain, own_group, pool_gain)


HALO = 16
ISSUE = ("kv_P", "kv_N", "q_N", "kv_F", "q_F", "op_N", "q_P", "op_P", "op_F")
ISSUE_WO = ("wo_P", "wo_N", "wo_F")


def quad_kernel(
    quads, tokens, head, group,
    x_ref, key_ref, value_ref, query_ref, outgate_ref, pool_ref, cell_out_ref, pool_out_ref,
    norm_ref, in_ref, keep_ref, bias_ref, conv_query_ref, conv_key_ref, gain_ref, group_ref,
    pool_gain_ref,
    out_ref,
    x_all, gain_all, w_all, wo_all, gatew, normed, inv_s, raw_gate, acc, pre_ref, ext, ext_p,
    q_s, k_s, num_s, small_s, mix_s, st_own, low_own, st_near, low_near, st_quad, low_quad,
    st_far, low_far, give, got, give_y, got_y, give_z, got_z, total, out_s,
    local_sem, halo_sem, gain_send, gain_recv, xz_send, xz_recv, xy_send, xy_recv,
    xs_send, xs_recv, z_send, x_send, w_recv, near_send, near_recv, far_send, far_recv,
    c_send, c_recv, y_send, y_recv, t_send, t_recv, out_sem,
):
    f32, bf16 = jnp.float32, jnp.bfloat16
    height = out_ref.shape[0]
    rows = tokens + HALO
    span = 2 * rows
    width = x_ref.shape[1]
    features = x_all.shape[2]
    depth, columns = key_ref.shape[0], cell_out_ref.shape[1]
    sp, tp = lax.axis_index("sp"), lax.axis_index("tp")
    q, l, x = sp // 4, (sp // 2) % 2, sp % 2
    y, side = tp // 2, tp % 2
    here = 2 * q + l
    n_sp = 4 * quads

    def device(plane, x_, y_, side_):
        return (2 * plane + x_, 2 * y_ + side_)

    partner_plane = 2 * q + 1 - l
    beside = device(here, 1 - x, y, side)
    partner = device(partner_plane, x, y, side)
    across = device(here, x, 1 - y, side)
    sibling = device(here, x, y, 1 - side)
    nears, fars = [], []
    for e in range(1, quads):
        other = lax.rem(q + e, quads)
        behind = (other < q).astype(jnp.int32)
        nears.append(2 * other + behind)
        fars.append(2 * other + 1 - behind)
    following = lax.rem(sp + 1, n_sp)
    crowd = [(0, 1), (1, 0), (1, 1)]

    def mate(a, b):
        return (sp, 2 * lax.rem(y + a, 2) + lax.rem(side + b, 2))

    barrier = pltpu.get_barrier_semaphore()
    def flipped(place):
        return place + 2 - 4 * lax.rem(place // 2, 2)

    greeted = [beside, partner, (following, tp), (lax.rem(sp + n_sp - 1, n_sp), tp)]
    greeted += [(flipped(following), tp), (lax.rem(flipped(sp) + n_sp - 1, n_sp), tp)]
    greeted += [mate(a, b) for a, b in crowd]
    greeted += [device(plane, x, y, side) for plane in nears + fars]
    for to in greeted:
        pl.semaphore_signal(barrier, inc=1, device_id=to, device_id_type=MESH)
    pl.semaphore_wait(barrier, len(greeted))

    started = []

    def begin(copy):
        copy.start()
        started.append(copy)

    own_column = pl.ds(pl.multiple_of(tp * width, width), width)

    def column_of(y_, side_):
        return pl.ds(pl.multiple_of((2 * y_ + side_) * width, width), width)

    pieces = (tokens // 2) // HALO * HALO
    cuts = [(HALO, pieces), (HALO + pieces, tokens - pieces), (0, HALO)]

    def x_place(block, cut, column):
        start, size = cuts[cut]
        return x_all.at[block, pl.ds(start, size), column]

    def x_mine(cut):
        start, size = cuts[cut]
        if cut == 2:
            return x_place(l, cut, own_column)
        return x_ref.at[pl.ds(start - HALO, size), :]

    def partner_copy(cut):
        return remote(
            x_mine(cut), x_place(l, cut, own_column), xz_send.at[cut], xz_recv.at[cut], partner
        )

    def across_copy(which, cut):
        src = x_mine(cut) if which == 0 else x_place(1 - l, cut, own_column)
        block = l if which == 0 else 1 - l
        return remote(
            src, x_place(block, cut, own_column), xy_send.at[which, cut], xy_recv.at[which, cut],
            across,
        )

    def sibling_copy(which, cut):
        block = l if which % 2 == 0 else 1 - l
        place = x_place(block, cut, column_of(y if which < 2 else 1 - y, side))
        src = x_mine(cut) if which == 0 else place
        return remote(src, place, xs_send.at[which, cut], xs_recv.at[which, cut], sibling)

    halos, halos_here = [], []
    for i, to in enumerate((following, flipped(following))):
        halos.append(remote(
            x_ref.at[pl.ds(tokens - HALO, HALO), :],
            x_all.at[lax.rem(following // 2, 2), pl.ds(0, HALO), own_column],
            halo_sem.at[i, 0], halo_sem.at[i, 1], (to, tp),
        ))
        place = x_place(l if i == 0 else 1 - l, 2, own_column)
        halos_here.append(remote(place, place, halo_sem.at[i, 0], halo_sem.at[i, 1], (to, tp)))
    for copy in halos:
        pl.when(sp < n_sp - 1)(copy.start)
    for cut in range(2):
        begin(partner_copy(cut))
        begin(across_copy(0, cut))
        begin(sibling_copy(0, cut))

    weights = [
        (key_ref, 0, head), (value_ref, head, head), (query_ref, 2 * head, head),
        (outgate_ref, 3 * head, head), (pool_ref, 4 * head, group),
        (cell_out_ref, 0, head), (pool_out_ref, head, group),
    ]
    classes = {"kv": (0, 1), "q": (2,), "op": (3, 4), "wo": (5, 6)}

    def weight_source(j, half):
        ref, start, size = weights[j]
        cut = pl.ds(pl.multiple_of(half * size, size), size)
        return ref.at[:, cut] if j < 5 else ref.at[cut, :]

    def weight_place(j, place):
        ref, start, size = weights[j]
        if j < 5:
            return w_all.at[pl.ds(pl.multiple_of(place * depth, depth), depth), pl.ds(start, size)]
        return wo_all.at[pl.ds(start, size), pl.ds(pl.multiple_of(place * columns, columns), columns)]

    def send_weight(name, plane):
        for j in classes[name]:
            begin(remote(
                weight_source(j, lax.rem(plane, 2)), weight_place(j, sp),
                z_send.at[plane, j], w_recv.at[sp, j], device(plane, x, y, side),
            ))

    def arrived(name, place):
        for j in classes[name]:
            there = weight_place(j, place)
            remote(there, there, x_send.at[0, j], w_recv.at[place, j], beside).wait_recv()

    def forward(name, plane):
        place = 2 * plane + x
        arrived(name, place)
        for j in classes[name]:
            there = weight_place(j, place)
            begin(remote(there, there, x_send.at[plane, j], w_recv.at[place, j], beside))

    groups = {"P": [partner_plane], "N": nears, "F": fars}

    def send_own(name):
        for j in classes[name]:
            begin(remote(
                weight_source(j, l), weight_place(j, sp), x_send.at[here, j], w_recv.at[sp, j],
                beside,
            ))

    def issue(steps):
        for step in steps:
            name, group_name = step.split("_")
            for plane in groups[group_name]:
                send_weight(name, plane)

    for name in ("kv", "q", "op", "wo"):
        send_own(name)
    issue(ISSUE)
    locals_ = [pltpu.make_async_copy(x_mine(c), x_place(l, c, own_column), local_sem.at[7 + c])
               for c in range(2)]
    locals_ += [
        pltpu.make_async_copy(weight_source(j, l), weight_place(j, sp), local_sem.at[j])
        for j in range(7)
    ]
    for copy in locals_:
        copy.start()

    gain_all[:, own_column] = jnp.broadcast_to(norm_ref[...].reshape(1, width), (HALO, width))
    gains = []
    for i, (a, b) in enumerate(crowd):
        there = gain_all.at[:, own_column]
        copy = remote(there, there, gain_send.at[i], gain_recv.at[i], mate(a, b))
        begin(copy)
        gains.append(copy)
    gatew[...] = jnp.zeros_like(gatew)
    gatew[0:16, :] = jnp.concatenate([in_ref[...], keep_ref[...]], axis=0)

    @pl.when((sp == 0) | (flipped(sp) == 0))
    def _():
        x_all[0, 0:HALO, own_column] = jnp.zeros((HALO, width), bf16)

    for copy, place in zip(halos_here, (sp, flipped(sp))):
        pl.when(place > 0)(copy.wait_recv)
    for which in range(2):
        begin(across_copy(which, 2))
        begin(sibling_copy(which, 2))

    def relay(cut):
        partner_copy(cut).wait_recv()
        begin(across_copy(1, cut))
        begin(sibling_copy(1, cut))

    def from_across(which, cut):
        across_copy(which, cut).wait_recv()
        begin(sibling_copy(2 + which, cut))

    def from_sibling_core(which):
        for block in (which, which + 2):
            for cut in range(3):
                sibling_copy(block, cut).wait_recv()

    def forwards(name, group_name):
        for plane in groups[group_name]:
            forward(name, plane)

    from_across(0, 0)
    relay(0)
    from_across(0, 1)
    from_across(0, 2)
    forwards("kv", "N")
    for copy in gains:
        copy.wait_recv()
    for copy in locals_:
        copy.wait()
    from_sibling_core(0)
    whole_gain = gain_all[0:1, :].astype(f32)

    def strips(size, most, body):
        for start in range(0, size, most):
            body(start, min(most, size - start))

    def normalize(b):
        def body(start, size):
            wide = x_all[b, pl.ds(start, size), :].astype(f32)
            squares = jnp.sum(wide * wide, axis=1, keepdims=True)
            there = pl.ds(pl.multiple_of(b * rows + start, HALO), size)
            normed[there, :] = (wide * whole_gain).astype(bf16)
            inverse = lax.rsqrt(squares / features + epsilon)
            inv_s[there, :] = jnp.broadcast_to(inverse, (size, 128))

        full = rows // 128

        @pl.loop(0, full)
        def _(i):
            body(pl.multiple_of(i * 128, 128), 128)

        if rows % 128:
            body(full * 128, rows % 128)

    def gate_rows(b):
        def body(start, size):
            there = pl.ds(pl.multiple_of(b * rows + HALO + start, HALO), size)
            to = pl.ds(pl.multiple_of(b * tokens + start, HALO), size)
            raw_gate[to, :] = inv_s[there, :] * lax.dot_general(
                normed[there, :], gatew[...], (((1,), (1,)), ((), ())),
                preferred_element_type=f32,
            )

        strips(tokens, 320, body)

    spans = {
        "kv": (0, 2 * head), "q": (2 * head, head), "op": (3 * head, head + group),
        "kvq": (0, 3 * head), "all": (0, 4 * head + group),
    }

    def add_product(name, plane, b, first=False, last=False):
        start, size = spans[name]
        cut = pl.ds(start, size)
        deep = pl.ds(pl.multiple_of(plane * 2 * depth, 2 * depth), 2 * depth)

        def body(row, count):
            there = pl.ds(pl.multiple_of(b * rows + row, HALO), count)
            product = jnp.dot(
                normed[there, deep], w_all[deep, cut], preferred_element_type=f32
            )
            if not first:
                product = product + acc[there, cut]
            if last:
                pre_ref[there, cut] = (product * inv_s[there, :1]).astype(bf16)
            else:
                acc[there, cut] = product

        strips(rows, 256, body)

    def beside_arrived(name, plane):
        arrived(name, 2 * plane + 1 - x)

    normalize(l)
    relay(1)
    gate_rows(l)
    for name in ("kv", "q", "op"):
        beside_arrived(name, here)
    forwards("q", "N")
    add_product("all", here, l, first=True)
    for cut in (2, 0, 1):
        from_across(1, cut)
    forwards("kv", "F")
    from_sibling_core(1)
    normalize(1 - l)
    gate_rows(1 - l)
    add_product("all", here, 1 - l, first=True)
    issue(ISSUE_WO)
    for plane in nears:
        beside_arrived("kv", plane)
        beside_arrived("q", plane)
        for b in range(2):
            add_product("kvq", plane, b)
    gate_t = raw_gate[...].T
    which_row = lax.broadcasted_iota(jnp.int32, (8, 2 * tokens), 0) == tp * 2 + l
    log_in_row = jnp.sum(jnp.where(which_row, gate_t[0:8, :], 0.0), axis=0, keepdims=True)
    keep = jnp.sum(jnp.where(which_row, gate_t[8:16, :], 0.0), axis=0, keepdims=True)
    keep = keep + (bias_ref[l] + math.log(tokens * n_sp))
    small = jnp.exp(-jnp.abs(keep))
    ratio = small / (2.0 + small)
    square = ratio * ratio
    series = jnp.full_like(square, 1.0 / 17.0)
    for odd in (15, 13, 11, 9, 7, 5, 3, 1):
        series = series * square + 1.0 / odd
    log_keep_row = jnp.minimum(keep, 0.0) - 2.0 * ratio * series

    finals, tops, gaps, cols = [], [], [], []
    for b in range(2):
        log_in = log_in_row[:, b * tokens : (b + 1) * tokens]
        cumulative = scanned(log_keep_row[:, b * tokens : (b + 1) * tokens], jnp.add, 0.0)
        gap = log_in - cumulative
        ceiling = scanned(gap, jnp.maximum, big_negative)
        final = cumulative[:, tokens - 1 :]
        top = final + ceiling[:, tokens - 1 :]
        share = jnp.exp(final + gap - top)
        finals.append(final)
        tops.append(top)
        gaps.append(gap)
        cols.append(columns_of([cumulative, ceiling, share]))

    forwards("kv", "P")
    forwards("q", "F")
    for plane in fars:
        beside_arrived("kv", plane)
        for b in range(2):
            add_product("kv", plane, b)
    forwards("op", "N")
    forwards("q", "P")
    beside_arrived("kv", partner_plane)
    for b in range(2):
        add_product("kv", partner_plane, b, last=True)

    taps = conv_key_ref.shape[0]
    own_head = pl.ds(pl.multiple_of(l * head, head), head)
    own_group = pl.ds(pl.multiple_of(l * group, group), group)

    def convolved(conv_ref, start):
        out = []
        for b in range(2):
            ext[...] = pre_ref[pl.ds(b * rows, rows), pl.ds(start, head)].astype(f32)
            running = None
            for j in range(taps):
                term = conv_ref[pl.ds(j, 1), own_head] * ext[pl.ds(HALO - taps + 1 + j, tokens), :]
                running = term if running is None else running + term
            out.append(running * jax.nn.sigmoid(running))
        return out

    for b, active in enumerate(convolved(conv_key_ref, 0)):
        k_s[pl.ds(b * tokens, tokens), :] = active.astype(bf16)

    def values_of(b, size):
        return pre_ref[pl.ds(b * rows + HALO, size), pl.ds(head, head)]

    memories, normals, nearby = [], [], []
    for b in range(2):
        share = cols[b][:, 2:3]
        keys = k_s[pl.ds(b * tokens, tokens), :]
        values = values_of(b, tokens).astype(f32)
        memories.append(
            lax.dot_general(
                (values * share).astype(bf16), keys, (((0,), (0,)), ((), ())),
                preferred_element_type=f32,
            )
        )
        normals.append(jnp.sum(keys.astype(f32) * share, axis=0, keepdims=True))
        st_own[b] = memories[b].astype(bf16)
        low_own[b] = jnp.concatenate(
            [
                normals[b],
                jnp.broadcast_to(tops[b], (1, head)),
                jnp.broadcast_to(finals[b], (1, head)),
                jnp.zeros((5, head), f32),
            ],
            axis=0,
        )
        nearby.append([
            remote(st_own.at[b], st_near.at[b], near_send.at[b, 0], near_recv.at[b, 0], beside),
            remote(low_own.at[b], low_near.at[b], near_send.at[b, 1], near_recv.at[b, 1], beside),
        ])
        for copy in nearby[b]:
            begin(copy)

    forwards("op", "P")
    tail = fars + [partner_plane]
    for i, plane in enumerate(tail):
        beside_arrived("q", plane)
        for b in range(2):
            add_product("q", plane, b, last=i == len(tail) - 1)
    forwards("op", "F")
    for b, active in enumerate(convolved(conv_query_ref, 2 * head)):
        q_s[pl.ds(b * tokens, tokens), :] = (active * head ** (-0.5)).astype(bf16)

    block = 128 if tokens % 128 == 0 else tokens
    for b in range(2):
        for t in range(0, tokens, block):
            reach = t + block
            scores = lax.dot_general(
                q_s[pl.ds(b * tokens + t, block), :], k_s[pl.ds(b * tokens, reach), :],
                (((1,), (1,)), ((), ())), preferred_element_type=f32,
            )
            weight = jnp.exp(
                jnp.minimum(gaps[b][:, :reach] - cols[b][t : t + block, 1:2], 0.0)
            )
            t_ids = t + lax.broadcasted_iota(jnp.int32, (block, reach), 0)
            s_ids = lax.broadcasted_iota(jnp.int32, (block, reach), 1)
            scores = jnp.where(t_ids >= s_ids, scores * weight, 0.0).astype(bf16)
            num_s[pl.ds(b * tokens + t, block), :] = jnp.dot(
                scores, values_of(b, reach), preferred_element_type=f32,
            )
            small_s[pl.ds(b * tokens + t, block), :] = jnp.broadcast_to(
                jnp.sum(scores.astype(f32), axis=1, keepdims=True), (block, 128)
            )

    for copies in nearby:
        for copy in copies:
            copy.wait_recv()
    near_tops = [low_near[b, 1:2, :1] for b in range(2)]
    near_finals = [low_near[b, 2:3, :1] for b in range(2)]
    nothing = jnp.full((1, 1), big_negative, f32)
    first, second = x == 0, x == 1

    def gathered(terms):
        ceiling = functools.reduce(jnp.maximum, [log for log, _, _ in terms])
        memory = jnp.zeros((head, head), f32)
        normal = jnp.zeros((1, head), f32)
        for log, block, line in terms:
            factor = jnp.exp(log - ceiling)
            memory = memory + factor * block().astype(f32)
            normal = normal + factor * line()
        return memory, normal, ceiling

    def near_block(b):
        return lambda: st_near[b]

    def near_line(b):
        return lambda: low_near[b, 0:1, :]

    def own_block(b):
        return lambda: memories[b]

    def own_line(b):
        return lambda: normals[b]

    zero = jnp.zeros((1, 1), f32)
    far_copies = []
    if quads > 1:
        after_near = [
            jnp.where(first, finals[1] + near_finals[1], finals[0] + near_finals[1] + finals[1]),
            jnp.where(first, zero, finals[1]),
        ]
        after_own = [
            jnp.where(first, near_finals[0] + finals[1] + near_finals[1],
                      near_finals[1] + finals[1]),
            jnp.where(first, near_finals[1], zero),
        ]
        quad_memory, quad_normal, quad_top = gathered(
            [(tops[b] + after_own[b], own_block(b), own_line(b)) for b in range(2)]
            + [(near_tops[b] + after_near[b], near_block(b), near_line(b)) for b in range(2)]
        )
        st_quad[...] = quad_memory.astype(bf16)
        low_quad[...] = jnp.concatenate(
            [
                quad_normal,
                jnp.broadcast_to(quad_top, (1, head)),
                jnp.broadcast_to(
                    finals[0] + finals[1] + near_finals[0] + near_finals[1], (1, head)
                ),
                jnp.zeros((5, head), f32),
            ],
            axis=0,
        )
        for d in range(1, quads):
            to = device(2 * lax.rem(q + d, quads) + l, x, y, side)
            copies = [
                remote(st_quad, st_far.at[d - 1], far_send.at[d - 1, 0], far_recv.at[d - 1, 0], to),
                remote(
                    low_quad, low_far.at[d - 1], far_send.at[d - 1, 1], far_recv.at[d - 1, 1], to
                ),
            ]
            far_copies.append(copies)
            for copy in copies:
                pl.when(q + d < quads)(copy.start)

            @pl.when(q < d)
            def _():
                st_far[d - 1] = jnp.zeros(st_far.shape[1:], bf16)
                low_far[d - 1] = jnp.zeros(low_far.shape[1:], f32)

    for plane in nears:
        beside_arrived("op", plane)
        for b in range(2):
            add_product("op", plane, b)
    forwards("wo", "P")
    beside_arrived("op", partner_plane)
    for b in range(2):
        add_product("op", partner_plane, b, last=quads == 1)
    def remember():
        later = jnp.zeros((1, 1), f32)
        if quads > 1:
            logs = []
            for d in range(1, quads):
                for copy in far_copies[d - 1]:
                    pl.when(q >= d)(copy.wait_recv)
                logs.append(jnp.where(q >= d, low_far[d - 1, 1:2, :1] + later, big_negative))
                later = later + low_far[d - 1, 2:3, :1]
            quad_ceiling = functools.reduce(jnp.maximum, logs)
            memory_in = jnp.zeros((head, head), f32)
            normal_in = jnp.zeros((1, head), f32)
            for d in range(1, quads):
                factor = jnp.where(q >= d, jnp.exp(logs[d - 1] - quad_ceiling), 0.0)
                memory_in = memory_in + factor * st_far[d - 1].astype(f32)
                normal_in = normal_in + factor * low_far[d - 1, 0:1, :]
        else:
            quad_ceiling = nothing
            memory_in = jnp.zeros((head, head), f32)
            normal_in = jnp.zeros((1, head), f32)
        come = (lambda: memory_in), (lambda: normal_in)
        entering = [
            gathered([
                (quad_ceiling + jnp.where(first, zero, near_finals[0]),) + come,
                (jnp.where(first, nothing, near_tops[0]), near_block(0), near_line(0)),
            ]),
            gathered([
                (quad_ceiling + finals[0] + near_finals[0] + jnp.where(first, zero, near_finals[1]),)
                + come,
                (tops[0] + jnp.where(first, near_finals[0], near_finals[1]),
                 own_block(0), own_line(0)),
                (near_tops[0] + jnp.where(first, zero, finals[0] + near_finals[1]),
                 near_block(0), near_line(0)),
                (jnp.where(first, nothing, near_tops[1]), near_block(1), near_line(1)),
            ]),
        ]
        for b in range(2):
            memory, normal, ceiling_in = entering[b]
            high = memory.astype(bf16)
            low = (memory - high.astype(f32)).astype(bf16)
            there = pl.ds(b * tokens, tokens)
            queries = q_s[there, :]
            over = (((1,), (1,)), ((), ()))
            far = lax.dot_general(queries, high, over, preferred_element_type=f32)
            far = far + lax.dot_general(queries, low, over, preferred_element_type=f32)
            far_sum = jnp.sum(queries.astype(f32) * normal, axis=1, keepdims=True)
            cum, near_top = cols[b][:, 0:1], cols[b][:, 1:2]
            near_log, far_log = cum + near_top, cum + ceiling_in
            ceiling = jnp.maximum(near_log, far_log)
            near_scale, far_scale = jnp.exp(near_log - ceiling), jnp.exp(far_log - ceiling)
            numerator = near_scale * num_s[there, :] + far_scale * far
            denominator = near_scale * small_s[there, :1] + far_scale * far_sum
            hidden = numerator / jnp.maximum(jnp.abs(denominator), jnp.exp(-ceiling))
            hidden = hidden * lax.rsqrt(jnp.mean(hidden * hidden, axis=1, keepdims=True) + epsilon)
            num_s[there, :] = hidden

    pl.when(q == 0)(remember)
    forwards("wo", "F")
    for i, plane in enumerate(fars):
        beside_arrived("op", plane)
        for b in range(2):
            add_product("op", plane, b, last=i == len(fars) - 1)
    level = (tp * 2 + l) % LEVELS
    ext_p[...] = pre_ref[:, 4 * head :].astype(f32)
    for b in range(2):
        base = b * rows + HALO
        window = None
        for step in range(LEVELS):
            low, high = (0, 2) if step == 0 else (2**step, 2 ** (step + 1))
            part = ext_p[pl.ds(base - low, tokens), :]
            for lag in range(low + 1, high):
                part = part + ext_p[pl.ds(base - lag, tokens), :]
            if window is None:
                window = part
            else:
                window = window + jnp.where(level >= step, part, 0.0)
        reach = lax.shift_left(jnp.int32(2), level.astype(jnp.int32))
        row_ids = (4 * q + 2 * b + x) * tokens + lax.broadcasted_iota(
            jnp.int32, (tokens, group), 0
        )
        counted = jnp.minimum(row_ids + 1, reach).astype(f32)
        pooled = (window / counted - ext_p[pl.ds(base, tokens), :]).astype(bf16)
        mix_s[pl.ds(b * tokens, tokens), head:] = (
            jnp.dot(pooled, group_ref[l], preferred_element_type=f32)
            * pool_gain_ref[:, own_group]
        ).astype(bf16)

    forwards("wo", "N")
    pl.when(q > 0)(remember)
    for b in range(2):
        there = pl.ds(b * tokens, tokens)
        gate = jax.nn.sigmoid(
            pre_ref[pl.ds(b * rows + HALO, tokens), pl.ds(3 * head, head)].astype(f32)
        )
        mix_s[there, :head] = (num_s[there, :] * gain_ref[:, own_head] * gate).astype(bf16)

    def product(block, y_, side_, place):
        start = pl.multiple_of(block * tokens + (2 * y_ + side_) * height, height)
        return jnp.dot(
            mix_s[pl.ds(start, height), :],
            wo_all[:, pl.ds(pl.multiple_of(place * columns, columns), columns)],
            preferred_element_type=f32,
        )

    chunks = [(0, 0, here)] + [(0, 1, plane) for plane in nears]
    chunks += [(0, 0, partner_plane)] + [(0, 1, plane) for plane in fars]
    chunks += [(1, 1, here), (1, 1, partner_plane)] + [(1, 0, plane) for plane in fars + nears]
    chunks = [
        (other, turned, 2 * plane + (1 - x if other else x)) for other, turned, plane in chunks
    ]

    def sibling_part(place):
        return remote(give.at[place], got.at[place], c_send.at[place], c_recv.at[place], sibling)

    def first_part(i, place):
        return remote(
            give_y.at[place], got_y.at[place], y_send.at[place], y_recv.at[place],
            partner if chunks[i][1] else across,
        )

    def second_part(i, place):
        return remote(
            give_z.at[place], got_z.at[place], t_send.at[place], t_recv.at[place],
            across if chunks[i][1] else partner,
        )

    def stage_a(i):
        other, turned, place = chunks[i]
        if other:
            arrived("wo", place)
        for s in range(2):
            for r in range(2):
                give[place, pl.ds((2 * s + r) * height, height), :] = product(
                    s, r, 1 - side, place
                ).astype(bf16)
        begin(sibling_part(place))

    def stage_b(i):
        other, turned, place = chunks[i]

        def slot(k, away):
            if turned:
                return (1 - l if away else l), k
            return k, (1 - y if away else y)

        away = [product(*slot(k, True), side, place) for k in range(2)]
        stay = [product(*slot(k, False), side, place) for k in range(2)]
        sibling_part(place).wait_recv()

        def from_sibling(s, r):
            start = pl.multiple_of((2 * s + r) * height, height)
            return got[place, pl.ds(start, height), :].astype(f32)

        for k in range(2):
            give_y[place, pl.ds(k * height, height), :] = (
                away[k] + from_sibling(*slot(k, True))
            ).astype(bf16)
        begin(first_part(i, place))
        for k in range(2):
            total[place, pl.ds(k * height, height), :] = stay[k] + from_sibling(*slot(k, False))

    def kept(i, away):
        own = y if chunks[i][1] else l
        return pl.ds(pl.multiple_of((1 - own if away else own) * height, height), height)

    def stage_c(i):
        other, turned, place = chunks[i]
        first_part(i, place).wait_recv()
        there = kept(i, True)
        give_z[place] = (total[place, there, :] + got_y[place, there, :].astype(f32)).astype(bf16)
        begin(second_part(i, place))

    def stage_d(i):
        other, turned, place = chunks[i]
        second_part(i, place).wait_recv()
        there = kept(i, False)
        out_s[place] = (
            total[place, there, :] + got_y[place, there, :].astype(f32)
            + got_z[place].astype(f32)
        ).astype(out_ref.dtype)
        store = pltpu.make_async_copy(
            out_s.at[place],
            out_ref.at[:, pl.ds(pl.multiple_of(place * columns, columns), columns)],
            out_sem.at[i],
        )
        store.start()
        stores.append(store)

    count = len(chunks)
    stores = []
    for i in range(count + 1):
        if i < count:
            stage_a(i)
        if i > 0:
            stage_b(i - 1)
    for i in range(count):
        stage_c(i)
        if i == 0:
            sent = len(started) - 1
            for copy in started[:sent - 2 * count]:
                copy.wait_send()
            early = sent - 2 * count
    for i in range(count):
        stage_d(i)
    for copy in stores:
        copy.wait()
    for copy in started[early:]:
        copy.wait_send()
    for copy in halos:
        pl.when(sp < n_sp - 1)(copy.wait_send)
    for d, copies in enumerate(far_copies):
        for copy in copies:
            pl.when(q + d + 1 < quads)(copy.wait_send)


def mixed_quads(
    inputs, norm_gain, query_weight, key_weight, value_weight, outgate_weight, inputgate_weight,
    forget_weight, forget_bias, conv_query, conv_key, cell_gain, pool_weight, group_weight,
    pool_gain, cell_out_weight, pool_out_weight,
):
    n_sp, n_tp = lax.axis_size("sp"), lax.axis_size("tp")
    quads = n_sp // 4
    f32, bf16 = jnp.float32, jnp.bfloat16
    vmem = pl.BlockSpec(memory_space=pltpu.VMEM)
    anywhere = pl.BlockSpec(memory_space=pl.ANY)
    scalars = pl.BlockSpec(memory_space=pltpu.SMEM)
    dma = pltpu.SemaphoreType.DMA
    head, group = query_weight.shape[1] // 2, pool_weight.shape[1] // 2
    tokens = inputs.shape[0]
    rows = tokens + HALO
    features, height = inputs.shape[1] * n_tp, tokens // n_tp
    columns = cell_out_weight.shape[1]
    width = columns * n_sp
    wide = 4 * head + group
    scratch = [
        ((2, rows, features), bf16),
        ((HALO, features), bf16),
        ((features, wide), bf16),
        ((head + group, width), bf16),
        ((128, features), bf16),
        ((2 * rows, features), bf16),
        ((2 * rows, 128), f32),
        ((2 * tokens, 128), f32),
        ((2 * rows, wide), f32),
        ((2 * rows, wide), bf16),
        ((rows, head), f32),
        ((2 * rows, group), f32),
        ((2 * tokens, head), bf16),
        ((2 * tokens, head), bf16),
        ((2 * tokens, head), f32),
        ((2 * tokens, 128), f32),
        ((2 * tokens, head + group), bf16),
        ((2, head, head), bf16),
        ((2, 8, head), f32),
        ((2, head, head), bf16),
        ((2, 8, head), f32),
        ((head, head), bf16),
        ((8, head), f32),
        ((max(quads - 1, 1), head, head), bf16),
        ((max(quads - 1, 1), 8, head), f32),
        ((n_sp, 4 * height, columns), bf16),
        ((n_sp, 4 * height, columns), bf16),
        ((n_sp, 2 * height, columns), bf16),
        ((n_sp, 2 * height, columns), bf16),
        ((n_sp, height, columns), bf16),
        ((n_sp, height, columns), bf16),
        ((n_sp, 2 * height, columns), f32),
        ((n_sp, height, columns), bf16),
    ]
    far = (max(quads - 1, 1), 2)
    sems = [
        (9,), (2, 2), (3,), (3,), (2,), (2,), (2, 3), (2, 3), (4, 3), (4, 3),
        (2 * quads, 7), (2 * quads, 7), (n_sp, 7), (2, 2), (2, 2), far, far,
        (n_sp,), (n_sp,), (n_sp,), (n_sp,), (n_sp,), (n_sp,), (n_sp,),
    ]
    return pl.pallas_call(
        functools.partial(quad_kernel, quads, tokens, head, group),
        out_shape=jax.ShapeDtypeStruct((height, width), bf16),
        in_specs=[anywhere] * 8 + [vmem] * 3 + [scalars] + [vmem] * 5,
        out_specs=anywhere,
        scratch_shapes=[pltpu.VMEM(shape, kind) for shape, kind in scratch]
        + [dma(shape) for shape in sems],
        compiler_params=pltpu.CompilerParams(
            collective_id=0, has_side_effects=True, vmem_limit_bytes=63 * 2**20
        ),
    )(
        inputs, key_weight, value_weight, query_weight, outgate_weight, pool_weight,
        cell_out_weight, pool_out_weight, norm_gain, inputgate_weight.T, forget_weight.T,
        forget_bias, conv_query, conv_key, cell_gain[None], group_weight, pool_gain[None],
    )


def local(
    inputs,
    norm_gain,
    query_weight,
    key_weight,
    value_weight,
    outgate_weight,
    inputgate_weight,
    forget_weight,
    forget_bias,
    conv_query,
    conv_key,
    cell_gain,
    pool_weight,
    group_weight,
    pool_gain,
    cell_out_weight,
    pool_out_weight,
):
    narrow = query_weight.shape[0] % 128 or cell_out_weight.shape[1] % 128
    if not narrow and inputs.shape[0] % 32 == 0 and lax.axis_size("tp") == 4:
        return mixed_quads(
            inputs, norm_gain, query_weight, key_weight, value_weight, outgate_weight,
            inputgate_weight, forget_weight, forget_bias, conv_query, conv_key, cell_gain,
            pool_weight, group_weight, pool_gain, cell_out_weight, pool_out_weight,
        )
    f32, bf16 = jnp.float32, jnp.bfloat16
    sp_index, tp_index = lax.axis_index("sp"), lax.axis_index("tp")
    n_sp = lax.axis_size("sp")
    pairs = n_sp // 2
    pair, half = sp_index // 2, sp_index % 2
    tokens_here = inputs.shape[0]
    span = 2 * tokens_here
    local_heads = forget_bias.shape[0]
    head = query_weight.shape[1] // 2
    group = pool_weight.shape[1] // 2

    def halves(array, axis):
        return jnp.split(array, 2, axis=axis)

    ingredients = [
        halves(w, 1)
        for w in (query_weight, key_weight, value_weight, outgate_weight, pool_weight)
    ]
    packed = jnp.stack([jnp.concatenate([w[j] for w in ingredients], axis=1) for j in range(2)])
    cell_halves, pool_halves = halves(cell_out_weight, 0), halves(pool_out_weight, 0)
    packed_out = jnp.stack(
        [jnp.concatenate([cell_halves[j], pool_halves[j]], axis=0) for j in range(2)]
    )
    gain_rows = jnp.broadcast_to(norm_gain[None, :], (16, norm_gain.shape[0]))
    rows_in = jnp.concatenate([inputs, gain_rows], axis=0)
    head_index = tp_index * local_heads + half
    gate_cols = jnp.concatenate(
        [
            lax.dynamic_slice_in_dim(inputgate_weight, head_index, 1, 1),
            lax.dynamic_slice_in_dim(forget_weight, head_index, 1, 1),
        ],
        axis=1,
    )
    gate_weight = jnp.pad(gate_cols, ((0, 0), (0, 126)))
    sequence_log = math.log(tokens_here * n_sp)
    bias = jnp.broadcast_to(forget_bias[half] + sequence_log, (1, 128))

    def own(array, axis, width):
        return lax.dynamic_slice_in_dim(array, half * width, width, axis)

    taps = jnp.concatenate([own(conv_query, 1, head), own(conv_key, 1, head)], axis=1)
    own_group = lax.dynamic_index_in_dim(group_weight, half, 0, keepdims=False)
    return mixed_rows(
        rows_in,
        packed,
        packed_out,
        gate_weight,
        bias,
        taps,
        own(cell_gain, 0, head)[None],
        own_group,
        own(pool_gain, 0, group)[None],
    )


def solution(mesh):
    in_specs = (
        P("sp", "tp"),
        P("tp"),
        P("sp", "tp"),
        P("sp", "tp"),
        P("sp", "tp"),
        P("sp", "tp"),
        P(),
        P(),
        P("tp"),
        P(None, "tp"),
        P(None, "tp"),
        P("tp"),
        P("sp", "tp"),
        P("tp", None, None),
        P("tp"),
        P("tp", "sp"),
        P("tp", "sp"),
    )
    out_specs = P(("sp", "tp"), None)
    return jax.shard_map(local, mesh=mesh, in_specs=in_specs, out_specs=out_specs, check_vma=False)
```
